256 devices in a mesh: ep: 32 (over z, x), tp: 8 (over y, core).
Axes of the slice: x: 4, y: 4, z: 8, core: 2. Of those that a mesh axis runs over, the one named last changes fastest.
Arguments:
- resid: bfloat16 [1024, 2048], P('ep'), may hold values from -6 to 6
- norm_gain: bfloat16 [2048], replicated, may hold values from 0.099609375 to 1.8984375
- w_query: bfloat16 [2048, 1024], P(None, 'tp'), may hold values from -0.125 to 0.125
- w_key: bfloat16 [2048, 1024], P(None, 'tp'), may hold values from -0.125 to 0.125
- w_value: bfloat16 [2048, 1024], P(None, 'tp'), may hold values from -0.125 to 0.125
- w_gate: bfloat16 [2048, 1024], P(None, 'tp'), may hold values from -0.125 to 0.125
- head_gain: bfloat16 [1024], P('tp'), may hold values from 0.099609375 to 1.8984375
- w_output: bfloat16 [1024, 2048], P('tp'), may hold values from -0.1875 to 0.1875
- state: float32 [1024, 8, 128, 128], P('ep', 'tp'), may hold values from -0.6 to 0.6
- positions: int32 [1024], P('ep'), may hold values from 1024 to 8191
- ffn_gain: bfloat16 [2048], replicated, may hold values from 0.099609375 to 1.8984375
- w_mix: bfloat16 [2048], replicated, may hold values from -0.125 to 0.125
- dense_gate: bfloat16 [2048, 5632], P('tp', 'ep'), may hold values from -0.125 to 0.125
- dense_up: bfloat16 [2048, 5632], P('tp', 'ep'), may hold values from -0.125 to 0.125
- dense_down: bfloat16 [5632, 2048], P('ep', 'tp'), may hold values from -0.15625 to 0.15625
- routes: int32 [1024, 2], P('ep'), may hold values from 0 to 31, all different within a row; in each aligned block of 32 rows (0 to 31, 32 to 63, ...) at most 4 rows name the same one
- route_weight: bfloat16 [1024, 2], P('ep'), may hold values from 0.19921875 to 1
- expert_gate: bfloat16 [32, 2048, 4096], P('ep', None, 'tp'), may hold values from -0.125 to 0.125
- expert_up: bfloat16 [32, 2048, 4096], P('ep', None, 'tp'), may hold values from -0.125 to 0.125
- expert_down: bfloat16 [32, 4096, 2048], P('ep', 'tp'), may hold values from -0.09375 to 0.09375
Outputs:
- final: bfloat16 [1024, 2048], P('ep', 'tp')
- new_state: float32 [1024, 8, 128, 128], P('ep', 'tp')
The draws below stay inside these ranges and needn't reach their ends.
Inputs may be any that keep to these rules, and one draw needn't show every extreme that they name: `routes`: each row names 2 different experts; in the rows of one index of ep no expert is named by more than 4 rows, a bound that some block reaches; every expert is named by some row.
All inputs are finite; a program needn't handle non-finite values.
Results may differ from the reference program's by a relative error of at most 0.018.
Values may be sent and summed in bfloat16 or wider, within the bound.
A program may use at most 64 MiB of HBM per device.

```python
import math
import jax
import jax.numpy as jnp
import numpy as np
from jax import lax

D = 2048
RET_HEADS = 8
HEAD_DIM = 128
RET_W = 1024
FFD = 5632
FFE = 4096
TOPK = 2
SEQ_DEV = 32
SEQS = 1024
EXPERTS = 32
CAP = 4
N_EP = 32
N_TP = 8


def place_ends(values, key, low, top_value):
    place = [jax.random.randint(jax.random.fold_in(key, axis), (), 0, length) for axis, length in enumerate(values.shape)]
    longest = values.shape.index(max(values.shape))
    neighbour = place[:longest] + [(place[longest] + 1) % values.shape[longest]] + place[longest + 1:]
    return values.at[tuple(place)].set(low).at[tuple(neighbour)].set(top_value)


def with_spikes(entries, own_key, source, target, parts, factor):
    def block_of(axis_at):
        return (jnp.arange(entries.shape[axis_at]) // (entries.shape[axis_at] // parts)).reshape((-1,) + (1,) * (entries.ndim - 1 - axis_at))

    near = jax.random.permutation(own_key, parts)[block_of(target)]
    far = (block_of(target) + parts // 2) % parts
    return jnp.where((block_of(source) == near) | (block_of(source) == far), factor * entries, entries)


def level_of(rng, dims, shards, low, top_value):
    factor_of = 1.0
    for dim, parts in shards:
        draws = jax.random.uniform(jax.random.fold_in(jax.random.fold_in(rng, 6), dim), (parts,), jnp.float32, low / len(shards), top_value / len(shards))
        factor_of = factor_of * jnp.repeat(jnp.exp(draws), dims[dim] // parts).reshape((-1,) + (1,) * (len(dims) - 1 - dim))
    return factor_of


def shared_out(rng, own, number, rows, count, top, bound, lean):
    sequence = jax.random.permutation(rng, count)
    heavy_load, usual = load_shares(count, rows * top, bound, lean, True), load_shares(count, rows * top, bound, lean, False)
    places = jnp.arange(count)

    def named(tallies, offset_by):
        used = int((tallies > 0).sum())
        fixed = max(1, used // 4)
        moved = fixed + (places - fixed + offset_by * (used - fixed)) % max(1, count - fixed)
        return jnp.zeros((count,), jnp.int32).at[sequence[jnp.where(places < fixed, places, moved)]].set(jnp.asarray(tallies, jnp.int32))

    tallies = jnp.where(number % 4 == 0, named(heavy_load, number // 4), named(usual, number - number // 4 - 1))
    mixed = jax.random.permutation(jax.random.fold_in(own, 3), count)
    source_of, receiver = mixed[0:count // 2 * 2:2], mixed[1:count // 2 * 2:2]
    margin = jnp.minimum(tallies[source_of] - 1, bound - tallies[receiver]) // 2
    margin = jnp.where((source_of == sequence[0]) | (receiver == sequence[0]) | (tallies[receiver] == 0), 0, jnp.maximum(margin, 0))
    moved = jax.random.randint(jax.random.fold_in(own, 4), (count // 2,), 0, 1 << 20) % (margin + 1)
    tallies = tallies.at[source_of].add(-moved).at[receiver].add(moved)
    labels = jnp.searchsorted(jnp.cumsum(tallies), jnp.arange(rows * top), side="right").astype(jnp.int32)
    grid = labels.reshape(top, rows).T
    grid = grid[jax.random.permutation(jax.random.fold_in(own, 1), rows)]
    offset_by = jax.random.randint(jax.random.fold_in(own, 2), (rows, 1), 0, top)
    return jnp.take_along_axis(grid, (jnp.arange(top)[None, :] + offset_by) % top, axis=1)


def load_shares(number_of, total, limit, skew, full):
    portions = [(1 << 20) // math.isqrt(rank ** skew) + 1 for rank in range(1, number_of + 1)]
    largest = limit if full else min(limit, max(-(-total // number_of), total * portions[0] // sum(portions)))
    least = 1 if total - largest >= number_of - 1 else 0
    given, rest = [largest] + [least] * (number_of - 1), total - largest - least * (number_of - 1)
    while rest > 0:
        free = [i for i in range(1, number_of) if given[i] < largest] or [i for i in range(1, number_of) if given[i] < limit]
        mass, remaining = sum([portions[i] for i in free]), rest
        for i in free:
            extra = min(limit - given[i], max(1, remaining * portions[i] // mass), rest)
            given[i] = given[i] + extra
            rest = rest - extra
    return np.array(given)


def scatter_about(stream_key, dims, deviation, limit, cuts=(), held_as=jnp.bfloat16):
    values = jax.random.normal(stream_key, dims, jnp.float32) * deviation
    if len(cuts) > 0:
        values = level_of(stream_key, dims, cuts, -0.22, 0.18) * values
    return jnp.clip(values, min=-limit, max=limit).astype(held_as)


def heavy_noise(own_key, dims, scale, most, cuts, heavy, kind=jnp.bfloat16):
    values = scale * jax.random.normal(own_key, dims, jnp.float32)
    if cuts:
        values = values * level_of(own_key, dims, cuts, -0.22, 0.18)
    return jnp.clip(with_spikes(values, jax.random.fold_in(own_key, 3), *heavy), -most, most).astype(kind)


def setup_inputs(seed: int = 0) -> dict:
    splits = jax.random.split(jax.random.key(seed), 21)
    resid = scatter_about(splits[0], (SEQS, D), 1.0, 6.0, ((0, 32),))
    norm_gain = jnp.clip(1.0 + 0.18 * jax.random.normal(splits[1], (D,), jnp.float32), 0.099609375, 1.8984375).astype(jnp.bfloat16)
    w_query = scatter_about(splits[2], (D, RET_W), D ** -0.5, 0.125, ((1, 8),))
    w_key = scatter_about(splits[3], (D, RET_W), D ** -0.5, 0.125, ((1, 8),))
    w_value = scatter_about(splits[4], (D, RET_W), D ** -0.5, 0.125, ((1, 8),))
    w_gate = scatter_about(splits[5], (D, RET_W), D ** -0.5, 0.125, ((1, 8),))
    head_gain = jnp.clip(1.0 + 0.18 * jax.random.normal(splits[6], (RET_W,), jnp.float32), 0.099609375, 1.8984375).astype(jnp.bfloat16)
    w_output = scatter_about(splits[7], (RET_W, D), RET_W ** -0.5, 0.1875, ((0, 8),))
    state = scatter_about(splits[8], (SEQS, RET_HEADS, HEAD_DIM, HEAD_DIM), 0.1, 0.6, ((0, 32), (1, 8)), jnp.float32)
    positions = place_ends(jax.random.randint(splits[9], (SEQS,), 1024, 8192), jax.random.fold_in(splits[9], 1), 1024, 8191).astype(jnp.int32)
    ffn_gain = jnp.clip(1.0 + 0.18 * jax.random.normal(splits[10], (D,), jnp.float32), 0.099609375, 1.8984375).astype(jnp.bfloat16)
    w_mix = scatter_about(splits[11], (D,), D ** -0.5, 0.125)
    dense_gate = scatter_about(splits[12], (D, FFD), D ** -0.5, 0.125, ((0, 8), (1, 32)))
    dense_up = scatter_about(splits[13], (D, FFD), D ** -0.5, 0.125, ((0, 8), (1, 32)))
    dense_down = heavy_noise(splits[14], (FFD, D), FFD ** -0.5, 0.15625, ((0, 32), (1, 8)), (0, 1, 32, 2.75))
    routes_keys = jax.random.split(jax.random.fold_in(splits[15], 1), SEQS // SEQ_DEV)
    routes_turns = jax.random.permutation(jax.random.fold_in(splits[15], 3), SEQS // SEQ_DEV)
    routes = jax.vmap(lambda own, number: shared_out(jax.random.fold_in(splits[15], 2), own, number, SEQ_DEV, EXPERTS, TOPK, CAP, 2))(routes_keys, routes_turns).reshape((SEQS, TOPK))
    route_weight = jnp.clip(0.19921875 + 0.80078125 * jax.random.uniform(splits[16], (SEQS, TOPK), jnp.float32) ** level_of(splits[16], (SEQS, TOPK), ((0, 32),), -0.2, 0.2), 0.19921875, 1.0).astype(jnp.bfloat16)
    expert_gate = scatter_about(splits[17], (EXPERTS, D, FFE), D ** -0.5, 0.125, ((0, 32), (2, 8)))
    expert_up = scatter_about(splits[18], (EXPERTS, D, FFE), D ** -0.5, 0.125, ((0, 32), (2, 8)))
    expert_down = scatter_about(splits[19], (EXPERTS, FFE, D), FFE ** -0.5, 0.09375, ((0, 32), (1, 8)))
    return dict(resid=resid, norm_gain=norm_gain, w_query=w_query, w_key=w_key, w_value=w_value, w_gate=w_gate, head_gain=head_gain, w_output=w_output, state=state, positions=positions, ffn_gain=ffn_gain, w_mix=w_mix, dense_gate=dense_gate, dense_up=dense_up, dense_down=dense_down, routes=routes, route_weight=route_weight, expert_gate=expert_gate, expert_up=expert_up, expert_down=expert_down)


EPSILON = 1e-06
THETA = 10000.0

def rms_norm(inputs, scaling):
    square = lax.optimization_barrier(jnp.mean(inputs * inputs, axis=-1, keepdims=True))
    return inputs * lax.rsqrt(square + EPSILON) * scaling.astype(jnp.float32)

def rounded(partial_value):
    return lax.optimization_barrier(partial_value.astype(jnp.bfloat16)).astype(jnp.float32)

def rotate(inputs, places):
    halfway = inputs.shape[-1] // 2
    inverse = THETA ** (-jnp.arange(halfway, dtype=jnp.float32) / halfway)
    angles = places.astype(jnp.float32)[:, None] * inverse[None, :]
    cosine = jnp.cos(angles)[:, None, :]
    sine_of = jnp.sin(angles)[:, None, :]
    former = inputs[..., :halfway]
    latter = inputs[..., halfway:]
    return jnp.concatenate([former * cosine - latter * sine_of, former * sine_of + latter * cosine], axis=-1)

def retain(queries, keys_in, values_in, gating, memory, places, head_first, head_gain):
    seqs_here = queries.shape[0]
    heads_here = memory.shape[1]
    head_size = memory.shape[2]
    head_shape = (seqs_here, heads_here, head_size)
    query_rot = rotate(queries.astype(jnp.float32).reshape(head_shape), places)
    key_rot = rotate(keys_in.astype(jnp.float32).reshape(head_shape), places) * head_size ** (-0.5)
    value_heads = values_in.astype(jnp.float32).reshape(head_shape)
    head_index = head_first + jnp.arange(heads_here, dtype=jnp.float32)
    decays = 1.0 - jnp.exp2(-1.0 - 1.5 * head_index)
    within = lax.optimization_barrier(jnp.sum(query_rot * key_rot, axis=-1, keepdims=True)) * value_heads
    carried = jnp.einsum('shd,shde->she', query_rot, memory, precision=lax.Precision.HIGHEST) * decays[None, :, None]
    mixture = within + carried
    new_memory = decays[None, :, None, None] * memory + key_rot[:, :, :, None] * value_heads[:, :, None, :]
    centre = lax.optimization_barrier(jnp.mean(mixture, axis=-1, keepdims=True))
    spread = lax.optimization_barrier(jnp.mean(jnp.square(mixture - centre), axis=-1, keepdims=True))
    normed = ((mixture - centre) * lax.rsqrt(spread + EPSILON)).reshape(seqs_here, heads_here * head_size)
    normed = normed * head_gain.astype(jnp.float32)
    output = (jax.nn.silu(gating.astype(jnp.float32)) * normed).astype(jnp.bfloat16)
    return (output, new_memory)

def select_slots(route_ids, expert, max_rows):
    flat_ids = route_ids.reshape(-1)
    hits = (flat_ids == expert).astype(jnp.int32)
    ranks = jnp.cumsum(hits) - 1
    slot_range = jnp.arange(max_rows, dtype=jnp.int32)
    matches = (hits[None, :] == 1) & (ranks[None, :] == slot_range[:, None])
    flat_index = jnp.arange(flat_ids.shape[0], dtype=jnp.int32)
    picked = lax.optimization_barrier(jnp.sum(jnp.where(matches, flat_index[None, :], 0), axis=1)).astype(jnp.int32)
    filled = jnp.any(matches, axis=1)
    return (picked, filled)

def expert_hidden(chosen, gate_weight, up_weight):
    gate_value = jnp.dot(chosen, gate_weight, preferred_element_type=jnp.float32)
    up_value = jnp.dot(chosen, up_weight, preferred_element_type=jnp.float32)
    return (jax.nn.silu(gate_value) * up_value).astype(jnp.bfloat16)

def reference(resid, norm_gain, w_query, w_key, w_value, w_gate, head_gain, w_output, state, positions, ffn_gain, w_mix, dense_gate, dense_up, dense_down, routes, route_weight, expert_gate, expert_up, expert_down):
    normed_in = rms_norm(resid.astype(jnp.float32), norm_gain).astype(jnp.bfloat16)

    def project(weight):
        return jnp.dot(normed_in, weight, preferred_element_type=jnp.float32).astype(jnp.bfloat16)
    retained, new_state = retain(project(w_query), project(w_key), project(w_value), project(w_gate), state, positions, 0.0, head_gain)
    width_tp = w_output.shape[0] // N_TP
    attention = jnp.zeros(resid.shape, jnp.float32)
    for block in range(N_TP):
        lower = block * width_tp
        attention = attention + rounded(jnp.dot(retained[:, lower:lower + width_tp], w_output[lower:lower + width_tp], preferred_element_type=jnp.float32))
    middle = resid.astype(jnp.float32) + attention
    normed_mid = rms_norm(middle, ffn_gain).astype(jnp.bfloat16)
    mixing = jax.nn.sigmoid(jnp.dot(normed_mid, w_mix[:, None], preferred_element_type=jnp.float32))
    model_tp = D // N_TP
    gate_sum = jnp.zeros((resid.shape[0], FFD), jnp.float32)
    up_sum = jnp.zeros((resid.shape[0], FFD), jnp.float32)
    for block in range(N_TP):
        lower = block * model_tp
        columns = normed_mid[:, lower:lower + model_tp]
        gate_sum = gate_sum + rounded(jnp.dot(columns, dense_gate[lower:lower + model_tp], preferred_element_type=jnp.float32))
        up_sum = up_sum + rounded(jnp.dot(columns, dense_up[lower:lower + model_tp], preferred_element_type=jnp.float32))
    dense_hidden = (jax.nn.silu(gate_sum) * up_sum).astype(jnp.bfloat16)
    hidden_ep = FFD // N_EP

    def dense_block(total, block):
        lower = block * hidden_ep
        part_hidden = lax.dynamic_slice_in_dim(dense_hidden, lower, hidden_ep, 1)
        part_down = lax.dynamic_slice_in_dim(dense_down, lower, hidden_ep, 0)
        return (total + rounded(jnp.dot(part_hidden, part_down, preferred_element_type=jnp.float32)), None)
    dense_out, _ = lax.scan(dense_block, jnp.zeros(resid.shape, jnp.float32), jnp.arange(N_EP, dtype=jnp.int32))
    max_rows = N_EP * CAP
    expert_tp = FFE // N_TP
    flat_weight = route_weight.reshape(-1).astype(jnp.float32)

    def one_expert(total, expert):
        picked, filled = select_slots(routes, expert, max_rows)
        token_rows = picked // TOPK
        chosen = normed_mid[token_rows]
        hidden_e = expert_hidden(chosen, expert_gate[expert], expert_up[expert])
        summed = jnp.zeros((max_rows, D), jnp.float32)
        for block in range(N_TP):
            lower = block * expert_tp
            summed = summed + rounded(jnp.dot(hidden_e[:, lower:lower + expert_tp], expert_down[expert, lower:lower + expert_tp], preferred_element_type=jnp.float32))
        result = rounded(summed)
        weights_e = jnp.where(filled, flat_weight[picked], 0.0)
        total = total.at[token_rows].add(weights_e[:, None] * result)
        return (total, None)
    moe_out, _ = lax.scan(one_expert, jnp.zeros(resid.shape, jnp.float32), jnp.arange(EXPERTS, dtype=jnp.int32))
    final = (middle + moe_out + mixing * dense_out).astype(jnp.bfloat16)
    return (final, new_state)
```

```python
import numpy as np
import jax
import jax.numpy as jnp
from jax import lax
from jax.experimental import pallas as pl
from jax.experimental.pallas import tpu as pltpu
from jax.sharding import PartitionSpec as P

EPSILON = 1e-06
THETA = 10000.0
BF = jnp.bfloat16
F32 = jnp.float32
NZ, NX, NT = 8, 4, 8


def iota(shape, dim):
    return lax.broadcasted_iota(jnp.int32, shape, dim)


def onehot(condition):
    return jnp.where(condition, 1.0, 0.0).astype(BF)


def dot(a, b):
    return jnp.dot(a, b, preferred_element_type=F32)


def as_column(row, n):
    return jnp.sum(jnp.where(iota((n, n), 0) == iota((n, n), 1), row, 0.0), axis=1, keepdims=True)


def as_row(column, n):
    return jnp.sum(jnp.where(iota((n, n), 0) == iota((n, n), 1), column, 0.0), axis=0, keepdims=True)


def step_kernel(
    resid_h, norm_gain_h, wq_h, wk_h, wv_h, wg_h, head_gain_h, wo_h, state_h, positions_h,
    ffn_gain_h, w_mix_h, dgate_h, dup_h, ddown_h, routes_h, rweight_h, eg_h, eu_h, ed_h, inv_h,
    final_h, new_state_h,
    resid, norm_gain, wqkvg, head_gain, wo, state, positions, ffn_gain, w_mix, dgate, dup, ddown,
    routes, rweight, eg, eu, ed, inv,
    mix, rs_send, rs_recv, p2_send, p2_recv, rows_x, gu, dn, part_y, yx_recv, yz_send, yz_recv,
    md_send, mz_recv, mx_send, mx_recv, ag_recv, er_send, er_recv, rx_send, rx_recv,
    rz_send, rz_recv, d5_send, d5_recv, acc, final_v,
    load_sem, out_sem,
    rs_s, rs_r, p2_s, p2_r, xz_s, xz_r, xx_s, xx_r, gw_s, gw_r, dw_s, dw_r, yx_s, yx_r, yz_s, yz_r,
    mz_s, mz_r, mx_s, mx_r, ag_s, ag_r, er_s, er_r, rx_s, rx_r, rz_s, rz_r, d5_s, d5_r,
):
    ep = lax.axis_index("ep")
    t = lax.axis_index("tp")
    z = ep // NX
    x = lax.rem(ep, NX)
    y = t // 2
    core = lax.rem(t, 2)

    def zdev(p):
        return (p * NX + x, t)

    def xdev(p):
        return (z * NX + p, t)

    def tdev(p):
        return (ep, p)

    barrier = pltpu.get_barrier_semaphore()
    for dev, me, n in ((zdev, z, NZ), (xdev, x, NX), (tdev, t, NT)):
        def greet(k, c, dev=dev, me=me, n=n):
            pl.semaphore_signal(barrier, inc=1, device_id=dev(lax.rem(me + k, n)), device_id_type=pl.DeviceIdType.MESH)
            return c
        lax.fori_loop(1, n, greet, 0)

    loads = {}
    pairs = [
        ("resid", resid_h, resid), ("norm_gain", norm_gain_h, norm_gain),
        ("wq", wq_h, wqkvg.at[:, 0:128]), ("wk", wk_h, wqkvg.at[:, 128:256]),
        ("wv", wv_h, wqkvg.at[:, 256:384]), ("wg", wg_h, wqkvg.at[:, 384:512]),
        ("positions", positions_h, positions), ("inv", inv_h, inv), ("head_gain", head_gain_h, head_gain),
        ("state", state_h.at[:, 0], state), ("wo", wo_h, wo),
        ("ffn_gain", ffn_gain_h, ffn_gain), ("w_mix", w_mix_h, w_mix),
        ("routes", routes_h, routes), ("rweight", rweight_h, rweight),
        ("dgate", dgate_h, dgate), ("dup", dup_h, dup), ("ddown", ddown_h, ddown),
        ("eg", eg_h.at[0], eg), ("eu", eu_h.at[0], eu), ("ed", ed_h.at[0], ed),
    ]
    for n, (name, src, dst) in enumerate(pairs):
        loads[name] = pltpu.make_async_copy(src, dst, load_sem.at[n])
        loads[name].start()

    def need(*names):
        for name in names:
            loads[name].wait()

    def remote(src, dst, ssem, rsem, dev):
        return pltpu.make_async_remote_copy(
            src_ref=src, dst_ref=dst, send_sem=ssem, recv_sem=rsem, device_id=dev,
            device_id_type=pl.DeviceIdType.MESH,
        )

    def send_all(n, me, dev, src_at, dst_here, ssem, rsem):
        def one(k, c):
            p = lax.rem(me + k, n)
            remote(src_at(p), dst_here, ssem.at[p], rsem.at[me], dev(p)).start()
            return c
        lax.fori_loop(1, n, one, 0)

    def recv_all(n, me, dev, src, dst_at, ssem, rsem):
        def one(k, c):
            p = lax.rem(me + k, n)
            remote(src, dst_at(p), ssem.at[p], rsem.at[p], dev(p)).wait_recv()
            return c
        lax.fori_loop(1, n, one, 0)

    def sent_all(n, me, dev, src_at, dst, ssem, rsem):
        def one(k, c):
            p = lax.rem(me + k, n)
            remote(src_at(p), dst, ssem.at[p], rsem.at[me], dev(p)).wait_send()
            return c
        lax.fori_loop(1, n, one, 0)

    need("resid", "norm_gain")
    res = resid[...].astype(F32)
    ms = jnp.mean(res * res, axis=-1, keepdims=True)
    gain_in = norm_gain[...].reshape(1, 2048).astype(F32)
    normed_in = (res * lax.rsqrt(ms + EPSILON) * gain_in).astype(BF)
    need("positions", "inv", "wq", "wk", "wv", "wg")
    angles = as_column(positions[...].astype(F32).reshape(1, 32), 32) * inv[...]
    cosine, sine = jnp.cos(angles), jnp.sin(angles)
    cos2 = jnp.concatenate([cosine, cosine], axis=-1)
    sin2 = jnp.concatenate([-sine, sine], axis=-1)
    qkvg = dot(normed_in, wqkvg[...]).astype(BF).astype(F32)

    def rotate(v):
        return v * cos2 + pltpu.roll(v, 64, 1) * sin2

    query = rotate(qkvg[:, 0:128])
    key = rotate(qkvg[:, 128:256]) * (128 ** -0.5)
    value = qkvg[:, 256:384]
    gating = qkvg[:, 384:512]
    decay = 1.0 - jnp.exp2(-1.0 - 1.5 * jnp.full((1, 128), t, jnp.int32).astype(F32))
    within = jnp.sum(query * key, axis=-1, keepdims=True) * value
    query_t = jnp.transpose(query)
    need("state")
    for s in range(32):
        mix[s : s + 1, :] = jnp.sum(state[s] * query_t[:, s : s + 1], axis=0, keepdims=True)
    need("head_gain", "wo")
    mixture = within + mix[...] * decay
    centre = jnp.mean(mixture, axis=-1, keepdims=True)
    spread = jnp.mean(jnp.square(mixture - centre), axis=-1, keepdims=True)
    normed = (mixture - centre) * lax.rsqrt(spread + EPSILON)
    normed = normed * head_gain[...].reshape(1, 128).astype(F32)
    retained = (jax.nn.silu(gating) * normed).astype(BF)
    partial = dot(retained, wo[...]).astype(BF)
    for p in range(NT):
        rs_send[p] = partial[:, 256 * p : 256 * (p + 1)]

    pl.semaphore_wait(barrier, NZ + NX + NT - 3)

    send_all(NT, t, tdev, lambda p: rs_send.at[p], rs_recv.at[t], rs_s, rs_r)
    rs_recv[t] = rs_send[t]

    key_t = jnp.transpose(key)
    for s in range(32):
        state[s] = state[s] * decay + key_t[:, s : s + 1] * value[s : s + 1, :]

    need("routes", "rweight", "dgate", "dup", "ddown", "ffn_gain", "w_mix")
    first, second = routes[:, 0:1], routes[:, 1:2]
    lane_e = iota((32, 32), 1)
    hit0, hit1 = (lane_e == first), (lane_e == second)
    both = jnp.where(hit0, 1.0, 0.0) + jnp.where(hit1, 1.0, 0.0)
    earlier = onehot(iota((32, 32), 1) < iota((32, 32), 0))
    rank = dot(earlier, both.astype(BF))
    rw = rweight[...].astype(F32)
    weight_e = jnp.where(hit0, rw[:, 0:1], 0.0) + jnp.where(hit1, rw[:, 1:2], 0.0)
    widen = onehot((iota((32, 128), 1) >> 2) == iota((32, 128), 0))
    slot = (iota((32, 128), 1) & 3).astype(F32)
    taken = dot(both.astype(BF), widen) * jnp.where(dot(rank.astype(BF), widen) == slot, 1.0, 0.0)
    combine = (dot(weight_e.astype(BF), widen) * taken).astype(BF)
    dispatch = jnp.transpose(taken).astype(BF)

    place_gate = onehot(iota((176, 384), 1) == iota((176, 384), 0))
    place_up = onehot(iota((176, 384), 1) == iota((176, 384), 0) + 176)
    gu[t] = (dot(dgate[...], place_gate) + dot(dup[...], place_up)).astype(BF)
    for p in range(NT):
        dn[p, 176:256, :] = jnp.zeros((80, 256), BF)
    dn[t, 0:176, :] = ddown[...]

    recv_all(NT, t, tdev, rs_send.at[0], lambda p: rs_recv.at[p], rs_s, rs_r)
    columns = pl.ds(pl.multiple_of(t * 256, 256), 256)
    attention = rs_recv[0].astype(F32)
    for p in range(1, NT):
        attention = attention + rs_recv[p].astype(F32)
    middle = resid[:, columns].astype(F32) + attention
    squares = as_row(jnp.sum(middle * middle, axis=-1, keepdims=True), 32)
    squares = jnp.concatenate([squares, jnp.zeros((1, 224), F32)], axis=1)

    for p in range(NT):
        p2_send[p, 0:4, :] = middle[4 * p : 4 * p + 4, :]
        p2_send[p, 4:5, :] = squares
    send_all(NT, t, tdev, lambda p: p2_send.at[p], p2_recv.at[t], p2_s, p2_r)
    p2_recv[t] = p2_send[t]
    new_state_copy = pltpu.make_async_copy(state, new_state_h.at[:, 0], out_sem.at[0])
    new_state_copy.start()
    recv_all(NT, t, tdev, p2_send.at[0], lambda p: p2_recv.at[p], p2_s, p2_r)

    total = p2_recv[0, 4:5, 0:128]
    for p in range(1, NT):
        total = total + p2_recv[p, 4:5, 0:128]
    scale = lax.rsqrt(as_column(total[:, 0:32], 32) * (1.0 / 2048) + EPSILON)
    gain_mid = ffn_gain[...].reshape(1, 2048).astype(F32)
    gain_here = gain_mid[:, 0:256]
    for p in range(1, NT):
        gain_here = jnp.where(t == p, gain_mid[:, 256 * p : 256 * (p + 1)], gain_here)
    normed_mid = (middle * scale * gain_here).astype(BF)

    outgoing = dot(dispatch, normed_mid).astype(BF)
    for p in range(NZ):
        md_send[p] = outgoing[16 * p : 16 * (p + 1), :]
    send_all(NZ, z, zdev, lambda p: md_send.at[p], mz_recv.at[z], mz_s, mz_r)
    mz_recv[z] = md_send[z]

    quarters = [
        jnp.concatenate([p2_recv[2 * q, 0:4, :], p2_recv[2 * q + 1, 0:4, :]], axis=1) for q in range(4)
    ]
    sq4 = sum(jnp.sum(v * v, axis=-1, keepdims=True) for v in quarters)
    scale4 = lax.rsqrt(sq4 * (1.0 / 2048) + EPSILON)
    mixer = w_mix[...].reshape(1, 2048).astype(F32)
    rows = [
        (quarters[q] * scale4 * gain_mid[:, 512 * q : 512 * (q + 1)]).astype(BF).astype(F32) for q in range(4)
    ]
    mixing = jax.nn.sigmoid(
        sum(jnp.sum(rows[q] * mixer[:, 512 * q : 512 * (q + 1)], axis=-1, keepdims=True) for q in range(4))
    )
    mixing16 = jnp.concatenate([mixing] * 4, axis=0)
    rows_x[x, z] = jnp.concatenate(rows, axis=0).astype(BF)
    send_all(NZ, z, zdev, lambda p: rows_x.at[x, z], rows_x.at[x, z], xz_s, xz_r)

    def to_x(zz):
        send_all(NX, x, xdev, lambda p: rows_x.at[x, zz], rows_x.at[x, zz], xx_s.at[zz], xx_r.at[zz])

    to_x(z)

    def ydev(p):
        return (ep, 2 * p + core)

    send_all(4, y, ydev, lambda p: gu.at[t], gu.at[t], gw_s, gw_r)
    send_all(4, y, ydev, lambda p: dn.at[t], dn.at[t], dw_s, dw_r)
    sibling = (ep, t + 1 - 2 * core)
    remote(gu.at[t], gu.at[t], gw_s.at[4 + y], gw_r.at[4 + y], sibling).start()
    remote(dn.at[t], dn.at[t], dw_s.at[4 + y], dw_r.at[4 + y], sibling).start()

    swap = onehot(
        iota((128, 128), 1)
        == ((iota((128, 128), 0) >> 2) & 7) * 16 + (iota((128, 128), 0) >> 5) * 4 + (iota((128, 128), 0) & 3)
    )
    unswap = onehot(
        iota((128, 128), 1)
        == ((iota((128, 128), 0) >> 2) & 3) * 32 + (iota((128, 128), 0) >> 4) * 4 + (iota((128, 128), 0) & 3)
    )
    recv_all(NZ, z, zdev, md_send.at[0], lambda p: mz_recv.at[p], mz_s, mz_r)
    swapped = dot(swap, jnp.concatenate([mz_recv[p] for p in range(NZ)], axis=0)).astype(BF)
    for p in range(NX):
        mx_send[p] = swapped[32 * p : 32 * (p + 1), :]
    send_all(NX, x, xdev, lambda p: mx_send.at[p], mx_recv.at[x], mx_s, mx_r)
    mx_recv[x] = mx_send[x]

    def pass_on(k, c):
        p = lax.rem(z + k, NZ)
        remote(rows_x.at[x, p], rows_x.at[x, p], xz_s.at[p], xz_r.at[p], zdev(p)).wait_recv()
        to_x(p)
        return c
    lax.fori_loop(1, NZ, pass_on, 0)

    recv_all(NX, x, xdev, mx_send.at[0], lambda p: mx_recv.at[p], mx_s, mx_r)
    ag_recv[t] = jnp.concatenate([mx_recv[p] for p in range(NX)], axis=0)
    send_all(NT, t, tdev, lambda p: ag_recv.at[t], ag_recv.at[t], ag_s, ag_r)

    def hand_over(k, c):
        p = lax.rem(y + k, 4)
        tt = 2 * p + core
        remote(gu.at[tt], gu.at[tt], gw_s.at[p], gw_r.at[p], ydev(p)).wait_recv()
        remote(gu.at[tt], gu.at[tt], gw_s.at[4 + p], gw_r.at[4 + p], sibling).start()
        remote(dn.at[tt], dn.at[tt], dw_s.at[p], dw_r.at[p], ydev(p)).wait_recv()
        remote(dn.at[tt], dn.at[tt], dw_s.at[4 + p], dw_r.at[4 + p], sibling).start()
        return c
    lax.fori_loop(1, 4, hand_over, 0)

    def all_weights(k, c):
        tt = 2 * k + 1 - core
        remote(gu.at[tt], gu.at[tt], gw_s.at[4 + k], gw_r.at[4 + k], sibling).wait_recv()
        remote(dn.at[tt], dn.at[tt], dw_s.at[4 + k], dw_r.at[4 + k], sibling).wait_recv()
        return c
    lax.fori_loop(0, 4, all_weights, 0)

    def rows_in(zz, c):
        recv_all(NX, x, xdev, rows_x.at[x, zz], lambda p: rows_x.at[p, zz], xx_s.at[zz], xx_r.at[zz])
        return c
    lax.fori_loop(0, NZ, rows_in, 0)

    tiles = rows_x[...].reshape(512, 512)
    spread_row = iota((128, 512), 0)
    spread_col = iota((128, 512), 1)
    gate_up = jnp.zeros((128, 384), F32)
    for q in range(4):
        take = onehot(spread_col == (spread_row >> 2) * 16 + 4 * q + (spread_row & 3))
        block = dot(take, tiles).astype(BF)
        gate_up = gate_up + dot(block, gu[2 * q : 2 * q + 2].reshape(512, 384))
    up = pltpu.roll(gate_up, 384 - 176, 1)
    hidden = jnp.where(iota((128, 256), 1) < 176, jax.nn.silu(gate_up[:, 0:256]) * up[:, 0:256], 0.0).astype(BF)
    back_row = iota((512, 128), 0)
    back_col = iota((512, 128), 1)
    packed = jnp.zeros((512, 512), F32)
    for q in range(4):
        block = jnp.concatenate([dot(hidden, dn[2 * q]), dot(hidden, dn[2 * q + 1])], axis=1).astype(BF)
        put = onehot(back_row == (back_col >> 2) * 16 + 4 * q + (back_col & 3))
        packed = packed + dot(put, block)
    part_y[...] = packed.astype(BF).reshape(NX, 128, 512)
    send_all(NX, x, xdev, lambda p: part_y.at[p], yx_recv.at[x], yx_s, yx_r)
    yx_recv[x] = part_y[x]

    need("eg", "eu", "ed")

    def chunk(p, c):
        @pl.when(p != t)
        def _():
            remote(ag_recv.at[t], ag_recv.at[p], ag_s.at[p], ag_r.at[p], tdev(p)).wait_recv()
        depth = pl.ds(pl.multiple_of(p * 256, 256), 256)
        rows_p = ag_recv[p]
        acc[:, 0:512] += dot(rows_p, eg[depth, :])
        acc[:, 512:1024] += dot(rows_p, eu[depth, :])
        return c
    acc[...] = jnp.zeros_like(acc)
    lax.fori_loop(0, NT, chunk, 0)
    hidden_e = (jax.nn.silu(acc[:, 0:512]) * acc[:, 512:1024]).astype(BF)

    def down(k, c):
        p = lax.rem(t + 1 + k, NT)
        er_send[p] = dot(hidden_e, ed[:, pl.ds(pl.multiple_of(p * 256, 256), 256)]).astype(BF)
        @pl.when(p != t)
        def _():
            remote(er_send.at[p], er_recv.at[t], er_s.at[p], er_r.at[t], tdev(p)).start()
        return c
    lax.fori_loop(0, NT, down, 0)
    er_recv[t] = er_send[t]

    recv_all(NX, x, xdev, part_y.at[0], lambda p: yx_recv.at[p], yx_s, yx_r)
    summed = yx_recv[0].astype(F32)
    for p in range(1, NX):
        summed = summed + yx_recv[p].astype(F32)
    yz_send[...] = summed.astype(BF).reshape(NZ, 16, 512)
    send_all(NZ, z, zdev, lambda p: yz_send.at[p], yz_recv.at[z], yz_s, yz_r)
    yz_recv[z] = yz_send[z]

    recv_all(NT, t, tdev, er_send.at[0], lambda p: er_recv.at[p], er_s, er_r)
    result = er_recv[0].astype(F32)
    for p in range(1, NT):
        result = result + er_recv[p].astype(F32)
    rx_send[...] = result.astype(BF).reshape(NX, 32, 256)
    send_all(NX, x, xdev, lambda p: rx_send.at[p], rx_recv.at[x], rx_s, rx_r)
    rx_recv[x] = rx_send[x]

    recv_all(NZ, z, zdev, yz_send.at[0], lambda p: yz_recv.at[p], yz_s, yz_r)
    dense = yz_recv[0].astype(F32)
    for p in range(1, NZ):
        dense = dense + yz_recv[p].astype(F32)
    dense = dense * mixing16
    for p in range(NT):
        q, half = p // 2, p % 2
        d5_send[p, 0:4, :] = dense[4 * q : 4 * q + 4, 256 * half : 256 * (half + 1)]
        d5_send[p, 4:8, :] = jnp.zeros((4, 256), F32)
    send_all(NT, t, tdev, lambda p: d5_send.at[p], d5_recv.at[t], d5_s, d5_r)
    d5_recv[t] = d5_send[t]

    recv_all(NX, x, xdev, rx_send.at[0], lambda p: rx_recv.at[p], rx_s, rx_r)
    home = dot(unswap, jnp.concatenate([rx_recv[p] for p in range(NX)], axis=0)).astype(BF)
    for p in range(NZ):
        rz_send[p] = home[16 * p : 16 * (p + 1), :]
    send_all(NZ, z, zdev, lambda p: rz_send.at[p], rz_recv.at[z], rz_s, rz_r)
    rz_recv[z] = rz_send[z]

    recv_all(NT, t, tdev, d5_send.at[0], lambda p: d5_recv.at[p], d5_s, d5_r)
    dense_rows = jnp.concatenate([d5_recv[p, 0:4, :] for p in range(NT)], axis=0)
    recv_all(NZ, z, zdev, rz_send.at[0], lambda p: rz_recv.at[p], rz_s, rz_r)
    moe = dot(combine, jnp.concatenate([rz_recv[p] for p in range(NZ)], axis=0))
    final_v[...] = (middle + moe + dense_rows).astype(BF)
    final_copy = pltpu.make_async_copy(final_v, final_h, out_sem.at[1])
    final_copy.start()

    sent_all(NT, t, tdev, lambda p: rs_send.at[p], rs_recv.at[t], rs_s, rs_r)
    sent_all(NT, t, tdev, lambda p: p2_send.at[p], p2_recv.at[t], p2_s, p2_r)
    sent_all(NZ, z, zdev, lambda p: md_send.at[p], mz_recv.at[z], mz_s, mz_r)
    sent_all(NZ, z, zdev, lambda p: rows_x.at[x, z], rows_x.at[x, z], xz_s, xz_r)

    def x_sent(zz, c):
        sent_all(NX, x, xdev, lambda p: rows_x.at[x, zz], rows_x.at[x, zz], xx_s.at[zz], xx_r.at[zz])
        return c
    lax.fori_loop(0, NZ, x_sent, 0)
    sent_all(4, y, ydev, lambda p: gu.at[t], gu.at[t], gw_s, gw_r)
    sent_all(4, y, ydev, lambda p: dn.at[t], dn.at[t], dw_s, dw_r)

    def w_sent(k, c):
        tt = 2 * k + core
        remote(gu.at[tt], gu.at[tt], gw_s.at[4 + k], gw_r.at[4 + k], sibling).wait_send()
        remote(dn.at[tt], dn.at[tt], dw_s.at[4 + k], dw_r.at[4 + k], sibling).wait_send()
        return c
    lax.fori_loop(0, 4, w_sent, 0)
    sent_all(NX, x, xdev, lambda p: mx_send.at[p], mx_recv.at[x], mx_s, mx_r)
    sent_all(NT, t, tdev, lambda p: ag_recv.at[t], ag_recv.at[t], ag_s, ag_r)
    sent_all(NX, x, xdev, lambda p: part_y.at[p], yx_recv.at[x], yx_s, yx_r)
    sent_all(NT, t, tdev, lambda p: er_send.at[p], er_recv.at[t], er_s, er_r)
    sent_all(NZ, z, zdev, lambda p: yz_send.at[p], yz_recv.at[z], yz_s, yz_r)
    sent_all(NX, x, xdev, lambda p: rx_send.at[p], rx_recv.at[x], rx_s, rx_r)
    sent_all(NT, t, tdev, lambda p: d5_send.at[p], d5_recv.at[t], d5_s, d5_r)
    sent_all(NZ, z, zdev, lambda p: rz_send.at[p], rz_recv.at[z], rz_s, rz_r)
    new_state_copy.wait()
    final_copy.wait()


def per_device(*args):
    inv = jnp.asarray((THETA ** (-np.arange(64) / 64.0)).astype(np.float32)[None, :])
    dma = pltpu.SemaphoreType.DMA
    vmem = pltpu.VMEM
    scratch = [
        vmem((32, 2048), BF), vmem((2048,), BF), vmem((2048, 512), BF), vmem((128,), BF),
        vmem((128, 2048), BF), vmem((32, 128, 128), F32), vmem((32,), jnp.int32), vmem((2048,), BF),
        vmem((2048,), BF), vmem((256, 176), BF), vmem((256, 176), BF), vmem((176, 256), BF),
        vmem((32, 2), jnp.int32), vmem((32, 2), BF), vmem((2048, 512), BF), vmem((2048, 512), BF),
        vmem((512, 2048), BF), vmem((1, 64), F32),
        vmem((32, 128), F32), vmem((8, 32, 256), BF), vmem((8, 32, 256), BF),
        vmem((8, 8, 256), F32), vmem((8, 8, 256), F32), vmem((4, 8, 16, 512), BF),
        vmem((8, 256, 384), BF), vmem((8, 256, 256), BF), vmem((4, 128, 512), BF), vmem((4, 128, 512), BF),
        vmem((8, 16, 512), BF), vmem((8, 16, 512), BF),
        vmem((8, 16, 256), BF), vmem((8, 16, 256), BF), vmem((4, 32, 256), BF), vmem((4, 32, 256), BF),
        vmem((8, 128, 256), BF), vmem((8, 128, 256), BF), vmem((8, 128, 256), BF),
        vmem((4, 32, 256), BF), vmem((4, 32, 256), BF), vmem((8, 16, 256), BF), vmem((8, 16, 256), BF),
        vmem((8, 8, 256), F32), vmem((8, 8, 256), F32), vmem((128, 1024), F32), vmem((32, 256), BF),
        dma((21,)), dma((2,)),
        dma((8,)), dma((8,)), dma((8,)), dma((8,)), dma((8,)), dma((8,)), dma((8, 4)), dma((8, 4)),
        dma((8,)), dma((8,)), dma((8,)), dma((8,)), dma((4,)), dma((4,)), dma((8,)), dma((8,)),
        dma((8,)), dma((8,)), dma((4,)), dma((4,)), dma((8,)), dma((8,)), dma((8,)), dma((8,)),
        dma((4,)), dma((4,)), dma((8,)), dma((8,)), dma((8,)), dma((8,)),
    ]
    hbm = pl.BlockSpec(memory_space=pl.ANY)
    return pl.pallas_call(
        step_kernel,
        out_shape=(
            jax.ShapeDtypeStruct((32, 256), BF),
            jax.ShapeDtypeStruct((32, 1, 128, 128), F32),
        ),
        in_specs=[hbm] * 21,
        out_specs=(hbm, hbm),
        scratch_shapes=scratch,
        compiler_params=pltpu.CompilerParams(
            collective_id=0, has_side_effects=True, vmem_limit_bytes=60 * 1024 * 1024
        ),
    )(*args, inv)


def solution(mesh):
    in_specs = (
        P("ep", None), P(), P(None, "tp"), P(None, "tp"), P(None, "tp"), P(None, "tp"), P("tp"),
        P("tp", None), P("ep", "tp", None, None), P("ep"), P(), P(), P("tp", "ep"), P("tp", "ep"),
        P("ep", "tp"), P("ep", None), P("ep", None), P("ep", None, "tp"), P("ep", None, "tp"),
        P("ep", "tp", None),
    )
    out_specs = (P("ep", "tp"), P("ep", "tp", None, None))
    return jax.shard_map(per_device, mesh=mesh, in_specs=in_specs, out_specs=out_specs, check_vma=False)
```

```python
import numpy as np
import jax
import jax.numpy as jnp
from jax import lax
from jax.experimental import pallas as pl
from jax.experimental.pallas import tpu as pltpu
from jax.sharding import PartitionSpec as P

EPSILON = 1e-06
THETA = 10000.0
BF = jnp.bfloat16
F32 = jnp.float32
NZ, NX, NT, NE = 8, 4, 8, 32


def iota(shape, dim):
    return lax.broadcasted_iota(jnp.int32, shape, dim)


def onehot(condition):
    return jnp.where(condition, 1.0, 0.0).astype(BF)


def dot(a, b):
    return jnp.dot(a, b, preferred_element_type=F32)


def dot_nt(a, b):
    return lax.dot_general(a, b, (((1,), (1,)), ((), ())), preferred_element_type=F32)


def as_column(row, n):
    return jnp.sum(jnp.where(iota((n, n), 0) == iota((n, n), 1), row, 0.0), axis=1, keepdims=True)


def as_row(column, n):
    return jnp.sum(jnp.where(iota((n, n), 0) == iota((n, n), 1), column, 0.0), axis=0, keepdims=True)


def step_kernel(
    resid_h, norm_gain_h, wq_h, wk_h, wv_h, wg_h, head_gain_h, wo_h, state_h, positions_h,
    ffn_gain_h, w_mix_h, dgate_h, dup_h, ddown_h, routes_h, rweight_h, eg_h, eu_h, ed_h, inv_h,
    final_v, new_state,
    resid, norm_gain, wqkvg, head_gain, wo, state, positions, ffn_gain, w_mix,
    routes, rweight, eg, eu, ed, inv,
    mix, rs_send, rs_recv, p2_send, p2_recv, rows_x, dw, part_y, yx_recv, yz_send, yz_recv,
    md_send, md_recv, ag_recv, pair_send, pair_recv, er_own, er_send, er_recv, mr_send, mr_recv,
    d5_send, d5_recv, acc,
    load_sem,
    rs_s, rs_r, p2_s, p2_r, xz_s, xz_r, xx_s, xx_r, wy_s, wy_r, wc_s, wc_r, yx_s, yx_r, yz_s, yz_r,
    md_s, md_r, ag_s, ag_r, ac_s, pair_s, pair_r, er_s, er_r, mr_s, mr_r, d5_s, d5_r,
):
    ep = lax.axis_index("ep")
    t = lax.axis_index("tp")
    z = ep // NX
    x = lax.rem(ep, NX)
    y = t // 2
    core = lax.rem(t, 2)

    def zdev(p):
        return (p * NX + x, t)

    def xdev(p):
        return (z * NX + p, t)

    def tdev(p):
        return (ep, p)

    def ydev(p):
        return (ep, 2 * p + core)

    def edev(p):
        return (p, t)

    sibling = (ep, t + 1 - 2 * core)

    scope = []

    def phase(name):
        if scope:
            scope.pop().__exit__(None, None, None)
        if name:
            scope.append(jax.named_scope(name))
            scope[0].__enter__()

    phase("greet")
    barrier = pltpu.get_barrier_semaphore()
    for dev, me, n in ((edev, ep, NE), (tdev, t, NT)):
        def greet(k, c, dev=dev, me=me, n=n):
            pl.semaphore_signal(barrier, inc=1, device_id=dev(lax.rem(me + k, n)), device_id_type=pl.DeviceIdType.MESH)
            return c
        lax.fori_loop(1, n, greet, 0)

    loads = {}
    pairs = [
        ("resid", resid_h, resid), ("norm_gain", norm_gain_h, norm_gain),
        ("wq", wq_h, wqkvg.at[:, 0:128]), ("wk", wk_h, wqkvg.at[:, 128:256]),
        ("wv", wv_h, wqkvg.at[:, 256:384]), ("wg", wg_h, wqkvg.at[:, 384:512]),
        ("positions", positions_h, positions), ("inv", inv_h, inv), ("head_gain", head_gain_h, head_gain),
        ("state", state_h.at[:, 0], state), ("wo", wo_h, wo),
        ("ffn_gain", ffn_gain_h, ffn_gain), ("w_mix", w_mix_h, w_mix),
        ("routes", routes_h, routes), ("rweight", rweight_h, rweight),
        ("ddown", ddown_h, dw.at[t, 0:176]), ("dgate", dgate_h, dw.at[t, 176:352]),
        ("dup", dup_h, dw.at[t, 352:528]),
        ("eg", eg_h.at[0], eg), ("eu", eu_h.at[0], eu), ("ed", ed_h.at[0], ed),
    ]
    for n, (name, src, dst) in enumerate(pairs):
        loads[name] = pltpu.make_async_copy(src, dst, load_sem.at[n])
        loads[name].start()

    def need(*names):
        for name in names:
            loads[name].wait()

    def remote(src, dst, ssem, rsem, dev):
        return pltpu.make_async_remote_copy(
            src_ref=src, dst_ref=dst, send_sem=ssem, recv_sem=rsem, device_id=dev,
            device_id_type=pl.DeviceIdType.MESH,
        )

    def send_all(n, me, dev, src_at, dst_here, ssem, rsem):
        def one(k, c):
            p = lax.rem(me + k, n)
            remote(src_at(p), dst_here, ssem.at[p], rsem.at[me], dev(p)).start()
            return c
        lax.fori_loop(1, n, one, 0)

    def recv_all(n, me, dev, src, dst_at, ssem, rsem):
        def one(k, c):
            p = lax.rem(me + k, n)
            remote(src, dst_at(p), ssem.at[p], rsem.at[p], dev(p)).wait_recv()
            return c
        lax.fori_loop(1, n, one, 0)

    def sent_all(n, me, dev, src_at, dst, ssem, rsem):
        def one(k, c):
            p = lax.rem(me + k, n)
            remote(src_at(p), dst, ssem.at[p], rsem.at[me], dev(p)).wait_send()
            return c
        lax.fori_loop(1, n, one, 0)

    phase("retention")
    need("resid", "norm_gain")
    res = resid[...].astype(F32)
    ms = jnp.mean(res * res, axis=-1, keepdims=True)
    gain_in = norm_gain[...].reshape(1, 2048).astype(F32)
    normed_in = (res * lax.rsqrt(ms + EPSILON) * gain_in).astype(BF)
    need("positions", "inv", "wq", "wk", "wv", "wg")
    angles = as_column(positions[...].astype(F32).reshape(1, 32), 32) * inv[...]
    cosine, sine = jnp.cos(angles), jnp.sin(angles)
    cos2 = jnp.concatenate([cosine, cosine], axis=-1)
    sin2 = jnp.concatenate([-sine, sine], axis=-1)
    qkvg = dot(normed_in, wqkvg[...]).astype(BF).astype(F32)

    def rotate(v):
        return v * cos2 + pltpu.roll(v, 64, 1) * sin2

    query = rotate(qkvg[:, 0:128])
    key = rotate(qkvg[:, 128:256]) * (128 ** -0.5)
    value = qkvg[:, 256:384]
    gating = qkvg[:, 384:512]
    decay = 1.0 - jnp.exp2(-1.0 - 1.5 * jnp.full((1, 128), t, jnp.int32).astype(F32))
    within = jnp.sum(query * key, axis=-1, keepdims=True) * value
    query_t = jnp.transpose(query)
    phase("state")
    need("state")
    for s in range(32):
        mix[s : s + 1, :] = jnp.sum(state[s] * query_t[:, s : s + 1], axis=0, keepdims=True)
    phase("head_out")
    need("head_gain", "wo")
    mixture = within + mix[...] * decay
    centre = jnp.mean(mixture, axis=-1, keepdims=True)
    spread = jnp.mean(jnp.square(mixture - centre), axis=-1, keepdims=True)
    normed = (mixture - centre) * lax.rsqrt(spread + EPSILON)
    normed = normed * head_gain[...].reshape(1, 128).astype(F32)
    retained = (jax.nn.silu(gating) * normed).astype(BF)
    partial = dot(retained, wo[...]).astype(BF)
    for p in range(NT):
        rs_send[p] = partial[:, 256 * p : 256 * (p + 1)]

    phase("barrier")
    pl.semaphore_wait(barrier, NE + NT - 2)

    phase("rs_send")
    send_all(NT, t, tdev, lambda p: rs_send.at[p], rs_recv.at[t], rs_s, rs_r)
    rs_recv[t] = rs_send[t]

    need("ddown", "dgate", "dup")
    mine = dw.at[t, 0:528]
    remote(mine, mine, wc_s.at[y], wc_r.at[y], sibling).start()

    key_t = jnp.transpose(key)
    for s in range(32):
        new_state[s, 0] = state[s] * decay + key_t[:, s : s + 1] * value[s : s + 1, :]

    need("routes", "rweight", "ffn_gain", "w_mix")
    ids = jnp.transpose(routes[...].astype(F32))
    rw = jnp.transpose(rweight[...].astype(F32))
    lane_e = iota((32, 32), 1).astype(F32)
    hit0, hit1 = (lane_e == ids[:, 0:1]), (lane_e == ids[:, 1:2])
    both = jnp.where(hit0, 1.0, 0.0) + jnp.where(hit1, 1.0, 0.0)
    earlier = onehot(iota((32, 32), 1) < iota((32, 32), 0))
    rank = dot(earlier, both.astype(BF))
    weight_e = jnp.where(hit0, rw[:, 0:1], 0.0) + jnp.where(hit1, rw[:, 1:2], 0.0)
    lane = iota((32, 256), 1)
    widen = onehot((lane >> 3) == iota((32, 256), 0))
    slot = (lane & 3).astype(F32)
    taken = dot(both.astype(BF), widen) * jnp.where(dot(rank.astype(BF), widen) == slot, 1.0, 0.0)
    weighted = dot(weight_e.astype(BF), widen) * taken
    halves = [((lane >> 2) & 1) == h for h in range(2)]
    dispatch = [jnp.transpose(jnp.where(halves[h], taken, 0.0)).astype(BF) for h in range(2)]
    combine = [jnp.where(halves[h], weighted, 0.0).astype(BF) for h in range(2)]
    up_row, up_col = iota((128, 256), 0), iota((128, 256), 1)
    unpack = [onehot(up_col == (up_row >> 2) * 8 + 4 * h + (up_row & 3)) for h in range(2)]
    pk_row, pk_col = iota((256, 128), 0), iota((256, 128), 1)
    pack = [onehot(pk_row == (pk_col >> 2) * 8 + 4 * h + (pk_col & 3)) for h in range(2)]
    for p in range(NT):
        dw[p, 528:560, :] = jnp.zeros((32, 256), BF)

    phase("rs_wait")
    recv_all(NT, t, tdev, rs_send.at[0], lambda p: rs_recv.at[p], rs_s, rs_r)
    phase("middle")
    columns = pl.ds(pl.multiple_of(t * 256, 256), 256)
    attention = rs_recv[0].astype(F32)
    for p in range(1, NT):
        attention = attention + rs_recv[p].astype(F32)
    middle = resid[:, columns].astype(F32) + attention
    squares = as_row(jnp.sum(middle * middle, axis=-1, keepdims=True), 32)
    squares = jnp.concatenate([squares, jnp.zeros((1, 224), F32)], axis=1)

    for p in range(NT):
        p2_send[p, 0:4, :] = middle[4 * p : 4 * p + 4, :]
        p2_send[p, 4:5, :] = squares
    send_all(NT, t, tdev, lambda p: p2_send.at[p], p2_recv.at[t], p2_s, p2_r)
    p2_recv[t] = p2_send[t]
    ahead, behind = lax.rem(y + 1, 4), lax.rem(y + 3, 4)
    onward = lax.rem(y + 1 + 2 * core, 4)
    origin = lax.rem(y + 3 + 2 * core, 4)
    across = lax.rem(y + 2, 4)
    remote(mine, mine, wy_s.at[0], wy_r.at[y], ydev(ahead)).start()
    remote(mine, mine, wy_s.at[1], wy_r.at[y], ydev(behind)).start()
    phase("p2_wait")
    recv_all(NT, t, tdev, p2_send.at[0], lambda p: p2_recv.at[p], p2_s, p2_r)

    phase("norms")
    total = p2_recv[0, 4:5, 0:128]
    for p in range(1, NT):
        total = total + p2_recv[p, 4:5, 0:128]
    scale = lax.rsqrt(as_column(total[:, 0:32], 32) * (1.0 / 2048) + EPSILON)
    gain_mid = ffn_gain[...].reshape(1, 2048).astype(F32)
    gain_here = gain_mid[:, 0:256]
    for p in range(1, NT):
        gain_here = jnp.where(t == p, gain_mid[:, 256 * p : 256 * (p + 1)], gain_here)
    normed_mid = (middle * scale * gain_here).astype(BF)

    outgoing = dot(dispatch[0], normed_mid[:, 0:128]) + dot(dispatch[1], normed_mid[:, 128:256])
    md_send[...] = outgoing.astype(BF).reshape(NE, 8, 128)
    far = 16

    def spread_out(src_at, dst_here, ssem, rsem):
        def one(k, c):
            p = lax.rem(ep + lax.rem(k + far, NE - 1) + 1, NE)
            remote(src_at(p), dst_here, ssem.at[p], rsem.at[ep], edev(p)).start()
            return c
        lax.fori_loop(0, NE - 1, one, 0)

    spread_out(lambda p: md_send.at[p], md_recv.at[ep], md_s, md_r)
    md_recv[ep] = md_send[ep]

    quarters = [
        jnp.concatenate([p2_recv[2 * q, 0:4, :], p2_recv[2 * q + 1, 0:4, :]], axis=1) for q in range(4)
    ]
    sq4 = sum(jnp.sum(v * v, axis=-1, keepdims=True) for v in quarters)
    scale4 = lax.rsqrt(sq4 * (1.0 / 2048) + EPSILON)
    mixer = w_mix[...].reshape(1, 2048).astype(F32)
    rows = [
        (quarters[q] * scale4 * gain_mid[:, 512 * q : 512 * (q + 1)]).astype(BF).astype(F32) for q in range(4)
    ]
    mixing = jax.nn.sigmoid(
        sum(jnp.sum(rows[q] * mixer[:, 512 * q : 512 * (q + 1)], axis=-1, keepdims=True) for q in range(4))
    )
    mixing16 = jnp.concatenate([mixing] * 4, axis=0)
    rows_x[x, z] = jnp.concatenate(rows, axis=0).astype(BF)
    send_all(NZ, z, zdev, lambda p: rows_x.at[x, z], rows_x.at[x, z], xz_s, xz_r)

    def to_x(zz):
        send_all(NX, x, xdev, lambda p: rows_x.at[x, zz], rows_x.at[x, zz], xx_s.at[zz], xx_r.at[zz])

    to_x(z)

    phase("relay")

    def weights_of(p):
        return dw.at[2 * p + core, 0:528]

    def from_y(p, slot):
        return remote(weights_of(p), weights_of(p), wy_s.at[slot], wy_r.at[p], ydev(p))

    def to_sibling(p):
        return remote(weights_of(p), weights_of(p), wc_s.at[p], wc_r.at[p], sibling)

    relayed = remote(weights_of(origin), weights_of(origin), wy_s.at[2], wy_r.at[origin], ydev(onward))
    from_y(origin, 2).wait_recv()
    relayed.start()
    to_sibling(origin).start()
    from_y(onward, 2).wait_recv()
    to_sibling(onward).start()

    phase("md_wait")
    recv_all(NE, ep, edev, md_send.at[0], lambda p: md_recv.at[p], md_s, md_r)
    arrived = md_recv[...].reshape(256, 128)
    ag_recv[t] = jnp.concatenate([dot(unpack[h], arrived) for h in range(2)], axis=1).astype(BF)
    own_rows = ag_recv.at[t]

    def group_send(k, c):
        p = lax.rem(y + 4 - k, 4)
        remote(own_rows, own_rows, ag_s.at[p], ag_r.at[t], ydev(p)).start()
        return c
    lax.fori_loop(1, 4, group_send, 0)
    remote(own_rows, own_rows, ac_s.at[y], ag_r.at[t], sibling).start()

    phase("xz_wait")
    def pass_on(k, c):
        p = lax.rem(z + k, NZ)
        remote(rows_x.at[x, p], rows_x.at[x, p], xz_s.at[p], xz_r.at[p], zdev(p)).wait_recv()
        to_x(p)
        return c
    lax.fori_loop(1, NZ, pass_on, 0)

    phase("weights_wait")
    from_y(across, 2).wait_recv()
    to_sibling(across).start()

    def all_weights(k, c):
        theirs = dw.at[2 * k + 1 - core, 0:528]
        remote(theirs, theirs, wc_s.at[k], wc_r.at[k], sibling).wait_recv()
        return c
    lax.fori_loop(0, 4, all_weights, 0)

    def rows_in(zz, c):
        recv_all(NX, x, xdev, rows_x.at[x, zz], lambda p: rows_x.at[p, zz], xx_s.at[zz], xx_r.at[zz])
        return c

    phase("xx_wait")
    lax.fori_loop(0, NZ, rows_in, 0)

    phase("dense_mm")
    tiles = rows_x[...].reshape(512, 512)
    spread_row = iota((128, 512), 0)
    spread_col = iota((128, 512), 1)
    gate_up = jnp.zeros((128, 384), F32)
    for q in range(4):
        take = onehot(spread_col == (spread_row >> 2) * 16 + 4 * q + (spread_row & 3))
        block = dot(take, tiles).astype(BF)
        gate_up = gate_up + dot_nt(block[:, 0:256], dw[2 * q, 176:560])
        gate_up = gate_up + dot_nt(block[:, 256:512], dw[2 * q + 1, 176:560])
    up = pltpu.roll(gate_up, 384 - 176, 1)
    hidden = jnp.where(iota((128, 256), 1) < 176, jax.nn.silu(gate_up[:, 0:256]) * up[:, 0:256], 0.0).astype(BF)
    back_row = iota((512, 128), 0)
    back_col = iota((512, 128), 1)
    packed = jnp.zeros((512, 512), F32)
    for q in range(4):
        block = jnp.concatenate([dot(hidden, dw[2 * q, 0:256]), dot(hidden, dw[2 * q + 1, 0:256])], axis=1).astype(BF)
        put = onehot(back_row == (back_col >> 2) * 16 + 4 * q + (back_col & 3))
        packed = packed + dot(put, block)
    part_y[...] = packed.astype(BF).reshape(NX, 128, 512)
    send_all(NX, x, xdev, lambda p: part_y.at[p], yx_recv.at[x], yx_s, yx_r)
    yx_recv[x] = part_y[x]

    phase("ag_gate_up")
    need("eg", "eu", "ed")

    def chunk(p):
        depth = pl.ds(pl.multiple_of(p * 256, 256), 256)
        rows_p = ag_recv[p]
        acc[:, 0:512] += dot(rows_p, eg[depth, :])
        acc[:, 512:1024] += dot(rows_p, eu[depth, :])

    acc[...] = jnp.zeros_like(acc)

    def two_chunks(k, c):
        p = lax.rem(y + k + k // 2, 4)
        p = jnp.where(k == 3, across, p)
        direct, other = 2 * p + core, 2 * p + 1 - core

        @pl.when(k > 0)
        def _():
            remote(ag_recv.at[direct], ag_recv.at[direct], ag_s.at[p], ag_r.at[direct], ydev(p)).wait_recv()
            remote(ag_recv.at[direct], ag_recv.at[direct], ac_s.at[p], ag_r.at[direct], sibling).start()
        chunk(direct)
        remote(ag_recv.at[other], ag_recv.at[other], ac_s.at[p], ag_r.at[other], sibling).wait_recv()
        chunk(other)
        return c
    lax.fori_loop(0, 4, two_chunks, 0)
    phase("down")
    hidden_e = (jax.nn.silu(acc[:, 0:512]) * acc[:, 512:1024]).astype(BF)

    def down_tile(p):
        return dot(hidden_e, ed[:, pl.ds(pl.multiple_of(p * 256, 256), 256)])

    def for_sibling(k, c):
        p = lax.rem(y + 2 + k, 4)
        pair_send[p] = down_tile(2 * p + 1 - core).astype(BF)
        remote(pair_send.at[p], pair_recv.at[p], pair_s.at[p], pair_r.at[p], sibling).start()
        return c
    lax.fori_loop(0, 4, for_sibling, 0)

    def for_own(k, c):
        p = lax.rem(y + 2 + k, 4)
        er_own[p] = down_tile(2 * p + core)
        return c
    lax.fori_loop(0, 4, for_own, 0)

    def pair_sum(p):
        remote(pair_send.at[p], pair_recv.at[p], pair_s.at[p], pair_r.at[p], sibling).wait_recv()
        return er_own[p] + pair_recv[p].astype(F32)

    def to_chips(k, c):
        p = lax.rem(y + 1 + lax.rem(k + 1, 3), 4)
        er_send[p] = pair_sum(p).astype(BF)
        remote(er_send.at[p], er_recv.at[y], er_s.at[p], er_r.at[y], ydev(p)).start()
        return c
    lax.fori_loop(0, 3, to_chips, 0)
    er_own[y] = pair_sum(y)

    phase("yx_wait")
    recv_all(NX, x, xdev, part_y.at[0], lambda p: yx_recv.at[p], yx_s, yx_r)
    summed = yx_recv[0].astype(F32)
    for p in range(1, NX):
        summed = summed + yx_recv[p].astype(F32)
    yz_send[...] = summed.astype(BF).reshape(NZ, 16, 512)
    send_all(NZ, z, zdev, lambda p: yz_send.at[p], yz_recv.at[z], yz_s, yz_r)
    yz_recv[z] = yz_send[z]

    phase("er_wait")
    recv_all(4, y, ydev, er_send.at[0], lambda p: er_recv.at[p], er_s, er_r)
    result = er_own[y]
    for k in range(1, 4):
        result = result + er_recv[lax.rem(y + k, 4)].astype(F32)
    result = result.astype(BF)
    mr_send[...] = (dot(pack[0], result[:, 0:128]) + dot(pack[1], result[:, 128:256])).astype(BF).reshape(NE, 8, 128)
    spread_out(lambda p: mr_send.at[p], mr_recv.at[ep], mr_s, mr_r)
    mr_recv[ep] = mr_send[ep]

    recv_all(NZ, z, zdev, yz_send.at[0], lambda p: yz_recv.at[p], yz_s, yz_r)
    dense = yz_recv[0].astype(F32)
    for p in range(1, NZ):
        dense = dense + yz_recv[p].astype(F32)
    dense = dense * mixing16
    for p in range(NT):
        q, half = p // 2, p % 2
        d5_send[p, 0:4, :] = dense[4 * q : 4 * q + 4, 256 * half : 256 * (half + 1)]
        d5_send[p, 4:8, :] = jnp.zeros((4, 256), F32)
    send_all(NT, t, tdev, lambda p: d5_send.at[p], d5_recv.at[t], d5_s, d5_r)
    d5_recv[t] = d5_send[t]

    phase("d5_wait")
    recv_all(NT, t, tdev, d5_send.at[0], lambda p: d5_recv.at[p], d5_s, d5_r)
    dense_rows = jnp.concatenate([d5_recv[p, 0:4, :] for p in range(NT)], axis=0)
    phase("mr_wait")
    recv_all(NE, ep, edev, mr_send.at[0], lambda p: mr_recv.at[p], mr_s, mr_r)
    returned = mr_recv[...].reshape(256, 128)
    phase("final")
    moe = jnp.concatenate([dot(combine[h], returned) for h in range(2)], axis=1)
    final_v[...] = (middle + moe + dense_rows).astype(BF)

    phase("drain")
    sent_all(NT, t, tdev, lambda p: rs_send.at[p], rs_recv.at[t], rs_s, rs_r)
    sent_all(NT, t, tdev, lambda p: p2_send.at[p], p2_recv.at[t], p2_s, p2_r)
    sent_all(NE, ep, edev, lambda p: md_send.at[p], md_recv.at[ep], md_s, md_r)
    sent_all(NZ, z, zdev, lambda p: rows_x.at[x, z], rows_x.at[x, z], xz_s, xz_r)

    def x_sent(zz, c):
        sent_all(NX, x, xdev, lambda p: rows_x.at[x, zz], rows_x.at[x, zz], xx_s.at[zz], xx_r.at[zz])
        return c
    lax.fori_loop(0, NZ, x_sent, 0)
    from_y(ahead, 0).wait_send()
    from_y(behind, 1).wait_send()
    relayed.wait_send()

    def core_sent(k, c):
        to_sibling(k).wait_send()
        tt = 2 * k + core
        remote(ag_recv.at[tt], ag_recv.at[tt], ac_s.at[k], ag_r.at[tt], sibling).wait_send()
        remote(pair_send.at[k], pair_recv.at[k], pair_s.at[k], pair_r.at[k], sibling).wait_send()
        return c
    lax.fori_loop(0, 4, core_sent, 0)
    sent_all(4, y, ydev, lambda p: own_rows, own_rows, ag_s, ag_r)
    sent_all(NX, x, xdev, lambda p: part_y.at[p], yx_recv.at[x], yx_s, yx_r)
    sent_all(4, y, ydev, lambda p: er_send.at[p], er_recv.at[y], er_s, er_r)
    sent_all(NZ, z, zdev, lambda p: yz_send.at[p], yz_recv.at[z], yz_s, yz_r)
    sent_all(NT, t, tdev, lambda p: d5_send.at[p], d5_recv.at[t], d5_s, d5_r)
    sent_all(NE, ep, edev, lambda p: mr_send.at[p], mr_recv.at[ep], mr_s, mr_r)
    phase(None)


def per_device(*args):
    args = list(args)
    for n in (12, 13, 15, 16):
        args[n] = args[n].T
    inv = jnp.asarray((THETA ** (-np.arange(64) / 64.0)).astype(np.float32)[None, :])
    vmem = pltpu.VMEM

    def dma(*shape):
        return pltpu.SemaphoreType.DMA(shape)

    scratch = [
        vmem((32, 2048), BF), vmem((2048,), BF), vmem((2048, 512), BF), vmem((128,), BF),
        vmem((128, 2048), BF), vmem((32, 128, 128), F32), vmem((32,), jnp.int32), vmem((2048,), BF),
        vmem((2048,), BF), vmem((2, 32), jnp.int32), vmem((2, 32), BF),
        vmem((2048, 512), BF), vmem((2048, 512), BF), vmem((512, 2048), BF), vmem((1, 64), F32),
        vmem((32, 128), F32), vmem((8, 32, 256), BF), vmem((8, 32, 256), BF),
        vmem((8, 8, 256), F32), vmem((8, 8, 256), F32), vmem((4, 8, 16, 512), BF),
        vmem((8, 560, 256), BF), vmem((4, 128, 512), BF), vmem((4, 128, 512), BF),
        vmem((8, 16, 512), BF), vmem((8, 16, 512), BF),
        vmem((32, 8, 128), BF), vmem((32, 8, 128), BF), vmem((8, 128, 256), BF),
        vmem((4, 128, 256), BF), vmem((4, 128, 256), BF), vmem((4, 128, 256), F32),
        vmem((4, 128, 256), BF), vmem((4, 128, 256), BF), vmem((32, 8, 128), BF), vmem((32, 8, 128), BF),
        vmem((8, 8, 256), F32), vmem((8, 8, 256), F32), vmem((128, 1024), F32),
        dma(21),
        dma(8), dma(8), dma(8), dma(8), dma(8), dma(8), dma(8, 4), dma(8, 4), dma(3), dma(4), dma(4), dma(4),
        dma(4), dma(4), dma(8), dma(8),
        dma(32), dma(32), dma(4), dma(8), dma(4), dma(4), dma(4), dma(4), dma(4), dma(32), dma(32), dma(8), dma(8),
    ]
    hbm = pl.BlockSpec(memory_space=pltpu.HBM)
    out = pl.BlockSpec(memory_space=pltpu.VMEM)
    return pl.pallas_call(
        step_kernel,
        out_shape=(
            jax.ShapeDtypeStruct((32, 256), BF),
            jax.ShapeDtypeStruct((32, 1, 128, 128), F32),
        ),
        in_specs=[hbm] * 21,
        out_specs=(out, out),
        scratch_shapes=scratch,
        compiler_params=pltpu.CompilerParams(
            collective_id=0, has_side_effects=True, vmem_limit_bytes=63200 * 1024
        ),
    )(*args, inv)


def solution(mesh):
    in_specs = (
        P("ep", None), P(), P(None, "tp"), P(None, "tp"), P(None, "tp"), P(None, "tp"), P("tp"),
        P("tp", None), P("ep", "tp", None, None), P("ep"), P(), P(), P("tp", "ep"), P("tp", "ep"),
        P("ep", "tp"), P("ep", None), P("ep", None), P("ep", None, "tp"), P("ep", None, "tp"),
        P("ep", "tp", None),
    )
    out_specs = (P("ep", "tp"), P("ep", "tp", None, None))
    return jax.shard_map(per_device, mesh=mesh, in_specs=in_specs, out_specs=out_specs, check_vma=False)
```

```python
import numpy as np
import jax
import jax.numpy as jnp
from jax import lax
from jax.experimental import pallas as pl
from jax.experimental.pallas import tpu as pltpu
from jax.sharding import PartitionSpec as P

EPSILON = 1e-06
THETA = 10000.0
BF = jnp.bfloat16
F32 = jnp.float32
NZ, NX, NT, NE = 8, 4, 8, 32


def iota(shape, dim):
    return lax.broadcasted_iota(jnp.int32, shape, dim)


def onehot(condition):
    return jnp.where(condition, 1.0, 0.0).astype(BF)


def dot(a, b):
    return jnp.dot(a, b, preferred_element_type=F32)


def dot_nt(a, b):
    return lax.dot_general(a, b, (((1,), (1,)), ((), ())), preferred_element_type=F32)


def as_column(row, n):
    return jnp.sum(jnp.where(iota((n, n), 0) == iota((n, n), 1), row, 0.0), axis=1, keepdims=True)


def as_row(column, n):
    return jnp.sum(jnp.where(iota((n, n), 0) == iota((n, n), 1), column, 0.0), axis=0, keepdims=True)


def step_kernel(
    resid_h, norm_gain_h, wq_h, wk_h, wv_h, wg_h, head_gain_h, wo_h, state_h, positions_h,
    ffn_gain_h, w_mix_h, dgate_h, dup_h, ddown_h, routes_h, rweight_h, eg_h, eu_h, ed_h, inv_h,
    final_h, new_state_h,
    resid, norm_gain, wqkvg, head_gain, wo, state, positions, ffn_gain, w_mix,
    routes, rweight, eg, eu, ed, inv,
    mix, rs_send, rs_recv, rr_send, rr_recv, sc_send, sc_recv, sx_send, sx_recv, rows_x, dw,
    part_y, ry_recv, my_send, yx_recv, yz_send, yz_recv, md_send, md_recv, ag_recv, pair_send, pair_recv, er_own, er_send, er_recv, mr_send, mr_recv,
    d5_send, d5_recv, acc, final_v,
    load_sem, out_sem,
    rs_s, rs_r, rr_s, rr_r, sc_s, sc_r, sx_s, sx_r, xz_s, xz_r, xx_s, xx_r, wy_s, wy_r, wc_s, wc_r,
    ry_s, ry_r, yx_s, yx_r, yz_s, yz_r,
    md_s, md_r, ag_s, ag_r, ac_s, pair_s, pair_r, er_s, er_r, mr_s, mr_r, d5_s, d5_r,
):
    ep = lax.axis_index("ep")
    t = lax.axis_index("tp")
    z = ep // NX
    x = lax.rem(ep, NX)
    y = t // 2
    core = lax.rem(t, 2)

    def zdev(p):
        return (p * NX + x, t)

    def xdev(p):
        return (z * NX + p, t)

    def tdev(p):
        return (ep, p)

    def ydev(p):
        return (ep, 2 * p + core)

    def edev(p):
        return (p, t)

    sibling = (ep, t + 1 - 2 * core)

    scope = []

    def phase(name):
        if scope:
            scope.pop().__exit__(None, None, None)
        if name:
            scope.append(jax.named_scope(name))
            scope[0].__enter__()

    loads = {}
    pairs = [
        ("resid", resid_h, resid), ("norm_gain", norm_gain_h, norm_gain),
        ("wq", wq_h, wqkvg.at[:, 0:128]), ("wk", wk_h, wqkvg.at[:, 128:256]),
        ("wv", wv_h, wqkvg.at[:, 256:384]), ("wg", wg_h, wqkvg.at[:, 384:512]),
        ("positions", positions_h, positions), ("inv", inv_h, inv), ("head_gain", head_gain_h, head_gain),
        ("state", state_h.at[:, 0], state), ("wo", wo_h, wo),
        ("ffn_gain", ffn_gain_h, ffn_gain), ("w_mix", w_mix_h, w_mix),
        ("routes", routes_h, routes), ("rweight", rweight_h, rweight),
        ("ddown", ddown_h, dw.at[t, 0:176]), ("dgate", dgate_h, dw.at[t, 176:352]),
        ("dup", dup_h, dw.at[t, 352:528]),
        ("eg", eg_h.at[0], eg), ("eu", eu_h.at[0], eu), ("ed", ed_h.at[0], ed),
    ]
    for n, (name, src, dst) in enumerate(pairs):
        loads[name] = pltpu.make_async_copy(src, dst, load_sem.at[n])
        loads[name].start()

    phase("greet")
    barrier = pltpu.get_barrier_semaphore()
    for dev, me, n in ((edev, ep, NE), (tdev, t, NT)):
        def greet(k, c, dev=dev, me=me, n=n):
            p = lax.rem(me + lax.rem(k + n // 2, n - 1) + 1, n)
            pl.semaphore_signal(barrier, inc=1, device_id=dev(p), device_id_type=pl.DeviceIdType.MESH)
            return c
        lax.fori_loop(0, n - 1, greet, 0)

    def need(*names):
        for name in names:
            loads[name].wait()

    def remote(src, dst, ssem, rsem, dev):
        return pltpu.make_async_remote_copy(
            src_ref=src, dst_ref=dst, send_sem=ssem, recv_sem=rsem, device_id=dev,
            device_id_type=pl.DeviceIdType.MESH,
        )

    def send_all(n, me, dev, src_at, dst_here, ssem, rsem):
        def one(k, c):
            p = lax.rem(me + k, n)
            remote(src_at(p), dst_here, ssem.at[p], rsem.at[me], dev(p)).start()
            return c
        lax.fori_loop(1, n, one, 0)

    def recv_all(n, me, dev, src, dst_at, ssem, rsem):
        def one(k, c):
            p = lax.rem(me + k, n)
            remote(src, dst_at(p), ssem.at[p], rsem.at[p], dev(p)).wait_recv()
            return c
        lax.fori_loop(1, n, one, 0)

    def sent_all(n, me, dev, src_at, dst, ssem, rsem):
        def one(k, c):
            p = lax.rem(me + k, n)
            remote(src_at(p), dst, ssem.at[p], rsem.at[me], dev(p)).wait_send()
            return c
        lax.fori_loop(1, n, one, 0)

    phase("retention")
    need("resid", "norm_gain")
    res = resid[...].astype(F32)
    ms = jnp.mean(res * res, axis=-1, keepdims=True)
    gain_in = norm_gain[...].reshape(1, 2048).astype(F32)
    normed_in = (res * lax.rsqrt(ms + EPSILON) * gain_in).astype(BF)
    need("positions", "inv", "wq", "wk", "wv", "wg")
    angles = as_column(positions[...].astype(F32).reshape(1, 32), 32) * inv[...]
    cosine, sine = jnp.cos(angles), jnp.sin(angles)
    cos2 = jnp.concatenate([cosine, cosine], axis=-1)
    sin2 = jnp.concatenate([-sine, sine], axis=-1)
    qkvg = dot(normed_in, wqkvg[...]).astype(BF).astype(F32)

    def rotate(v):
        return v * cos2 + pltpu.roll(v, 64, 1) * sin2

    query = rotate(qkvg[:, 0:128])
    key = rotate(qkvg[:, 128:256]) * (128 ** -0.5)
    value = qkvg[:, 256:384]
    gating = qkvg[:, 384:512]
    decay = 1.0 - jnp.exp2(-1.0 - 1.5 * jnp.full((1, 128), t, jnp.int32).astype(F32))
    within = jnp.sum(query * key, axis=-1, keepdims=True) * value
    query_t = jnp.transpose(query)
    phase("state")
    need("state")
    for s in range(32):
        mix[s : s + 1, :] = jnp.sum(state[s] * query_t[:, s : s + 1], axis=0, keepdims=True)
    phase("head_out")
    need("head_gain", "wo")
    mixture = within + mix[...] * decay
    centre = jnp.mean(mixture, axis=-1, keepdims=True)
    spread = jnp.mean(jnp.square(mixture - centre), axis=-1, keepdims=True)
    normed = (mixture - centre) * lax.rsqrt(spread + EPSILON)
    normed = normed * head_gain[...].reshape(1, 128).astype(F32)
    retained = (jax.nn.silu(gating) * normed).astype(BF)
    partial = dot(retained, wo[...])
    for p in range(NT):
        rs_send[p] = partial[:, 256 * p : 256 * (p + 1)].astype(BF)
    for p in range(NT):
        tile = [partial[4 * p : 4 * p + 4, 512 * q : 512 * (q + 1)] for q in range(4)]
        rr_send[p] = jnp.concatenate(tile, axis=0).astype(BF)

    phase("barrier")
    pl.semaphore_wait(barrier, NE + NT - 2)

    phase("rs_send")
    send_all(NT, t, tdev, lambda p: rs_send.at[p], rs_recv.at[t], rs_s, rs_r)
    send_all(NT, t, tdev, lambda p: rr_send.at[p], rr_recv.at[t], rr_s, rr_r)
    rs_recv[t] = rs_send[t]
    rr_recv[t] = rr_send[t]

    need("ddown", "dgate", "dup")
    ahead, behind = lax.rem(y + 1, 4), lax.rem(y + 3, 4)
    onward = lax.rem(y + 1 + 2 * core, 4)
    origin = lax.rem(y + 3 + 2 * core, 4)
    across = lax.rem(y + 2, 4)
    parts = (pl.ds(272, 256), pl.ds(0, 272))

    def weights_to_y(h, owner, slot, target):
        block = dw.at[2 * owner + core, parts[h]]
        return remote(block, block, wy_s.at[h, slot], wy_r.at[h, owner], ydev(target))

    def weights_to_sibling(h, owner):
        block = dw.at[2 * owner + core, parts[h]]
        return remote(block, block, wc_s.at[h, owner], wc_r.at[h, owner], sibling)

    weights_to_y(0, y, 0, ahead).start()
    weights_to_y(0, y, 1, behind).start()
    for h in range(2):
        weights_to_sibling(h, y).start()

    key_t = jnp.transpose(key)
    for s in range(32):
        state[s] = state[s] * decay + key_t[:, s : s + 1] * value[s : s + 1, :]

    need("routes", "rweight", "ffn_gain", "w_mix")
    ids = jnp.transpose(routes[...].astype(F32))
    rw = jnp.transpose(rweight[...].astype(F32))
    lane_e = iota((32, 32), 1).astype(F32)
    hit0, hit1 = (lane_e == ids[:, 0:1]), (lane_e == ids[:, 1:2])
    both = jnp.where(hit0, 1.0, 0.0) + jnp.where(hit1, 1.0, 0.0)
    earlier = onehot(iota((32, 32), 1) < iota((32, 32), 0))
    rank = dot(earlier, both.astype(BF))
    weight_e = jnp.where(hit0, rw[:, 0:1], 0.0) + jnp.where(hit1, rw[:, 1:2], 0.0)
    lane = iota((32, 256), 1)
    widen = onehot((lane >> 3) == iota((32, 256), 0))
    slot = (lane & 3).astype(F32)
    taken = dot(both.astype(BF), widen) * jnp.where(dot(rank.astype(BF), widen) == slot, 1.0, 0.0)
    weighted = dot(weight_e.astype(BF), widen) * taken
    halves = [((lane >> 2) & 1) == h for h in range(2)]
    dispatch = [jnp.transpose(jnp.where(halves[h], taken, 0.0)).astype(BF) for h in range(2)]
    combine = [jnp.where(halves[h], weighted, 0.0).astype(BF) for h in range(2)]
    up_row, up_col = iota((128, 256), 0), iota((128, 256), 1)
    unpack = [onehot(up_col == (up_row >> 2) * 8 + 4 * h + (up_row & 3)) for h in range(2)]
    pk_row, pk_col = iota((256, 128), 0), iota((256, 128), 1)
    pack = [onehot(pk_row == (pk_col >> 2) * 8 + 4 * h + (pk_col & 3)) for h in range(2)]
    for p in range(NT):
        dw[p, 528:560, :] = jnp.zeros((32, 256), BF)
    gain_mid = ffn_gain[...].reshape(1, 2048).astype(F32)
    gain_here = gain_mid[:, 0:256]
    for p in range(1, NT):
        gain_here = jnp.where(t == p, gain_mid[:, 256 * p : 256 * (p + 1)], gain_here)
    mixer = w_mix[...].reshape(1, 2048).astype(F32)

    def as_tile(row):
        return jnp.concatenate(
            [jnp.broadcast_to(row[:, 512 * q : 512 * (q + 1)], (4, 512)) for q in range(4)], axis=0
        )

    gain_tile, mixer_tile = as_tile(gain_mid), as_tile(mixer)
    pick_row, pick_col = iota((16, 32), 0), iota((16, 32), 1)
    resid_tile = jnp.zeros((16, 512), F32)
    for q in range(4):
        pick = onehot((pick_col == 4 * t + (pick_row & 3)) & ((pick_row >> 2) == q))
        resid_tile = resid_tile + dot(pick, resid[:, 512 * q : 512 * (q + 1)])
    new_state_copy = pltpu.make_async_copy(state, new_state_h.at[:, 0], out_sem.at[0])
    new_state_copy.start()

    phase("rs_wait")
    recv_all(NT, t, tdev, rs_send.at[0], lambda p: rs_recv.at[p], rs_s, rs_r)
    phase("middle")
    columns = pl.ds(pl.multiple_of(t * 256, 256), 256)
    attention = rs_recv[0].astype(F32)
    for p in range(1, NT):
        attention = attention + rs_recv[p].astype(F32)
    middle = resid[:, columns].astype(F32) + attention
    scaled = (middle * gain_here).astype(BF)
    outgoing = dot(dispatch[0], scaled[:, 0:128]) + dot(dispatch[1], scaled[:, 128:256])
    md_send[...] = outgoing.astype(BF).reshape(NE, 8, 128)
    far = 16

    def spread_out(src_at, dst_here, ssem, rsem):
        def one(k, c):
            p = lax.rem(ep + lax.rem(k + far, NE - 1) + 1, NE)
            remote(src_at(p), dst_here, ssem.at[p], rsem.at[ep], edev(p)).start()
            return c
        lax.fori_loop(0, NE - 1, one, 0)

    spread_out(lambda p: md_send.at[p], md_recv.at[ep], md_s, md_r)
    md_recv[ep] = md_send[ep]

    phase("rr_wait")
    recv_all(NT, t, tdev, rr_send.at[0], lambda p: rr_recv.at[p], rr_s, rr_r)
    middle_tile = rr_recv[0].astype(F32)
    for p in range(1, NT):
        middle_tile = middle_tile + rr_recv[p].astype(F32)
    middle_tile = middle_tile + resid_tile

    def over_quarters(column):
        total = column[0:4] + column[4:8] + column[8:12] + column[12:16]
        return jnp.concatenate([total] * 4, axis=0)

    squares = over_quarters(jnp.sum(middle_tile * middle_tile, axis=-1, keepdims=True))
    scale_tile = lax.rsqrt(squares * (1.0 / 2048) + EPSILON)
    normed_tile = (middle_tile * scale_tile * gain_tile).astype(BF)
    mixing16 = jax.nn.sigmoid(
        over_quarters(jnp.sum(normed_tile.astype(F32) * mixer_tile, axis=-1, keepdims=True))
    )
    rows_x[x, z] = normed_tile
    send_all(NZ, z, zdev, lambda p: rows_x.at[x, z], rows_x.at[x, z], xz_s, xz_r)

    def to_x(zz):
        send_all(NX, x, xdev, lambda p: rows_x.at[x, zz], rows_x.at[x, zz], xx_s.at[zz], xx_r.at[zz])

    to_x(z)

    lane16 = iota((16, 128), 1)
    sc_send[...] = jnp.sum(jnp.where(lane16 == iota((16, 128), 0), scale_tile, 0.0)[0:4], axis=0, keepdims=True)
    send_all(NT, t, tdev, lambda p: sc_send, sc_recv.at[t], sc_s, sc_r)
    sc_recv[t] = sc_send[...]
    weights_to_y(1, y, 0, ahead).start()
    weights_to_y(1, y, 1, behind).start()

    def relay(h):
        weights_to_y(h, origin, 2, onward).wait_recv()
        weights_to_y(h, origin, 2, onward).start()
        weights_to_sibling(h, origin).start()

    phase("relay_a")
    relay(0)

    phase("md_wait")
    recv_all(NE, ep, edev, md_send.at[0], lambda p: md_recv.at[p], md_s, md_r)
    arrived = md_recv[...].reshape(256, 128)
    ag_recv[t] = jnp.concatenate([dot(unpack[h], arrived) for h in range(2)], axis=1).astype(BF)
    own_rows = ag_recv.at[t]

    def group_send(k, c):
        p = lax.rem(y + 4 - k, 4)
        remote(own_rows, own_rows, ag_s.at[p], ag_r.at[t], ydev(p)).start()
        return c
    lax.fori_loop(1, 4, group_send, 0)
    remote(own_rows, own_rows, ac_s.at[y], ag_r.at[t], sibling).start()

    phase("xz_wait")
    def pass_on(k, c):
        p = lax.rem(z + k, NZ)
        remote(rows_x.at[x, p], rows_x.at[x, p], xz_s.at[p], xz_r.at[p], zdev(p)).wait_recv()
        to_x(p)
        return c
    lax.fori_loop(1, NZ, pass_on, 0)

    phase("relay_b")
    relay(1)

    phase("sc_wait")
    recv_all(NT, t, tdev, sc_send, lambda p: sc_recv.at[p], sc_s, sc_r)
    factors = jnp.concatenate([jnp.broadcast_to(sc_recv[p], (4, 128)) for p in range(NT)], axis=0)
    factors = jnp.sum(
        jnp.where(iota((32, 128), 1) == (iota((32, 128), 0) & 3), factors, 0.0), axis=1, keepdims=True
    )
    sx_send[...] = jnp.sum(taken * factors, axis=0, keepdims=True)
    spread_out(lambda p: sx_send, sx_recv.at[ep], sx_s, sx_r)
    sx_recv[ep] = sx_send[...]

    phase("weights_wait")
    for h in range(2):
        weights_to_y(h, onward, 2, onward).wait_recv()
        weights_to_sibling(h, onward).start()
    for h in range(2):
        weights_to_y(h, across, 2, onward).wait_recv()
        weights_to_sibling(h, across).start()

    def all_weights(k, c):
        for h in range(2):
            theirs = dw.at[2 * k + 1 - core, parts[h]]
            remote(theirs, theirs, wc_s.at[h, k], wc_r.at[h, k], sibling).wait_recv()
        return c
    lax.fori_loop(0, 4, all_weights, 0)

    def rows_in(zz, c):
        recv_all(NX, x, xdev, rows_x.at[x, zz], lambda p: rows_x.at[p, zz], xx_s.at[zz], xx_r.at[zz])
        return c

    phase("xx_wait")
    lax.fori_loop(0, NZ, rows_in, 0)

    phase("dense_mm")
    tiles = rows_x[...].reshape(512, 512)
    spread_row = iota((128, 512), 0)
    spread_col = iota((128, 512), 1)
    gate_up = jnp.zeros((128, 384), F32)
    for q in range(4):
        take = onehot(spread_col == (spread_row >> 2) * 16 + 4 * q + (spread_row & 3))
        block = dot(take, tiles).astype(BF)
        gate_up = gate_up + dot_nt(block[:, 0:256], dw[2 * q, 176:560])
        gate_up = gate_up + dot_nt(block[:, 256:512], dw[2 * q + 1, 176:560])
    up = pltpu.roll(gate_up, 384 - 176, 1)
    hidden = jnp.where(iota((128, 256), 1) < 176, jax.nn.silu(gate_up[:, 0:256]) * up[:, 0:256], 0.0).astype(BF)
    back_row = iota((512, 128), 0)
    back_col = iota((512, 128), 1)
    packed = jnp.zeros((512, 512), F32)
    for q in range(4):
        block = jnp.concatenate([dot(hidden, dw[2 * q, 0:256]), dot(hidden, dw[2 * q + 1, 0:256])], axis=1).astype(BF)
        put = onehot(back_row == (back_col >> 2) * 16 + 4 * q + (back_col & 3))
        packed = packed + dot(put, block)
    part_y[...] = packed.astype(BF).reshape(NX, 128, 512)
    x_on, x_back, x_across = lax.rem(x + 1 + 2 * core, 4), lax.rem(x + 3 + 2 * core, 4), lax.rem(x + 2, 4)

    def half(h):
        return pl.ds(64 * h, 64)

    def y_across(h):
        return remote(part_y.at[x_across, half(h)], ry_recv.at[half(h)], ry_s.at[h], ry_r.at[h], xdev(x_on))

    def y_back(h):
        return remote(part_y.at[x_back, half(h)], yx_recv.at[1, half(h)], yx_s.at[1, h], yx_r.at[1, h], xdev(x_back))

    def y_on(h):
        return remote(my_send.at[half(h)], yx_recv.at[0, half(h)], yx_s.at[0, h], yx_r.at[0, h], xdev(x_on))

    for h in range(2):
        y_across(h).start()
    for h in range(2):
        y_back(h).start()

    def merge_on():
        for h in range(2):
            y_across(h).wait_recv()
            mine = part_y[x_on, half(h)].astype(F32) + ry_recv[half(h)].astype(F32)
            my_send[half(h)] = mine.astype(BF)
            y_on(h).start()

    need("eg", "eu", "ed")

    def chunk(p):
        depth = pl.ds(pl.multiple_of(p * 256, 256), 256)
        rows_p = ag_recv[p]
        acc[:, 0:512] += dot(rows_p, eg[depth, :])
        acc[:, 512:1024] += dot(rows_p, eu[depth, :])

    acc[...] = jnp.zeros_like(acc)

    def two_chunks(k, c):
        p = lax.rem(y + k + k // 2, 4)
        p = jnp.where(k == 3, across, p)
        direct, other = 2 * p + core, 2 * p + 1 - core

        @pl.when(k > 0)
        def _():
            remote(ag_recv.at[direct], ag_recv.at[direct], ag_s.at[p], ag_r.at[direct], ydev(p)).wait_recv()
            remote(ag_recv.at[direct], ag_recv.at[direct], ac_s.at[p], ag_r.at[direct], sibling).start()
        chunk(direct)
        remote(ag_recv.at[other], ag_recv.at[other], ac_s.at[p], ag_r.at[other], sibling).wait_recv()
        chunk(other)
        return c
    lax.fori_loop(0, 4, two_chunks, 0)
    phase("merge_on")
    merge_on()
    phase("down")
    recv_all(NE, ep, edev, sx_send, lambda p: sx_recv.at[p], sx_s, sx_r)
    every = jnp.concatenate([sx_recv[p] for p in range(NE)], axis=0)
    repeat = jnp.where((iota((128, 32), 0) >> 2) == iota((128, 32), 1), 1.0, 0.0)
    every = jnp.dot(repeat, every, preferred_element_type=F32, precision=lax.Precision.HIGHEST)
    wanted = iota((128, 256), 1) == 8 * ep + (iota((128, 256), 0) & 3)
    factor = jnp.sum(jnp.where(wanted, every, 0.0), axis=1, keepdims=True)
    hidden_e = (jax.nn.silu(acc[:, 0:512] * factor) * (acc[:, 512:1024] * factor)).astype(BF)

    def down_tile(p):
        return dot(hidden_e, ed[:, pl.ds(pl.multiple_of(p * 256, 256), 256)])

    def for_sibling(k, c):
        p = lax.rem(y + 2 + k, 4)
        pair_send[p] = down_tile(2 * p + 1 - core).astype(BF)
        remote(pair_send.at[p], pair_recv.at[p], pair_s.at[p], pair_r.at[p], sibling).start()
        return c
    lax.fori_loop(0, 4, for_sibling, 0)

    def for_own(k, c):
        p = lax.rem(y + 2 + k, 4)
        er_own[p] = down_tile(2 * p + core)
        return c
    lax.fori_loop(0, 4, for_own, 0)

    def pair_sum(p):
        remote(pair_send.at[p], pair_recv.at[p], pair_s.at[p], pair_r.at[p], sibling).wait_recv()
        return er_own[p] + pair_recv[p].astype(F32)

    def to_chips(k, c):
        p = lax.rem(y + 1 + lax.rem(k + 1, 3), 4)
        er_send[p] = pair_sum(p).astype(BF)
        remote(er_send.at[p], er_recv.at[y], er_s.at[p], er_r.at[y], ydev(p)).start()
        return c
    lax.fori_loop(0, 3, to_chips, 0)
    er_own[y] = pair_sum(y)

    phase("yx_wait")
    for h in range(2):
        y_back(h).wait_recv()
        y_on(h).wait_recv()
    summed = part_y[x].astype(F32) + yx_recv[0].astype(F32) + yx_recv[1].astype(F32)
    yz_send[...] = summed.astype(BF).reshape(NZ, 16, 512)
    send_all(NZ, z, zdev, lambda p: yz_send.at[p], yz_recv.at[z], yz_s, yz_r)
    yz_recv[z] = yz_send[z]

    phase("drain_early")
    sent_all(NT, t, tdev, lambda p: rs_send.at[p], rs_recv.at[t], rs_s, rs_r)
    sent_all(NT, t, tdev, lambda p: rr_send.at[p], rr_recv.at[t], rr_s, rr_r)
    sent_all(NT, t, tdev, lambda p: sc_send, sc_recv.at[t], sc_s, sc_r)
    sent_all(NE, ep, edev, lambda p: sx_send, sx_recv.at[ep], sx_s, sx_r)
    sent_all(NE, ep, edev, lambda p: md_send.at[p], md_recv.at[ep], md_s, md_r)
    sent_all(NZ, z, zdev, lambda p: rows_x.at[x, z], rows_x.at[x, z], xz_s, xz_r)

    def x_sent(zz, c):
        sent_all(NX, x, xdev, lambda p: rows_x.at[x, zz], rows_x.at[x, zz], xx_s.at[zz], xx_r.at[zz])
        return c
    lax.fori_loop(0, NZ, x_sent, 0)
    for h in range(2):
        weights_to_y(h, y, 0, ahead).wait_send()
        weights_to_y(h, y, 1, behind).wait_send()
        weights_to_y(h, origin, 2, onward).wait_send()
        y_across(h).wait_send()
        y_back(h).wait_send()
        y_on(h).wait_send()

    def core_sent(k, c):
        for h in range(2):
            weights_to_sibling(h, k).wait_send()
        tt = 2 * k + core
        remote(ag_recv.at[tt], ag_recv.at[tt], ac_s.at[k], ag_r.at[tt], sibling).wait_send()
        remote(pair_send.at[k], pair_recv.at[k], pair_s.at[k], pair_r.at[k], sibling).wait_send()
        return c
    lax.fori_loop(0, 4, core_sent, 0)
    sent_all(4, y, ydev, lambda p: own_rows, own_rows, ag_s, ag_r)
    new_state_copy.wait()

    phase("er_wait")
    recv_all(4, y, ydev, er_send.at[0], lambda p: er_recv.at[p], er_s, er_r)
    result = er_own[y]
    for k in range(1, 4):
        result = result + er_recv[lax.rem(y + k, 4)].astype(F32)
    result = result.astype(BF)
    mr_send[...] = (dot(pack[0], result[:, 0:128]) + dot(pack[1], result[:, 128:256])).astype(BF).reshape(NE, 8, 128)
    spread_out(lambda p: mr_send.at[p], mr_recv.at[ep], mr_s, mr_r)
    mr_recv[ep] = mr_send[ep]

    recv_all(NZ, z, zdev, yz_send.at[0], lambda p: yz_recv.at[p], yz_s, yz_r)
    dense = yz_recv[0].astype(F32)
    for p in range(1, NZ):
        dense = dense + yz_recv[p].astype(F32)
    dense = dense * mixing16
    for p in range(NT):
        q, half = p // 2, p % 2
        d5_send[p, 0:4, :] = dense[4 * q : 4 * q + 4, 256 * half : 256 * (half + 1)]
        d5_send[p, 4:8, :] = jnp.zeros((4, 256), F32)
    send_all(NT, t, tdev, lambda p: d5_send.at[p], d5_recv.at[t], d5_s, d5_r)
    d5_recv[t] = d5_send[t]

    phase("d5_wait")
    recv_all(NT, t, tdev, d5_send.at[0], lambda p: d5_recv.at[p], d5_s, d5_r)
    sent_all(4, y, ydev, lambda p: er_send.at[p], er_recv.at[y], er_s, er_r)
    sent_all(NZ, z, zdev, lambda p: yz_send.at[p], yz_recv.at[z], yz_s, yz_r)
    dense_rows = jnp.concatenate([d5_recv[p, 0:4, :] for p in range(NT)], axis=0)
    phase("mr_wait")
    recv_all(NE, ep, edev, mr_send.at[0], lambda p: mr_recv.at[p], mr_s, mr_r)
    returned = mr_recv[...].reshape(256, 128)
    phase("final")
    moe = jnp.concatenate([dot(combine[h], returned) for h in range(2)], axis=1)
    final_v[...] = (middle + moe + dense_rows).astype(BF)
    final_copy = pltpu.make_async_copy(final_v, final_h, out_sem.at[1])
    final_copy.start()

    phase("drain")
    sent_all(NT, t, tdev, lambda p: d5_send.at[p], d5_recv.at[t], d5_s, d5_r)
    sent_all(NE, ep, edev, lambda p: mr_send.at[p], mr_recv.at[ep], mr_s, mr_r)
    final_copy.wait()
    phase(None)


def hand_out(final_in, state_in, final_out, state_out, final_v, state_v, in_sem, out_sem):
    pieces = [(final_in, final_v, final_out)]
    for n in range(8):
        part = pl.ds(4 * n, 4)
        pieces.append((state_in.at[part], state_v.at[part], state_out.at[part]))
    ins = [pltpu.make_async_copy(a, b, in_sem.at[n]) for n, (a, b, _) in enumerate(pieces)]
    outs = [pltpu.make_async_copy(b, c, out_sem.at[n]) for n, (_, b, c) in enumerate(pieces)]
    for copy in ins:
        copy.start()
    for copy, out in zip(ins, outs):
        copy.wait()
        out.start()
    for out in outs:
        out.wait()


def per_device(*args):
    args = list(args)
    for n in (12, 13, 15, 16):
        args[n] = args[n].T
    inv = jnp.asarray((THETA ** (-np.arange(64) / 64.0)).astype(np.float32)[None, :])
    vmem = pltpu.VMEM

    def dma(*shape):
        return pltpu.SemaphoreType.DMA(shape)

    scratch = [
        vmem((32, 2048), BF), vmem((2048,), BF), vmem((2048, 512), BF), vmem((128,), BF),
        vmem((128, 2048), BF), vmem((32, 128, 128), F32), vmem((32,), jnp.int32), vmem((2048,), BF),
        vmem((2048,), BF), vmem((2, 32), jnp.int32), vmem((2, 32), BF),
        vmem((2048, 512), BF), vmem((2048, 512), BF), vmem((512, 2048), BF), vmem((1, 64), F32),
        vmem((32, 128), F32), vmem((8, 32, 256), BF), vmem((8, 32, 256), BF),
        vmem((8, 16, 512), BF), vmem((8, 16, 512), BF), vmem((1, 128), F32), vmem((8, 1, 128), F32),
        vmem((1, 256), F32), vmem((32, 1, 256), F32), vmem((4, 8, 16, 512), BF), vmem((8, 560, 256), BF),
        vmem((4, 128, 512), BF), vmem((128, 512), BF), vmem((128, 512), BF), vmem((2, 128, 512), BF),
        vmem((8, 16, 512), BF), vmem((8, 16, 512), BF),
        vmem((32, 8, 128), BF), vmem((32, 8, 128), BF), vmem((8, 128, 256), BF),
        vmem((4, 128, 256), BF), vmem((4, 128, 256), BF), vmem((4, 128, 256), F32),
        vmem((4, 128, 256), BF), vmem((4, 128, 256), BF), vmem((32, 8, 128), BF), vmem((32, 8, 128), BF),
        vmem((8, 8, 256), F32), vmem((8, 8, 256), F32), vmem((128, 1024), F32), vmem((32, 256), BF),
        dma(21), dma(2),
        dma(8), dma(8), dma(8), dma(8), dma(8), dma(8), dma(32), dma(32), dma(8), dma(8), dma(8, 4), dma(8, 4),
        dma(2, 3), dma(2, 4), dma(2, 4), dma(2, 4), dma(2), dma(2), dma(2, 2), dma(2, 2), dma(8), dma(8),
        dma(32), dma(32), dma(4), dma(8), dma(4), dma(4), dma(4), dma(4), dma(4), dma(32), dma(32), dma(8), dma(8),
    ]
    hbm = pl.BlockSpec(memory_space=pltpu.HBM)
    final, new_state = pl.pallas_call(
        step_kernel,
        out_shape=(
            jax.ShapeDtypeStruct((32, 256), BF),
            jax.ShapeDtypeStruct((32, 1, 128, 128), F32),
        ),
        in_specs=[hbm] * 21,
        out_specs=(hbm, hbm),
        scratch_shapes=scratch,
        compiler_params=pltpu.CompilerParams(
            collective_id=0, has_side_effects=True, vmem_limit_bytes=63200 * 1024
        ),
    )(*args, inv)
    return pl.pallas_call(
        hand_out,
        out_shape=(
            jax.ShapeDtypeStruct((32, 256), BF),
            jax.ShapeDtypeStruct((32, 1, 128, 128), F32),
        ),
        in_specs=[hbm, hbm],
        out_specs=(hbm, hbm),
        scratch_shapes=[vmem((32, 256), BF), vmem((32, 1, 128, 128), F32), dma(9), dma(9)],
        compiler_params=pltpu.CompilerParams(vmem_limit_bytes=63200 * 1024),
    )(final, new_state)


def solution(mesh):
    in_specs = (
        P("ep", None), P(), P(None, "tp"), P(None, "tp"), P(None, "tp"), P(None, "tp"), P("tp"),
        P("tp", None), P("ep", "tp", None, None), P("ep"), P(), P(), P("tp", "ep"), P("tp", "ep"),
        P("ep", "tp"), P("ep", None), P("ep", None), P("ep", None, "tp"), P("ep", None, "tp"),
        P("ep", "tp", None),
    )
    out_specs = (P("ep", "tp"), P("ep", "tp", None, None))
    return jax.shard_map(per_device, mesh=mesh, in_specs=in_specs, out_specs=out_specs, check_vma=False)
```

```python
import numpy as np
import jax
import jax.numpy as jnp
from jax import lax
from jax.experimental import pallas as pl
from jax.experimental.pallas import tpu as pltpu
from jax.sharding import PartitionSpec as P

EPSILON = 1e-06
THETA = 10000.0
BF = jnp.bfloat16
F32 = jnp.float32
NZ, NX, NT, NE = 8, 4, 8, 32


def iota(shape, dim):
    return lax.broadcasted_iota(jnp.int32, shape, dim)


def onehot(condition):
    return jnp.where(condition, 1.0, 0.0).astype(BF)


def dot(a, b):
    return jnp.dot(a, b, preferred_element_type=F32)


def dot_nt(a, b):
    return lax.dot_general(a, b, (((1,), (1,)), ((), ())), preferred_element_type=F32)


def as_column(row, n):
    return jnp.sum(jnp.where(iota((n, n), 0) == iota((n, n), 1), row, 0.0), axis=1, keepdims=True)


def as_row(column, n):
    return jnp.sum(jnp.where(iota((n, n), 0) == iota((n, n), 1), column, 0.0), axis=0, keepdims=True)


def step_kernel(
    resid_h, norm_gain_h, wq_h, wk_h, wv_h, wg_h, head_gain_h, wo_h, state_h, positions_h,
    ffn_gain_h, w_mix_h, dgate_h, dup_h, ddown_h, routes_h, rweight_h, eg_h, eu_h, ed_h, inv_h,
    final_h, new_state_h,
    resid, norm_gain, wqkvg, head_gain, wo, state, positions, ffn_gain, w_mix,
    routes, rweight, eg, eu, ed, inv,
    mix, rs_send, rs_recv, rr_send, rr_recv, sc_send, sc_recv, sx_send, sx_recv, rows_x, dw,
    part_y, ry_recv, my_send, yx_recv, yz_send, yz_recv, md_send, md_recv, ag_recv, pair_send, pair_recv, er_own, er_send, er_recv, mr_send, mr_recv,
    d5_send, d5_recv, acc, final_v,
    load_sem, out_sem,
    rs_s, rs_r, rr_s, rr_r, sc_s, sc_r, sx_s, sx_r, xz_s, xz_r, xx_s, xx_r, wy_s, wy_r, wc_s, wc_r,
    ry_s, ry_r, yx_s, yx_r, yz_s, yz_r,
    md_s, md_r, ag_s, ag_r, ac_s, pair_s, pair_r, er_s, er_r, mr_s, mr_r, d5_s, d5_r,
):
    ep = lax.axis_index("ep")
    t = lax.axis_index("tp")
    z = ep // NX
    x = lax.rem(ep, NX)
    y = t // 2
    core = lax.rem(t, 2)

    def zdev(p):
        return (p * NX + x, t)

    def xdev(p):
        return (z * NX + p, t)

    def tdev(p):
        return (ep, p)

    def ydev(p):
        return (ep, 2 * p + core)

    def edev(p):
        return (p, t)

    sibling = (ep, t + 1 - 2 * core)

    scope = []

    def phase(name):
        if scope:
            scope.pop().__exit__(None, None, None)
        if name:
            scope.append(jax.named_scope(name))
            scope[0].__enter__()

    loads = {}
    pairs = [
        ("resid", resid_h, resid), ("norm_gain", norm_gain_h, norm_gain),
        ("wq", wq_h, wqkvg.at[:, 0:128]), ("wk", wk_h, wqkvg.at[:, 128:256]),
        ("wv", wv_h, wqkvg.at[:, 256:384]), ("wg", wg_h, wqkvg.at[:, 384:512]),
        ("positions", positions_h, positions), ("inv", inv_h, inv), ("head_gain", head_gain_h, head_gain),
        ("state", state_h.at[:, 0], state), ("wo", wo_h, wo),
        ("ffn_gain", ffn_gain_h, ffn_gain), ("w_mix", w_mix_h, w_mix),
        ("routes", routes_h, routes), ("rweight", rweight_h, rweight),
        ("ddown", ddown_h, dw.at[t, 0:176]), ("dgate", dgate_h, dw.at[t, 176:352]),
        ("dup", dup_h, dw.at[t, 352:528]),
        ("eg", eg_h.at[0], eg), ("eu", eu_h.at[0], eu), ("ed", ed_h.at[0], ed),
    ]
    for n, (name, src, dst) in enumerate(pairs):
        slot = 2 if name in ("wq", "wk", "wv", "wg") else n
        loads[name] = pltpu.make_async_copy(src, dst, load_sem.at[slot])
        loads[name].start()

    phase("greet")
    barrier = pltpu.get_barrier_semaphore()
    for dev, me, n in ((edev, ep, NE), (tdev, t, NT)):
        def greet(k, c, dev=dev, me=me, n=n):
            p = lax.rem(me + lax.rem(k + n // 2, n - 1) + 1, n)
            pl.semaphore_signal(barrier, inc=1, device_id=dev(p), device_id_type=pl.DeviceIdType.MESH)
            return c
        lax.fori_loop(0, n - 1, greet, 0)

    def need(*names):
        for name in names:
            loads[name].wait()

    def remote(src, dst, ssem, rsem, dev):
        return pltpu.make_async_remote_copy(
            src_ref=src, dst_ref=dst, send_sem=ssem, recv_sem=rsem, device_id=dev,
            device_id_type=pl.DeviceIdType.MESH,
        )

    def send_all(n, me, dev, src_at, dst_here, ssem, rsem):
        def one(k, c):
            p = lax.rem(me + k, n)
            remote(src_at(p), dst_here, ssem, rsem, dev(p)).start()
            return c
        lax.fori_loop(1, n, one, 0)

    def arrived_all(block, ssem, rsem):
        remote(block, block, ssem, rsem, sibling).wait_recv()

    def sent_all(block, ssem, rsem):
        remote(block, block, ssem, rsem, sibling).wait_send()

    phase("retention")
    need("resid", "norm_gain")
    res = resid[...].astype(F32)
    ms = jnp.mean(res * res, axis=-1, keepdims=True)
    gain_in = norm_gain[...].reshape(1, 2048).astype(F32)
    normed_in = (res * lax.rsqrt(ms + EPSILON) * gain_in).astype(BF)
    need("positions", "inv")
    pltpu.make_async_copy(wqkvg, wqkvg, load_sem.at[2]).wait()
    angles = as_column(positions[...].astype(F32).reshape(1, 32), 32) * inv[...]
    cosine, sine = jnp.cos(angles), jnp.sin(angles)
    cos2 = jnp.concatenate([cosine, cosine], axis=-1)
    sin2 = jnp.concatenate([-sine, sine], axis=-1)
    qkvg = dot(normed_in, wqkvg[...]).astype(BF).astype(F32)

    def rotate(v):
        return v * cos2 + pltpu.roll(v, 64, 1) * sin2

    query = rotate(qkvg[:, 0:128])
    key = rotate(qkvg[:, 128:256]) * (128 ** -0.5)
    value = qkvg[:, 256:384]
    gating = qkvg[:, 384:512]
    decay = 1.0 - jnp.exp2(-1.0 - 1.5 * jnp.full((1, 128), t, jnp.int32).astype(F32))
    within = jnp.sum(query * key, axis=-1, keepdims=True) * value
    query_t = jnp.transpose(query)
    phase("state")
    need("state")
    for s in range(32):
        mix[s : s + 1, :] = jnp.sum(state[s] * query_t[:, s : s + 1], axis=0, keepdims=True)
    phase("head_out")
    need("head_gain", "wo")
    mixture = within + mix[...] * decay
    centre = jnp.mean(mixture, axis=-1, keepdims=True)
    spread = jnp.mean(jnp.square(mixture - centre), axis=-1, keepdims=True)
    normed = (mixture - centre) * lax.rsqrt(spread + EPSILON)
    normed = normed * head_gain[...].reshape(1, 128).astype(F32)
    retained = (jax.nn.silu(gating) * normed).astype(BF)
    partial = dot(retained, wo[...])
    for p in range(NT):
        rs_send[p] = partial[:, 256 * p : 256 * (p + 1)].astype(BF)
    for p in range(NT):
        tile = [partial[4 * p : 4 * p + 4, 512 * q : 512 * (q + 1)] for q in range(4)]
        rr_send[p] = jnp.concatenate(tile, axis=0).astype(BF)

    phase("barrier")
    pl.semaphore_wait(barrier, NE + NT - 2)

    phase("rs_send")
    send_all(NT, t, tdev, lambda p: rs_send.at[p], rs_recv.at[t], rs_s, rs_r)
    send_all(NT, t, tdev, lambda p: rr_send.at[p], rr_recv.at[t], rr_s, rr_r)
    rs_recv[t] = rs_send[t]
    rr_recv[t] = rr_send[t]

    need("ddown", "dgate", "dup")
    ahead, behind = lax.rem(y + 1, 4), lax.rem(y + 3, 4)
    onward = lax.rem(y + 1 + 2 * core, 4)
    origin = lax.rem(y + 3 + 2 * core, 4)
    across = lax.rem(y + 2, 4)
    parts = (pl.ds(272, 256), pl.ds(0, 272))

    def weights_to_y(h, owner, target):
        block = dw.at[2 * owner + core, parts[h]]
        return remote(block, block, wy_s, wy_r.at[h, owner], ydev(target))

    def weights_to_sibling(h, owner):
        block = dw.at[2 * owner + core, parts[h]]
        return remote(block, block, wc_s, wc_r, sibling)

    weights_to_y(0, y, ahead).start()
    weights_to_y(0, y, behind).start()
    for h in range(2):
        weights_to_sibling(h, y).start()

    key_t = jnp.transpose(key)
    for s in range(32):
        state[s] = state[s] * decay + key_t[:, s : s + 1] * value[s : s + 1, :]

    need("routes", "rweight", "ffn_gain", "w_mix")
    ids = jnp.transpose(routes[...].astype(F32))
    rw = jnp.transpose(rweight[...].astype(F32))
    lane_e = iota((32, 32), 1).astype(F32)
    hit0, hit1 = (lane_e == ids[:, 0:1]), (lane_e == ids[:, 1:2])
    both = jnp.where(hit0, 1.0, 0.0) + jnp.where(hit1, 1.0, 0.0)
    earlier = onehot(iota((32, 32), 1) < iota((32, 32), 0))
    rank = dot(earlier, both.astype(BF))
    weight_e = jnp.where(hit0, rw[:, 0:1], 0.0) + jnp.where(hit1, rw[:, 1:2], 0.0)
    lane = iota((32, 256), 1)
    widen = onehot((lane >> 3) == iota((32, 256), 0))
    slot = (lane & 3).astype(F32)
    taken = dot(both.astype(BF), widen) * jnp.where(dot(rank.astype(BF), widen) == slot, 1.0, 0.0)
    weighted = dot(weight_e.astype(BF), widen) * taken
    halves = [((lane >> 2) & 1) == h for h in range(2)]
    dispatch = [jnp.transpose(jnp.where(halves[h], taken, 0.0)).astype(BF) for h in range(2)]
    combine = [jnp.where(halves[h], weighted, 0.0).astype(BF) for h in range(2)]
    up_row, up_col = iota((128, 256), 0), iota((128, 256), 1)
    unpack = [onehot(up_col == (up_row >> 2) * 8 + 4 * h + (up_row & 3)) for h in range(2)]
    pk_row, pk_col = iota((256, 128), 0), iota((256, 128), 1)
    pack = [onehot(pk_row == (pk_col >> 2) * 8 + 4 * h + (pk_col & 3)) for h in range(2)]
    for p in range(NT):
        dw[p, 528:560, :] = jnp.zeros((32, 256), BF)
    gain_mid = ffn_gain[...].reshape(1, 2048).astype(F32)
    gain_here = gain_mid[:, 0:256]
    for p in range(1, NT):
        gain_here = jnp.where(t == p, gain_mid[:, 256 * p : 256 * (p + 1)], gain_here)
    mixer = w_mix[...].reshape(1, 2048).astype(F32)

    def as_tile(row):
        return jnp.concatenate(
            [jnp.broadcast_to(row[:, 512 * q : 512 * (q + 1)], (4, 512)) for q in range(4)], axis=0
        )

    gain_tile, mixer_tile = as_tile(gain_mid), as_tile(mixer)
    pick_row, pick_col = iota((16, 32), 0), iota((16, 32), 1)
    resid_tile = jnp.zeros((16, 512), F32)
    for q in range(4):
        pick = onehot((pick_col == 4 * t + (pick_row & 3)) & ((pick_row >> 2) == q))
        resid_tile = resid_tile + dot(pick, resid[:, 512 * q : 512 * (q + 1)])
    new_state_copy = pltpu.make_async_copy(state, new_state_h.at[:, 0], out_sem.at[0])
    new_state_copy.start()

    phase("rs_wait")
    arrived_all(rs_recv.at[0:7], rs_s, rs_r)
    phase("middle")
    columns = pl.ds(pl.multiple_of(t * 256, 256), 256)
    attention = rs_recv[0].astype(F32)
    for p in range(1, NT):
        attention = attention + rs_recv[p].astype(F32)
    middle = resid[:, columns].astype(F32) + attention
    scaled = (middle * gain_here).astype(BF)
    outgoing = dot(dispatch[0], scaled[:, 0:128]) + dot(dispatch[1], scaled[:, 128:256])
    md_send[...] = outgoing.astype(BF).reshape(NE, 8, 128)
    far = 16

    def spread_out(src_at, dst_here, ssem, rsem):
        def one(k, c):
            p = lax.rem(ep + lax.rem(k + far, NE - 1) + 1, NE)
            remote(src_at(p), dst_here, ssem, rsem, edev(p)).start()
            return c
        lax.fori_loop(0, NE - 1, one, 0)

    spread_out(lambda p: md_send.at[p], md_recv.at[ep], md_s, md_r)
    md_recv[ep] = md_send[ep]

    phase("rr_wait")
    arrived_all(rr_recv.at[0:7], rr_s, rr_r)
    middle_tile = rr_recv[0].astype(F32)
    for p in range(1, NT):
        middle_tile = middle_tile + rr_recv[p].astype(F32)
    middle_tile = middle_tile + resid_tile

    def over_quarters(column):
        total = column[0:4] + column[4:8] + column[8:12] + column[12:16]
        return jnp.concatenate([total] * 4, axis=0)

    squares = over_quarters(jnp.sum(middle_tile * middle_tile, axis=-1, keepdims=True))
    scale_tile = lax.rsqrt(squares * (1.0 / 2048) + EPSILON)
    normed_tile = (middle_tile * scale_tile * gain_tile).astype(BF)
    mixing16 = jax.nn.sigmoid(
        over_quarters(jnp.sum(normed_tile.astype(F32) * mixer_tile, axis=-1, keepdims=True))
    )
    rows_x[x, z] = normed_tile
    send_all(NZ, z, zdev, lambda p: rows_x.at[x, z], rows_x.at[x, z], xz_s, xz_r.at[z])

    def to_x(zz):
        send_all(NX, x, xdev, lambda p: rows_x.at[x, zz], rows_x.at[x, zz], xx_s, xx_r)

    to_x(z)

    lane16 = iota((16, 128), 1)
    sc_send[...] = jnp.sum(jnp.where(lane16 == iota((16, 128), 0), scale_tile, 0.0)[0:4], axis=0, keepdims=True)
    send_all(NT, t, tdev, lambda p: sc_send, sc_recv.at[t], sc_s, sc_r)
    sc_recv[t] = sc_send[...]
    weights_to_y(1, y, ahead).start()
    weights_to_y(1, y, behind).start()

    def relay(h):
        weights_to_y(h, origin, onward).wait_recv()
        weights_to_y(h, origin, onward).start()
        weights_to_sibling(h, origin).start()

    phase("relay_a")
    relay(0)

    phase("md_wait")
    arrived_all(md_recv.at[0:31], md_s, md_r)
    arrived = md_recv[...].reshape(256, 128)
    ag_recv[t] = jnp.concatenate([dot(unpack[h], arrived) for h in range(2)], axis=1).astype(BF)
    own_rows = ag_recv.at[t]

    remote(own_rows, own_rows, ag_s, ag_r.at[t], ydev(onward)).start()
    remote(own_rows, own_rows, ag_s, ag_r.at[t], ydev(origin)).start()
    remote(own_rows, own_rows, ac_s, ag_r.at[t], sibling).start()

    phase("xz_wait")
    def pass_on(k, c):
        p = lax.rem(z + k, NZ)
        remote(rows_x.at[x, p], rows_x.at[x, p], xz_s, xz_r.at[p], zdev(p)).wait_recv()
        to_x(p)
        return c
    lax.fori_loop(1, NZ, pass_on, 0)

    phase("relay_b")
    relay(1)

    phase("sc_wait")
    arrived_all(sc_recv.at[0:7], sc_s, sc_r)
    factors = jnp.concatenate([jnp.broadcast_to(sc_recv[p], (4, 128)) for p in range(NT)], axis=0)
    factors = jnp.sum(
        jnp.where(iota((32, 128), 1) == (iota((32, 128), 0) & 3), factors, 0.0), axis=1, keepdims=True
    )
    sx_send[...] = jnp.sum(taken * factors, axis=0, keepdims=True)
    spread_out(lambda p: sx_send, sx_recv.at[ep], sx_s, sx_r)
    sx_recv[ep] = sx_send[...]

    need("eg", "eu", "ed")

    def chunk(p):
        depth = pl.ds(pl.multiple_of(p * 256, 256), 256)
        rows_p = ag_recv[p]
        acc[:, 0:512] += dot(rows_p, eg[depth, :])
        acc[:, 512:1024] += dot(rows_p, eu[depth, :])

    acc[...] = jnp.zeros_like(acc)

    def group_rows(p, ssem, dev):
        block = ag_recv.at[2 * p + core]
        return remote(block, block, ssem, ag_r.at[2 * p + core], dev)

    def direct_chunk(p):
        group_rows(p, ag_s, ydev(p)).wait_recv()
        group_rows(p, ac_s, sibling).start()

    def other_chunk(p):
        block = ag_recv.at[2 * p + 1 - core]
        remote(block, block, ac_s, ag_r.at[2 * p + 1 - core], sibling).wait_recv()
        chunk(2 * p + 1 - core)

    chunk(t)
    other_chunk(y)
    phase("weights_on")
    for h in range(2):
        weights_to_y(h, onward, onward).wait_recv()
        weights_to_sibling(h, onward).start()
    phase("chunks")
    direct_chunk(origin)
    group_rows(origin, ag_s, ydev(onward)).start()
    chunk(2 * origin + core)
    direct_chunk(onward)
    chunk(2 * onward + core)
    other_chunk(onward)
    other_chunk(origin)
    phase("weights_across")
    for h in range(2):
        weights_to_y(h, across, onward).wait_recv()
        weights_to_sibling(h, across).start()
    phase("last_chunk")
    direct_chunk(across)
    chunk(2 * across + core)
    other_chunk(across)
    phase("weights_wait")
    arrived_all(dw.at[0:4, 0:528], wc_s, wc_r)

    phase("xx_wait")
    arrived_all(rows_x.at[0:3], xx_s, xx_r)

    phase("dense_mm")
    tiles = rows_x[...].reshape(512, 512)
    spread_row = iota((128, 512), 0)
    spread_col = iota((128, 512), 1)
    gate_up = jnp.zeros((128, 384), F32)
    for q in range(4):
        take = onehot(spread_col == (spread_row >> 2) * 16 + 4 * q + (spread_row & 3))
        block = dot(take, tiles).astype(BF)
        gate_up = gate_up + dot_nt(block[:, 0:256], dw[2 * q, 176:560])
        gate_up = gate_up + dot_nt(block[:, 256:512], dw[2 * q + 1, 176:560])
    up = pltpu.roll(gate_up, 384 - 176, 1)
    hidden = jnp.where(iota((128, 256), 1) < 176, jax.nn.silu(gate_up[:, 0:256]) * up[:, 0:256], 0.0).astype(BF)
    back_row = iota((512, 128), 0)
    back_col = iota((512, 128), 1)
    packed = jnp.zeros((512, 512), F32)
    for q in range(4):
        block = jnp.concatenate([dot(hidden, dw[2 * q, 0:256]), dot(hidden, dw[2 * q + 1, 0:256])], axis=1).astype(BF)
        put = onehot(back_row == (back_col >> 2) * 16 + 4 * q + (back_col & 3))
        packed = packed + dot(put, block)
    part_y[...] = packed.astype(BF).reshape(NX, 128, 512)
    x_on, x_back, x_across = lax.rem(x + 1 + 2 * core, 4), lax.rem(x + 3 + 2 * core, 4), lax.rem(x + 2, 4)

    def half(h):
        return pl.ds(64 * h, 64)

    def y_across(h):
        return remote(part_y.at[x_across, half(h)], ry_recv.at[half(h)], ry_s, ry_r.at[h], xdev(x_on))

    def y_back(h):
        return remote(part_y.at[x_back, half(h)], yx_recv.at[1, half(h)], yx_s, yx_r, xdev(x_back))

    def y_on(h):
        return remote(my_send.at[half(h)], yx_recv.at[0, half(h)], yx_s, yx_r, xdev(x_on))

    for h in range(2):
        y_across(h).start()
    for h in range(2):
        y_back(h).start()

    def merge_on():
        for h in range(2):
            y_across(h).wait_recv()
            mine = part_y[x_on, half(h)].astype(F32) + ry_recv[half(h)].astype(F32)
            my_send[half(h)] = mine.astype(BF)
            y_on(h).start()

    phase("down")
    arrived_all(sx_recv.at[0:31], sx_s, sx_r)
    every = jnp.concatenate([sx_recv[p] for p in range(NE)], axis=0)
    repeat = jnp.where((iota((128, 32), 0) >> 2) == iota((128, 32), 1), 1.0, 0.0)
    every = jnp.dot(repeat, every, preferred_element_type=F32, precision=lax.Precision.HIGHEST)
    wanted = iota((128, 256), 1) == 8 * ep + (iota((128, 256), 0) & 3)
    factor = jnp.sum(jnp.where(wanted, every, 0.0), axis=1, keepdims=True)
    hidden_e = (jax.nn.silu(acc[:, 0:512] * factor) * (acc[:, 512:1024] * factor)).astype(BF)

    def down_tile(p):
        return dot(hidden_e, ed[:, pl.ds(pl.multiple_of(p * 256, 256), 256)])

    def for_sibling(k, c):
        p = lax.rem(y + 2 + k, 4)
        pair_send[p] = down_tile(2 * p + 1 - core).astype(BF)
        remote(pair_send.at[p], pair_recv.at[p], pair_s, pair_r.at[p], sibling).start()
        return c
    lax.fori_loop(0, 4, for_sibling, 0)

    def for_own(k, c):
        p = lax.rem(y + 2 + k, 4)
        er_own[p] = down_tile(2 * p + core)
        return c
    lax.fori_loop(0, 4, for_own, 0)

    def pair_sum(p):
        remote(pair_send.at[p], pair_recv.at[p], pair_s, pair_r.at[p], sibling).wait_recv()
        return er_own[p] + pair_recv[p].astype(F32)

    def group_to(p, target, slot):
        return remote(er_send.at[p], er_recv.at[slot], er_s, er_r.at[slot], ydev(target))

    er_send[across] = pair_sum(across).astype(BF)
    group_to(across, onward, 0).start()
    er_send[origin] = pair_sum(origin).astype(BF)
    group_to(origin, origin, 1).start()
    er_own[y] = pair_sum(y)
    er_own[onward] = pair_sum(onward)

    def group_merge():
        group_to(across, onward, 0).wait_recv()
        er_send[onward] = (er_own[onward] + er_recv[0].astype(F32)).astype(BF)
        group_to(onward, onward, 2).start()

    phase("merge_on")
    merge_on()
    phase("group_merge")
    group_merge()
    phase("yx_wait")
    arrived_all(yx_recv, yx_s, yx_r)
    summed = part_y[x].astype(F32) + yx_recv[0].astype(F32) + yx_recv[1].astype(F32)
    yz_send[...] = summed.astype(BF).reshape(NZ, 16, 512)
    send_all(NZ, z, zdev, lambda p: yz_send.at[p], yz_recv.at[z], yz_s, yz_r)
    yz_recv[z] = yz_send[z]

    phase("drain_early")
    sent_all(rs_recv.at[0:7], rs_s, rs_r)
    sent_all(rr_recv.at[0:7], rr_s, rr_r)
    sent_all(sc_recv.at[0:7], sc_s, sc_r)
    sent_all(sx_recv.at[0:31], sx_s, sx_r)
    sent_all(md_recv.at[0:31], md_s, md_r)
    sent_all(rows_x.at[0, 0:7], xz_s, xz_r.at[0])

    sent_all(rows_x.at[0:3], xx_s, xx_r)
    sent_all(dw.at[0:3, 0:528], wy_s, wy_r.at[0, 0])
    sent_all(dw.at[0:4, 0:528], wc_s, wc_r)
    sent_all(ry_recv, ry_s, ry_r.at[0])
    sent_all(yx_recv, yx_s, yx_r)
    sent_all(ag_recv.at[0:3], ag_s, ag_r.at[0])
    sent_all(ag_recv.at[0:4], ac_s, ag_r.at[0])
    sent_all(pair_send, pair_s, pair_r.at[0])
    new_state_copy.wait()

    phase("er_wait")
    group_to(origin, origin, 1).wait_recv()
    group_to(onward, onward, 2).wait_recv()
    result = (er_own[y] + er_recv[1].astype(F32) + er_recv[2].astype(F32)).astype(BF)
    mr_send[...] = (dot(pack[0], result[:, 0:128]) + dot(pack[1], result[:, 128:256])).astype(BF).reshape(NE, 8, 128)
    spread_out(lambda p: mr_send.at[p], mr_recv.at[ep], mr_s, mr_r)
    mr_recv[ep] = mr_send[ep]

    arrived_all(yz_recv.at[0:7], yz_s, yz_r)
    dense = yz_recv[0].astype(F32)
    for p in range(1, NZ):
        dense = dense + yz_recv[p].astype(F32)
    dense = dense * mixing16
    for p in range(NT):
        q, half = p // 2, p % 2
        d5_send[p, 0:4, :] = dense[4 * q : 4 * q + 4, 256 * half : 256 * (half + 1)]
        d5_send[p, 4:8, :] = jnp.zeros((4, 256), F32)
    send_all(NT, t, tdev, lambda p: d5_send.at[p], d5_recv.at[t], d5_s, d5_r)
    d5_recv[t] = d5_send[t]

    phase("d5_wait")
    arrived_all(d5_recv.at[0:7], d5_s, d5_r)
    sent_all(er_recv.at[0:3], er_s, er_r.at[0])
    sent_all(yz_recv.at[0:7], yz_s, yz_r)
    dense_rows = jnp.concatenate([d5_recv[p, 0:4, :] for p in range(NT)], axis=0)
    phase("mr_wait")
    arrived_all(mr_recv.at[0:31], mr_s, mr_r)
    returned = mr_recv[...].reshape(256, 128)
    phase("final")
    moe = jnp.concatenate([dot(combine[h], returned) for h in range(2)], axis=1)
    final_v[...] = (middle + moe + dense_rows).astype(BF)
    final_copy = pltpu.make_async_copy(final_v, final_h, out_sem.at[1])
    final_copy.start()

    phase("drain")
    sent_all(d5_recv.at[0:7], d5_s, d5_r)
    sent_all(mr_recv.at[0:31], mr_s, mr_r)
    final_copy.wait()
    phase(None)


def hand_out(final_in, state_in, final_out, state_out, final_v, state_v, in_sem, out_sem):
    pieces = [(final_in, final_v, final_out)]
    for n in range(8):
        part = pl.ds(4 * n, 4)
        pieces.append((state_in.at[part], state_v.at[part], state_out.at[part]))
    ins = [pltpu.make_async_copy(a, b, in_sem.at[n]) for n, (a, b, _) in enumerate(pieces)]
    outs = [pltpu.make_async_copy(b, c, out_sem.at[n]) for n, (_, b, c) in enumerate(pieces)]
    for copy in ins:
        copy.start()
    for copy, out in zip(ins, outs):
        copy.wait()
        out.start()
    for out in outs:
        out.wait()


def per_device(*args):
    args = list(args)
    for n in (12, 13, 15, 16):
        args[n] = args[n].T
    inv = jnp.asarray((THETA ** (-np.arange(64) / 64.0)).astype(np.float32)[None, :])
    vmem = pltpu.VMEM

    def dma(*shape):
        return pltpu.SemaphoreType.DMA(shape)

    one = pltpu.SemaphoreType.DMA

    scratch = [
        vmem((32, 2048), BF), vmem((2048,), BF), vmem((2048, 512), BF), vmem((128,), BF),
        vmem((128, 2048), BF), vmem((32, 128, 128), F32), vmem((32,), jnp.int32), vmem((2048,), BF),
        vmem((2048,), BF), vmem((2, 32), jnp.int32), vmem((2, 32), BF),
        vmem((2048, 512), BF), vmem((2048, 512), BF), vmem((512, 2048), BF), vmem((1, 64), F32),
        vmem((32, 128), F32), vmem((8, 32, 256), BF), vmem((8, 32, 256), BF),
        vmem((8, 16, 512), BF), vmem((8, 16, 512), BF), vmem((1, 128), F32), vmem((8, 1, 128), F32),
        vmem((1, 256), F32), vmem((32, 1, 256), F32), vmem((4, 8, 16, 512), BF), vmem((8, 560, 256), BF),
        vmem((4, 128, 512), BF), vmem((128, 512), BF), vmem((128, 512), BF), vmem((2, 128, 512), BF),
        vmem((8, 16, 512), BF), vmem((8, 16, 512), BF),
        vmem((32, 8, 128), BF), vmem((32, 8, 128), BF), vmem((8, 128, 256), BF),
        vmem((4, 128, 256), BF), vmem((4, 128, 256), BF), vmem((4, 128, 256), F32),
        vmem((4, 128, 256), BF), vmem((4, 128, 256), BF), vmem((32, 8, 128), BF), vmem((32, 8, 128), BF),
        vmem((8, 8, 256), F32), vmem((8, 8, 256), F32), vmem((128, 1024), F32), vmem((32, 256), BF),
        dma(21), dma(2),
        one, one, one, one, one, one, one, one, one, dma(8), one, one,
        one, dma(2, 4), one, one, one, dma(2), one, one, one, one,
        one, one, one, dma(8), one, one, dma(4), one, dma(3), one, one, one, one,
    ]
    hbm = pl.BlockSpec(memory_space=pltpu.HBM)
    final, new_state = pl.pallas_call(
        step_kernel,
        out_shape=(
            jax.ShapeDtypeStruct((32, 256), BF),
            jax.ShapeDtypeStruct((32, 1, 128, 128), F32),
        ),
        in_specs=[hbm] * 21,
        out_specs=(hbm, hbm),
        scratch_shapes=scratch,
        compiler_params=pltpu.CompilerParams(
            collective_id=0, has_side_effects=True, vmem_limit_bytes=63200 * 1024
        ),
    )(*args, inv)
    return pl.pallas_call(
        hand_out,
        out_shape=(
            jax.ShapeDtypeStruct((32, 256), BF),
            jax.ShapeDtypeStruct((32, 1, 128, 128), F32),
        ),
        in_specs=[hbm, hbm],
        out_specs=(hbm, hbm),
        scratch_shapes=[vmem((32, 256), BF), vmem((32, 1, 128, 128), F32), dma(9), dma(9)],
        compiler_params=pltpu.CompilerParams(vmem_limit_bytes=63200 * 1024),
    )(final, new_state)


def solution(mesh):
    in_specs = (
        P("ep", None), P(), P(None, "tp"), P(None, "tp"), P(None, "tp"), P(None, "tp"), P("tp"),
        P("tp", None), P("ep", "tp", None, None), P("ep"), P(), P(), P("tp", "ep"), P("tp", "ep"),
        P("ep", "tp"), P("ep", None), P("ep", None), P("ep", None, "tp"), P("ep", None, "tp"),
        P("ep", "tp", None),
    )
    out_specs = (P("ep", "tp"), P("ep", "tp", None, None))
    return jax.shard_map(per_device, mesh=mesh, in_specs=in_specs, out_specs=out_specs, check_vma=False)
```

```python
import numpy as np
import jax
import jax.numpy as jnp
from jax import lax
from jax.experimental import pallas as pl
from jax.experimental.pallas import tpu as pltpu
from jax.sharding import PartitionSpec as P

EPSILON = 1e-06
THETA = 10000.0
BF = jnp.bfloat16
F32 = jnp.float32
NZ, NX, NT, NE = 8, 4, 8, 32


def iota(shape, dim):
    return lax.broadcasted_iota(jnp.int32, shape, dim)


def onehot(condition):
    return jnp.where(condition, 1.0, 0.0).astype(BF)


def dot(a, b):
    return jnp.dot(a, b, preferred_element_type=F32)


def dot_nt(a, b):
    return lax.dot_general(a, b, (((1,), (1,)), ((), ())), preferred_element_type=F32)


def as_column(row, n):
    return jnp.sum(jnp.where(iota((n, n), 0) == iota((n, n), 1), row, 0.0), axis=1, keepdims=True)


def as_row(column, n):
    return jnp.sum(jnp.where(iota((n, n), 0) == iota((n, n), 1), column, 0.0), axis=0, keepdims=True)


def step_kernel(
    resid_h, norm_gain_h, wq_h, wk_h, wv_h, wg_h, head_gain_h, wo_h, state_h, positions_h,
    ffn_gain_h, w_mix_h, dgate_h, dup_h, ddown_h, routes_h, rweight_h, eg_h, eu_h, ed_h, inv_h,
    final_h, new_state_h,
    resid, norm_gain, wqkvg, head_gain, wo, state, positions, ffn_gain, w_mix,
    routes, rweight, eg, eu, ed, inv,
    mix, rs_send, rs_recv, rr_send, rr_recv, sc_send, sc_recv, sx_send, sx_recv, rows_x, dw,
    part_y, ry_recv, my_send, yx_recv, md_send, md_recv, ag_recv, pair_send, pair_recv, er_own, er_send, er_recv, mr_send, mr_recv,
    zt_send, zt_recv, acc, final_v, rows_a, gate_up,
    load_sem, out_sem,
    rs_s, rs_r, rr_s, rr_r, sc_s, sc_r, sx_s, sx_r, xz_s, xz_r, xx_s, xx_r, wy_s, wy_r, wc_s, wc_r,
    ry_s, ry_r, yx_s, yx_r,
    md_s, md_r, ag_s, ag_r, ac_s, pair_s, pair_r, er_s, er_r, mr_s, mr_r, zt_s, zt_r,
):
    ep = lax.axis_index("ep")
    t = lax.axis_index("tp")
    z = ep // NX
    x = lax.rem(ep, NX)
    y = t // 2
    core = lax.rem(t, 2)

    def zdev(p):
        return (p * NX + x, t)

    def xdev(p):
        return (z * NX + p, t)

    def tdev(p):
        return (ep, p)

    def ydev(p):
        return (ep, 2 * p + core)

    def edev(p):
        return (p, t)

    sibling = (ep, t + 1 - 2 * core)

    scope = []

    def phase(name):
        if scope:
            scope.pop().__exit__(None, None, None)
        if name:
            scope.append(jax.named_scope(name))
            scope[0].__enter__()

    loads = {}
    pairs = [
        ("resid", resid_h, resid), ("norm_gain", norm_gain_h, norm_gain),
        ("wq", wq_h, wqkvg.at[:, 0:128]), ("wk", wk_h, wqkvg.at[:, 128:256]),
        ("wv", wv_h, wqkvg.at[:, 256:384]), ("wg", wg_h, wqkvg.at[:, 384:512]),
        ("positions", positions_h, positions), ("inv", inv_h, inv), ("head_gain", head_gain_h, head_gain),
        ("state", state_h.at[:, 0], state), ("wo", wo_h, wo),
        ("ffn_gain", ffn_gain_h, ffn_gain), ("w_mix", w_mix_h, w_mix),
        ("routes", routes_h, routes), ("rweight", rweight_h, rweight),
        ("ddown", ddown_h, dw.at[t, 0:176]), ("dgate", dgate_h, dw.at[t, 176:352]),
        ("dup", dup_h, dw.at[t, 352:528]),
        ("eg", eg_h.at[0], eg), ("eu", eu_h.at[0], eu), ("ed", ed_h.at[0], ed),
    ]
    for n, (name, src, dst) in enumerate(pairs):
        slot = 2 if name in ("wq", "wk", "wv", "wg") else n
        loads[name] = pltpu.make_async_copy(src, dst, load_sem.at[slot])
        loads[name].start()

    phase("greet")
    barrier = pltpu.get_barrier_semaphore()

    def greet(dev):
        pl.semaphore_signal(barrier, inc=1, device_id=dev, device_id_type=pl.DeviceIdType.MESH)

    def greet_column(k, c):
        for p in range(NT):
            greet((lax.rem(z + k, NZ) * NX + x, p))
        return c

    def greet_planes(k, c):
        for n in range(1, NX):
            greet((lax.rem(z + k, NZ) * NX + lax.rem(x + n, NX), t))
        return c

    def greet_group(k, c):
        greet(tdev(lax.rem(t + k, NT)))
        return c

    lax.fori_loop(NZ // 2, NZ, greet_column, 0)
    lax.fori_loop(NZ // 2, NZ, greet_planes, 0)
    lax.fori_loop(1, NZ // 2, greet_column, 0)
    lax.fori_loop(0, NZ // 2, greet_planes, 0)
    lax.fori_loop(1, NT, greet_group, 0)

    def need(*names):
        for name in names:
            loads[name].wait()

    def remote(src, dst, ssem, rsem, dev):
        return pltpu.make_async_remote_copy(
            src_ref=src, dst_ref=dst, send_sem=ssem, recv_sem=rsem, device_id=dev,
            device_id_type=pl.DeviceIdType.MESH,
        )

    def send_all(n, me, dev, src_at, dst_here, ssem, rsem):
        def one(k, c):
            p = lax.rem(me + k, n)
            remote(src_at(p), dst_here, ssem, rsem, dev(p)).start()
            return c
        lax.fori_loop(1, n, one, 0)

    def arrived_all(block, ssem, rsem):
        remote(block, block, ssem, rsem, sibling).wait_recv()

    def sent_all(block, ssem, rsem):
        remote(block, block, ssem, rsem, sibling).wait_send()

    phase("retention")
    need("resid", "norm_gain")
    res = resid[...].astype(F32)
    ms = jnp.mean(res * res, axis=-1, keepdims=True)
    gain_in = norm_gain[...].reshape(1, 2048).astype(F32)
    normed_in = (res * lax.rsqrt(ms + EPSILON) * gain_in).astype(BF)
    need("positions", "inv")
    pltpu.make_async_copy(wqkvg, wqkvg, load_sem.at[2]).wait()
    angles = as_column(positions[...].astype(F32).reshape(1, 32), 32) * inv[...]
    cosine, sine = jnp.cos(angles), jnp.sin(angles)
    cos2 = jnp.concatenate([cosine, cosine], axis=-1)
    sin2 = jnp.concatenate([-sine, sine], axis=-1)
    qkvg = dot(normed_in, wqkvg[...]).astype(BF).astype(F32)

    def rotate(v):
        return v * cos2 + pltpu.roll(v, 64, 1) * sin2

    query = rotate(qkvg[:, 0:128])
    key = rotate(qkvg[:, 128:256]) * (128 ** -0.5)
    value = qkvg[:, 256:384]
    gating = qkvg[:, 384:512]
    decay = 1.0 - jnp.exp2(-1.0 - 1.5 * jnp.full((1, 128), t, jnp.int32).astype(F32))
    within = jnp.sum(query * key, axis=-1, keepdims=True) * value
    query_t = jnp.transpose(query)
    phase("state")
    need("state")
    for s in range(32):
        mix[s : s + 1, :] = jnp.sum(state[s] * query_t[:, s : s + 1], axis=0, keepdims=True)
    phase("head_out")
    need("head_gain", "wo")
    mixture = within + mix[...] * decay
    centre = jnp.mean(mixture, axis=-1, keepdims=True)
    spread = jnp.mean(jnp.square(mixture - centre), axis=-1, keepdims=True)
    normed = (mixture - centre) * lax.rsqrt(spread + EPSILON)
    normed = normed * head_gain[...].reshape(1, 128).astype(F32)
    retained = (jax.nn.silu(gating) * normed).astype(BF)
    partial = dot(retained, wo[...])
    for p in range(NT):
        rs_send[p] = partial[:, 256 * p : 256 * (p + 1)].astype(BF)
    for p in range(NT):
        tile = [partial[4 * p : 4 * p + 4, 512 * q : 512 * (q + 1)] for q in range(4)]
        rr_send[p] = jnp.concatenate(tile, axis=0).astype(BF)

    phase("barrier")
    pl.semaphore_wait(barrier, NZ * NT - 1 + NZ * (NX - 1))

    phase("rs_send")
    send_all(NT, t, tdev, lambda p: rs_send.at[p], rs_recv.at[t], rs_s, rs_r)
    send_all(NT, t, tdev, lambda p: rr_send.at[p], rr_recv.at[t], rr_s, rr_r)
    rs_recv[t] = rs_send[t]
    rr_recv[t] = rr_send[t]

    need("ddown", "dgate", "dup")
    ahead, behind = lax.rem(y + 1, 4), lax.rem(y + 3, 4)
    onward = lax.rem(y + 1 + 2 * core, 4)
    origin = lax.rem(y + 3 + 2 * core, 4)
    across = lax.rem(y + 2, 4)
    parts = (pl.ds(272, 256), pl.ds(0, 272))

    def weights_to_y(h, owner, target):
        block = dw.at[2 * owner + core, parts[h]]
        return remote(block, block, wy_s, wy_r.at[h, owner], ydev(target))

    def weights_to_sibling(h, owner):
        block = dw.at[2 * owner + core, parts[h]]
        return remote(block, block, wc_s, wc_r, sibling)

    weights_to_y(0, y, ahead).start()
    weights_to_y(0, y, behind).start()
    for h in range(2):
        weights_to_sibling(h, y).start()

    key_t = jnp.transpose(key)
    for s in range(32):
        state[s] = state[s] * decay + key_t[:, s : s + 1] * value[s : s + 1, :]

    need("routes", "rweight", "ffn_gain", "w_mix")
    ids = jnp.transpose(routes[...].astype(F32))
    rw = jnp.transpose(rweight[...].astype(F32))
    lane_e = iota((32, 32), 1).astype(F32)
    hit0, hit1 = (lane_e == ids[:, 0:1]), (lane_e == ids[:, 1:2])
    both = jnp.where(hit0, 1.0, 0.0) + jnp.where(hit1, 1.0, 0.0)
    earlier = onehot(iota((32, 32), 1) < iota((32, 32), 0))
    rank = dot(earlier, both.astype(BF))
    weight_e = jnp.where(hit0, rw[:, 0:1], 0.0) + jnp.where(hit1, rw[:, 1:2], 0.0)
    lane = iota((32, 256), 1)
    widen = onehot((lane >> 3) == iota((32, 256), 0))
    slot = (lane & 3).astype(F32)
    taken = dot(both.astype(BF), widen) * jnp.where(dot(rank.astype(BF), widen) == slot, 1.0, 0.0)
    weighted = dot(weight_e.astype(BF), widen) * taken
    halves = [((lane >> 2) & 1) == h for h in range(2)]
    dispatch = [jnp.transpose(jnp.where(halves[h], taken, 0.0)).astype(BF) for h in range(2)]
    combine = [jnp.where(halves[h], weighted, 0.0).astype(BF) for h in range(2)]
    up_row, up_col = iota((128, 256), 0), iota((128, 256), 1)
    unpack = [onehot(up_col == (up_row >> 2) * 8 + 4 * h + (up_row & 3)) for h in range(2)]
    pk_row, pk_col = iota((256, 128), 0), iota((256, 128), 1)
    pack = [onehot(pk_row == (pk_col >> 2) * 8 + 4 * h + (pk_col & 3)) for h in range(2)]
    for p in range(NT):
        dw[p, 528:560, :] = jnp.zeros((32, 256), BF)
    gain_mid = ffn_gain[...].reshape(1, 2048).astype(F32)
    gain_here = gain_mid[:, 0:256]
    for p in range(1, NT):
        gain_here = jnp.where(t == p, gain_mid[:, 256 * p : 256 * (p + 1)], gain_here)
    mixer = w_mix[...].reshape(1, 2048).astype(F32)

    def as_tile(row):
        return jnp.concatenate(
            [jnp.broadcast_to(row[:, 512 * q : 512 * (q + 1)], (4, 512)) for q in range(4)], axis=0
        )

    gain_tile, mixer_tile = as_tile(gain_mid), as_tile(mixer)
    pick_row, pick_col = iota((16, 32), 0), iota((16, 32), 1)
    resid_tile = jnp.zeros((16, 512), F32)
    for q in range(4):
        pick = onehot((pick_col == 4 * t + (pick_row & 3)) & ((pick_row >> 2) == q))
        resid_tile = resid_tile + dot(pick, resid[:, 512 * q : 512 * (q + 1)])
    new_state_copy = pltpu.make_async_copy(state, new_state_h.at[:, 0], out_sem.at[0])
    new_state_copy.start()

    phase("rs_wait")
    arrived_all(rs_recv.at[0:7], rs_s, rs_r)
    phase("middle")
    columns = pl.ds(pl.multiple_of(t * 256, 256), 256)
    attention = rs_recv[0].astype(F32)
    for p in range(1, NT):
        attention = attention + rs_recv[p].astype(F32)
    middle = resid[:, columns].astype(F32) + attention
    scaled = (middle * gain_here).astype(BF)
    outgoing = dot(dispatch[0], scaled[:, 0:128]) + dot(dispatch[1], scaled[:, 128:256])
    md_send[...] = outgoing.astype(BF).reshape(NE, 8, 128)

    def spread_out(src_at, dst_here, ssem, rsem):
        def to(p):
            remote(src_at(p), dst_here, ssem, rsem, edev(p)).start()

        def one(k, c):
            for n in range(NX):
                to(lax.rem(z + k, NZ) * NX + n)
            return c
        lax.fori_loop(NZ // 2, NZ, one, 0)
        lax.fori_loop(1, NZ // 2, one, 0)
        for n in range(1, NX):
            to(z * NX + lax.rem(x + n, NX))

    spread_out(lambda p: md_send.at[p], md_recv.at[ep], md_s, md_r)
    md_recv[ep] = md_send[ep]

    phase("rr_wait")
    arrived_all(rr_recv.at[0:7], rr_s, rr_r)
    middle_tile = rr_recv[0].astype(F32)
    for p in range(1, NT):
        middle_tile = middle_tile + rr_recv[p].astype(F32)
    middle_tile = middle_tile + resid_tile

    def over_quarters(column):
        total = column[0:4] + column[4:8] + column[8:12] + column[12:16]
        return jnp.concatenate([total] * 4, axis=0)

    squares = over_quarters(jnp.sum(middle_tile * middle_tile, axis=-1, keepdims=True))
    scale_tile = lax.rsqrt(squares * (1.0 / 2048) + EPSILON)
    normed_tile = (middle_tile * scale_tile * gain_tile).astype(BF)
    mixing16 = jax.nn.sigmoid(
        over_quarters(jnp.sum(normed_tile.astype(F32) * mixer_tile, axis=-1, keepdims=True))
    )
    rows_x[x, z] = normed_tile
    send_all(NZ, z, zdev, lambda p: rows_x.at[x, z], rows_x.at[x, z], xz_s, xz_r.at[z])

    def to_x(zz):
        send_all(NX, x, xdev, lambda p: rows_x.at[x, zz], rows_x.at[x, zz], xx_s, xx_r)

    to_x(z)

    lane4, row4 = iota((4, 128), 1), iota((4, 128), 0)
    both_factors = jnp.where(lane4 == row4, scale_tile[0:4], 0.0) + jnp.where(lane4 == row4 + 4, mixing16[0:4], 0.0)
    sc_send[...] = jnp.sum(both_factors, axis=0, keepdims=True)
    send_all(NT, t, tdev, lambda p: sc_send, sc_recv.at[t], sc_s, sc_r)
    sc_recv[t] = sc_send[...]
    weights_to_y(1, y, ahead).start()
    weights_to_y(1, y, behind).start()

    def relay(h):
        weights_to_y(h, origin, onward).wait_recv()
        weights_to_y(h, origin, onward).start()
        weights_to_sibling(h, origin).start()

    phase("relay_a")
    relay(0)

    phase("xz_near")

    def pass_on(n, c):
        d = n // 2 + 1
        p = lax.rem(z + d + lax.rem(n, 2) * (NZ - 2 * d), NZ)
        remote(rows_x.at[x, p], rows_x.at[x, p], xz_s, xz_r.at[p], zdev(p)).wait_recv()
        to_x(p)
        return c
    lax.fori_loop(0, 2, pass_on, 0)

    phase("md_wait")
    arrived_all(md_recv.at[0:31], md_s, md_r)
    arrived = md_recv[...].reshape(256, 128)
    ag_recv[t] = jnp.concatenate([dot(unpack[h], arrived) for h in range(2)], axis=1).astype(BF)
    own_rows = ag_recv.at[t]

    remote(own_rows, own_rows, ag_s, ag_r.at[t], ydev(onward)).start()
    remote(own_rows, own_rows, ag_s, ag_r.at[t], ydev(origin)).start()
    remote(own_rows, own_rows, ac_s, ag_r.at[t], sibling).start()

    phase("xz_wait")
    lax.fori_loop(2, NZ - 1, pass_on, 0)

    phase("relay_b")
    relay(1)

    phase("sc_wait")
    arrived_all(sc_recv.at[0:7], sc_s, sc_r)
    factors = jnp.concatenate([jnp.broadcast_to(sc_recv[p], (4, 128)) for p in range(NT)], axis=0)
    fac_lane, fac_row = iota((32, 128), 1), iota((32, 128), 0) & 3
    mixing = jnp.sum(jnp.where(fac_lane == fac_row + 4, factors, 0.0), axis=1, keepdims=True)
    factors = jnp.sum(jnp.where(fac_lane == fac_row, factors, 0.0), axis=1, keepdims=True)
    sx_send[...] = jnp.sum(taken * factors, axis=0, keepdims=True)
    spread_out(lambda p: sx_send, sx_recv.at[ep], sx_s, sx_r)
    sx_recv[ep] = sx_send[...]

    need("eg", "eu", "ed")

    def chunk(p):
        depth = pl.ds(pl.multiple_of(p * 256, 256), 256)
        rows_p = ag_recv[p]
        acc[:, 0:512] += dot(rows_p, eg[depth, :])
        acc[:, 512:1024] += dot(rows_p, eu[depth, :])

    acc[...] = jnp.zeros_like(acc)

    def group_rows(p, ssem, dev):
        block = ag_recv.at[2 * p + core]
        return remote(block, block, ssem, ag_r.at[2 * p + core], dev)

    def direct_chunk(p):
        group_rows(p, ag_s, ydev(p)).wait_recv()
        group_rows(p, ac_s, sibling).start()

    def other_chunk(p):
        block = ag_recv.at[2 * p + 1 - core]
        remote(block, block, ac_s, ag_r.at[2 * p + 1 - core], sibling).wait_recv()
        chunk(2 * p + 1 - core)

    chunk(t)
    other_chunk(y)
    phase("weights_on")
    for h in range(2):
        weights_to_y(h, onward, onward).wait_recv()
        weights_to_sibling(h, onward).start()
    phase("chunks")
    direct_chunk(origin)
    group_rows(origin, ag_s, ydev(onward)).start()
    chunk(2 * origin + core)
    direct_chunk(onward)
    chunk(2 * onward + core)
    other_chunk(onward)
    other_chunk(origin)
    phase("weights_across")
    for h in range(2):
        weights_to_y(h, across, onward).wait_recv()
        weights_to_sibling(h, across).start()
    phase("ag_across")
    direct_chunk(across)
    phase("xx_wait")
    arrived_all(rows_x.at[0:3], xx_s, xx_r)
    phase("dense_a")
    tiles = rows_x[...].reshape(512, 512)
    spread_row = iota((128, 512), 0)
    spread_col = iota((128, 512), 1)
    for q in range(4):
        take = onehot(spread_col == (spread_row >> 2) * 16 + 4 * q + (spread_row & 3))
        block = dot(take, tiles).astype(BF)
        rows_a[2 * q] = block[:, 0:256]
        rows_a[2 * q + 1] = block[:, 256:512]

    def gate_up_by(side):
        total = jnp.zeros((128, 384), F32)
        for p in range(4):
            n = 2 * p + side
            total = total + dot_nt(rows_a[n], dw[n, 176:560])
        return total

    gate_up[...] = gate_up_by(core)
    phase("last_chunk")
    chunk(2 * across + core)
    other_chunk(across)
    phase("weights_wait")
    arrived_all(dw.at[0:4, 0:528], wc_s, wc_r)
    phase("dense_mm")
    both_sums = gate_up[...] + gate_up_by(1 - core)
    up = pltpu.roll(both_sums, 384 - 176, 1)
    hidden = jnp.where(iota((128, 256), 1) < 176, jax.nn.silu(both_sums[:, 0:256]) * up[:, 0:256], 0.0).astype(BF)
    x_on, x_back, x_across = lax.rem(x + 1 + 2 * core, 4), lax.rem(x + 3 + 2 * core, 4), lax.rem(x + 2, 4)

    def y_across(q):
        return remote(part_y.at[q, x_across], ry_recv.at[q], ry_s, ry_r.at[q], xdev(x_on))

    def y_back(q):
        return remote(part_y.at[q, x_back], yx_recv.at[1, q], yx_s, yx_r.at[q], xdev(x_back))

    def y_on(q):
        return remote(my_send.at[q], yx_recv.at[0, q], yx_s, yx_r.at[q], xdev(x_on))

    for q in range(4):
        for n in range(2):
            part = dot(hidden, dw[2 * q + n, 0:256]).astype(BF)
            part_y[q, :, :, 256 * n : 256 * (n + 1)] = part.reshape(NX, 32, 256)
        y_across(q).start()
        y_back(q).start()

    def merge_on():
        for q in range(4):
            y_across(q).wait_recv()
            my_send[q] = (part_y[q, x_on].astype(F32) + ry_recv[q].astype(F32)).astype(BF)
            y_on(q).start()

    phase("down")
    arrived_all(sx_recv.at[0:31], sx_s, sx_r)
    every = jnp.concatenate([sx_recv[p] for p in range(NE)], axis=0)
    repeat = jnp.where((iota((128, 32), 0) >> 2) == iota((128, 32), 1), 1.0, 0.0)
    every = jnp.dot(repeat, every, preferred_element_type=F32, precision=lax.Precision.HIGHEST)
    wanted = iota((128, 256), 1) == 8 * ep + (iota((128, 256), 0) & 3)
    factor = jnp.sum(jnp.where(wanted, every, 0.0), axis=1, keepdims=True)
    hidden_e = (jax.nn.silu(acc[:, 0:512] * factor) * (acc[:, 512:1024] * factor)).astype(BF)

    def down_tile(p):
        return dot(hidden_e, ed[:, pl.ds(pl.multiple_of(p * 256, 256), 256)])

    def for_sibling(k, c):
        p = lax.rem(y + 2 + k, 4)
        pair_send[p] = down_tile(2 * p + 1 - core).astype(BF)
        remote(pair_send.at[p], pair_recv.at[p], pair_s, pair_r.at[p], sibling).start()
        return c
    lax.fori_loop(0, 4, for_sibling, 0)

    def for_own(k, c):
        p = lax.rem(y + 2 + k, 4)
        er_own[p] = down_tile(2 * p + core)
        return c
    lax.fori_loop(0, 4, for_own, 0)

    def pair_sum(p):
        remote(pair_send.at[p], pair_recv.at[p], pair_s, pair_r.at[p], sibling).wait_recv()
        return er_own[p] + pair_recv[p].astype(F32)

    def group_to(p, target, slot, h, sem):
        part = pl.ds(64 * h, 64)
        return remote(er_send.at[p, part], er_recv.at[slot, part], er_s, er_r.at[sem], ydev(target))

    er_send[across] = pair_sum(across).astype(BF)
    for h in range(2):
        group_to(across, onward, 0, h, h).start()
    er_send[origin] = pair_sum(origin).astype(BF)
    for h in range(2):
        group_to(origin, origin, 1, h, 2).start()
    er_own[y] = pair_sum(y)
    er_own[onward] = pair_sum(onward)

    def group_merge():
        for h in range(2):
            group_to(across, onward, 0, h, h).wait_recv()
            part = pl.ds(64 * h, 64)
            er_send[onward, part] = (er_own[onward, part] + er_recv[0, part].astype(F32)).astype(BF)
            group_to(onward, onward, 2, h, 3).start()

    phase("merge_on")
    merge_on()
    phase("group_merge")
    group_merge()
    phase("yx_wait")
    zs_row, zs_col = iota((64, 32), 0), iota((64, 32), 1)
    to_half = [onehot(zs_row == (zs_col >> 2) * 8 + 4 * h + (zs_col & 3)) for h in range(2)]

    def to_column(p, n):
        remote(zt_send.at[p, n], zt_recv.at[z * NT + t], zt_s, zt_r, (p * NX + x, n)).start()

    for q in range(4):
        arrived_all(yx_recv.at[:, q], yx_s, yx_r.at[q])
        summed = part_y[q, x].astype(F32) + yx_recv[0, q].astype(F32) + yx_recv[1, q].astype(F32)
        summed = summed.astype(BF)
        low, high = dot(to_half[0], summed), dot(to_half[1], summed)
        for n in range(2):
            tile = low[:, 256 * n : 256 * n + 128] + high[:, 256 * n + 128 : 256 * n + 256]
            zt_send[:, 2 * q + n] = tile.astype(BF).reshape(NZ, 8, 128)

        def column_out(k, c, q=q):
            for n in range(2):
                to_column(lax.rem(z + k, NZ), 2 * q + n)
            return c
        lax.fori_loop(NZ // 2, NZ, column_out, 0)
        lax.fori_loop(1, NZ // 2, column_out, 0)

    def group_out(k, c):
        to_column(z, lax.rem(t + k, NT))
        return c
    lax.fori_loop(1, NT, group_out, 0)
    zt_recv[z * NT + t] = zt_send[z, t]

    phase("drain_early")
    sent_all(rs_recv.at[0:7], rs_s, rs_r)
    sent_all(rr_recv.at[0:7], rr_s, rr_r)
    sent_all(sc_recv.at[0:7], sc_s, sc_r)
    sent_all(sx_recv.at[0:31], sx_s, sx_r)
    sent_all(md_recv.at[0:31], md_s, md_r)
    sent_all(rows_x.at[0, 0:7], xz_s, xz_r.at[0])

    sent_all(rows_x.at[0:3], xx_s, xx_r)
    sent_all(dw.at[0:3, 0:528], wy_s, wy_r.at[0, 0])
    sent_all(dw.at[0:4, 0:528], wc_s, wc_r)
    sent_all(ry_recv, ry_s, ry_r.at[0])
    sent_all(yx_recv, yx_s, yx_r.at[0])
    sent_all(ag_recv.at[0:3], ag_s, ag_r.at[0])
    sent_all(ag_recv.at[0:4], ac_s, ag_r.at[0])
    sent_all(pair_send, pair_s, pair_r.at[0])
    new_state_copy.wait()

    phase("er_wait")
    arrived_all(er_recv.at[1], er_s, er_r.at[2])
    arrived_all(er_recv.at[2], er_s, er_r.at[3])
    result = (er_own[y] + er_recv[1].astype(F32) + er_recv[2].astype(F32)).astype(BF)
    mr_send[...] = (dot(pack[0], result[:, 0:128]) + dot(pack[1], result[:, 128:256])).astype(BF).reshape(NE, 8, 128)
    spread_out(lambda p: mr_send.at[p], mr_recv.at[ep], mr_s, mr_r)
    mr_recv[ep] = mr_send[ep]

    phase("zt_wait")
    un_row, un_col = iota((32, 512), 0), iota((32, 512), 1)
    un_token = ((un_col >> 3) & 7) * 4 + (un_col & 3)
    gather = [onehot((un_token == un_row) & (((un_col >> 2) & 1) == h)) for h in range(2)]
    sent_all(er_recv.at[0:3], er_s, er_r.at[0])
    arrived_all(zt_recv.at[0:63], zt_s, zt_r)
    columns_in = zt_recv[...].reshape(512, 128)
    dense_rows = jnp.concatenate([dot(gather[h], columns_in) for h in range(2)], axis=1) * mixing
    phase("mr_wait")
    arrived_all(mr_recv.at[0:31], mr_s, mr_r)
    returned = mr_recv[...].reshape(256, 128)
    phase("final")
    moe = jnp.concatenate([dot(combine[h], returned) for h in range(2)], axis=1)
    final_v[...] = (middle + moe + dense_rows).astype(BF)
    final_copy = pltpu.make_async_copy(final_v, final_h, out_sem.at[1])
    final_copy.start()

    phase("drain")
    sent_all(zt_recv.at[0:63], zt_s, zt_r)
    sent_all(mr_recv.at[0:31], mr_s, mr_r)
    final_copy.wait()
    phase(None)


def hand_out(final_in, state_in, final_out, state_out, final_v, state_v, in_sem, out_sem):
    pieces = [(final_in, final_v, final_out)]
    for n in range(8):
        part = pl.ds(4 * n, 4)
        pieces.append((state_in.at[part], state_v.at[part], state_out.at[part]))
    ins = [pltpu.make_async_copy(a, b, in_sem.at[n]) for n, (a, b, _) in enumerate(pieces)]
    outs = [pltpu.make_async_copy(b, c, out_sem.at[n]) for n, (_, b, c) in enumerate(pieces)]
    for copy in ins:
        copy.start()
    for copy, out in zip(ins, outs):
        copy.wait()
        out.start()
    for out in outs:
        out.wait()


def per_device(*args):
    args = list(args)
    for n in (12, 13, 15, 16):
        args[n] = args[n].T
    inv = jnp.asarray((THETA ** (-np.arange(64) / 64.0)).astype(np.float32)[None, :])
    vmem = pltpu.VMEM

    def dma(*shape):
        return pltpu.SemaphoreType.DMA(shape)

    one = pltpu.SemaphoreType.DMA

    scratch = [
        vmem((32, 2048), BF), vmem((2048,), BF), vmem((2048, 512), BF), vmem((128,), BF),
        vmem((128, 2048), BF), vmem((32, 128, 128), F32), vmem((32,), jnp.int32), vmem((2048,), BF),
        vmem((2048,), BF), vmem((2, 32), jnp.int32), vmem((2, 32), BF),
        vmem((2048, 512), BF), vmem((2048, 512), BF), vmem((512, 2048), BF), vmem((1, 64), F32),
        vmem((32, 128), F32), vmem((8, 32, 256), BF), vmem((8, 32, 256), BF),
        vmem((8, 16, 512), BF), vmem((8, 16, 512), BF), vmem((1, 128), F32), vmem((8, 1, 128), F32),
        vmem((1, 256), F32), vmem((32, 1, 256), F32), vmem((4, 8, 16, 512), BF), vmem((8, 560, 256), BF),
        vmem((4, 4, 32, 512), BF), vmem((4, 32, 512), BF), vmem((4, 32, 512), BF), vmem((2, 4, 32, 512), BF),
        vmem((32, 8, 128), BF), vmem((32, 8, 128), BF), vmem((8, 128, 256), BF),
        vmem((4, 128, 256), BF), vmem((4, 128, 256), BF), vmem((4, 128, 256), F32),
        vmem((4, 128, 256), BF), vmem((4, 128, 256), BF), vmem((32, 8, 128), BF), vmem((32, 8, 128), BF),
        vmem((8, 8, 8, 128), BF), vmem((64, 8, 128), BF), vmem((128, 1024), F32), vmem((32, 256), BF),
        vmem((8, 128, 256), BF), vmem((128, 384), F32),
        dma(21), dma(2),
        one, one, one, one, one, one, one, one, one, dma(8), one, one,
        one, dma(2, 4), one, one, one, dma(4), one, dma(4),
        one, one, one, dma(8), one, one, dma(4), one, dma(4), one, one, one, one,
    ]
    hbm = pl.BlockSpec(memory_space=pltpu.HBM)
    final, new_state = pl.pallas_call(
        step_kernel,
        out_shape=(
            jax.ShapeDtypeStruct((32, 256), BF),
            jax.ShapeDtypeStruct((32, 1, 128, 128), F32),
        ),
        in_specs=[hbm] * 21,
        out_specs=(hbm, hbm),
        scratch_shapes=scratch,
        compiler_params=pltpu.CompilerParams(
            collective_id=0, has_side_effects=True, vmem_limit_bytes=63200 * 1024
        ),
    )(*args, inv)
    return pl.pallas_call(
        hand_out,
        out_shape=(
            jax.ShapeDtypeStruct((32, 256), BF),
            jax.ShapeDtypeStruct((32, 1, 128, 128), F32),
        ),
        in_specs=[hbm, hbm],
        out_specs=(hbm, hbm),
        scratch_shapes=[vmem((32, 256), BF), vmem((32, 1, 128, 128), F32), dma(9), dma(9)],
        compiler_params=pltpu.CompilerParams(vmem_limit_bytes=63200 * 1024),
    )(final, new_state)


def solution(mesh):
    in_specs = (
        P("ep", None), P(), P(None, "tp"), P(None, "tp"), P(None, "tp"), P(None, "tp"), P("tp"),
        P("tp", None), P("ep", "tp", None, None), P("ep"), P(), P(), P("tp", "ep"), P("tp", "ep"),
        P("ep", "tp"), P("ep", None), P("ep", None), P("ep", None, "tp"), P("ep", None, "tp"),
        P("ep", "tp", None),
    )
    out_specs = (P("ep", "tp"), P("ep", "tp", None, None))
    return jax.shard_map(per_device, mesh=mesh, in_specs=in_specs, out_specs=out_specs, check_vma=False)
```

```python
import numpy as np
import jax
import jax.numpy as jnp
from jax import lax
from jax.experimental import pallas as pl
from jax.experimental.pallas import tpu as pltpu
from jax.sharding import PartitionSpec as P

EPSILON = 1e-06
THETA = 10000.0
BF = jnp.bfloat16
F32 = jnp.float32
NZ, NX, NT, NE = 8, 4, 8, 32


def iota(shape, dim):
    return lax.broadcasted_iota(jnp.int32, shape, dim)


def onehot(condition):
    return jnp.where(condition, 1.0, 0.0).astype(BF)


def dot(a, b):
    return jnp.dot(a, b, preferred_element_type=F32)


def dot_nt(a, b):
    return lax.dot_general(a, b, (((1,), (1,)), ((), ())), preferred_element_type=F32)


def as_column(row, n):
    return jnp.sum(jnp.where(iota((n, n), 0) == iota((n, n), 1), row, 0.0), axis=1, keepdims=True)


def as_row(column, n):
    return jnp.sum(jnp.where(iota((n, n), 0) == iota((n, n), 1), column, 0.0), axis=0, keepdims=True)


def step_kernel(
    resid_h, norm_gain_h, wq_h, wk_h, wv_h, wg_h, head_gain_h, wo_h, state_h, positions_h,
    ffn_gain_h, w_mix_h, dgate_h, dup_h, ddown_h, routes_h, rweight_h, eg_h, eu_h, ed_h, inv_h,
    final_h, new_state_h,
    resid, norm_gain, wqkvg, head_gain, wo, state, positions, ffn_gain, w_mix,
    routes, rweight, eg, eu, ed, inv,
    mix, rs_send, rs_recv, rr_send, rr_recv, sc_send, sc_recv, sx_send, sx_recv, rows_x, dw,
    part_y, ry_recv, my_send, yx_recv, md_send, md_recv, ag_recv, pair_send, pair_recv, er_own, er_send, er_recv, mr_send, mr_recv,
    zt_send, zt_recv, acc, final_v, rows_a, gate_up,
    load_sem, out_sem,
    rs_s, rs_r, rr_s, rr_r, sc_s, sc_r, sx_s, sx_r, xz_s, xz_r, xx_s, xx_r, wy_s, wy_r, wc_s, wc_r,
    ry_s, ry_r, yx_s, yx_r,
    md_s, md_r, ag_s, ag_r, ah_r, ac_s, pair_s, pair_r, er_s, er_r, mr_s, mr_r, zt_s, zt_r,
):
    ep = lax.axis_index("ep")
    t = lax.axis_index("tp")
    z = ep // NX
    x = lax.rem(ep, NX)
    y = t // 2
    core = lax.rem(t, 2)

    def zdev(p):
        return (p * NX + x, t)

    def xdev(p):
        return (z * NX + p, t)

    def tdev(p):
        return (ep, p)

    def ydev(p):
        return (ep, 2 * p + core)

    def edev(p):
        return (p, t)

    sibling = (ep, t + 1 - 2 * core)

    scope = []

    def phase(name):
        if scope:
            scope.pop().__exit__(None, None, None)
        if name:
            scope.append(jax.named_scope(name))
            scope[0].__enter__()

    loads = {}
    pairs = [
        ("resid", resid_h, resid), ("norm_gain", norm_gain_h, norm_gain),
        ("wq", wq_h, wqkvg.at[:, 0:128]), ("wk", wk_h, wqkvg.at[:, 128:256]),
        ("wv", wv_h, wqkvg.at[:, 256:384]), ("wg", wg_h, wqkvg.at[:, 384:512]),
        ("positions", positions_h, positions), ("inv", inv_h, inv), ("head_gain", head_gain_h, head_gain),
        ("state", state_h.at[:, 0], state), ("wo", wo_h, wo),
        ("ffn_gain", ffn_gain_h, ffn_gain), ("w_mix", w_mix_h, w_mix),
        ("routes", routes_h, routes), ("rweight", rweight_h, rweight),
        ("ddown", ddown_h, dw.at[t, 0:176]), ("dgate", dgate_h, dw.at[t, 176:352]),
        ("dup", dup_h, dw.at[t, 352:528]),
        ("eg", eg_h.at[0], eg), ("eu", eu_h.at[0], eu), ("ed", ed_h.at[0], ed),
    ]
    for n, (name, src, dst) in enumerate(pairs):
        slot = 2 if name in ("wq", "wk", "wv", "wg") else n
        loads[name] = pltpu.make_async_copy(src, dst, load_sem.at[slot])
        loads[name].start()

    phase("greet")
    barrier = pltpu.get_barrier_semaphore()

    def greet(dev):
        pl.semaphore_signal(barrier, inc=1, device_id=dev, device_id_type=pl.DeviceIdType.MESH)

    def greet_column(k, c):
        for p in range(NT):
            greet((lax.rem(z + k, NZ) * NX + x, p))
        return c

    def greet_planes(k, c):
        for n in range(1, NX):
            greet((lax.rem(z + k, NZ) * NX + lax.rem(x + n, NX), t))
        return c

    def greet_group(k, c):
        greet(tdev(lax.rem(t + k, NT)))
        return c

    lax.fori_loop(NZ // 2, NZ, greet_column, 0)
    lax.fori_loop(NZ // 2, NZ, greet_planes, 0)
    lax.fori_loop(1, NZ // 2, greet_column, 0)
    lax.fori_loop(0, NZ // 2, greet_planes, 0)
    lax.fori_loop(1, NT, greet_group, 0)

    def need(*names):
        for name in names:
            loads[name].wait()

    def remote(src, dst, ssem, rsem, dev):
        return pltpu.make_async_remote_copy(
            src_ref=src, dst_ref=dst, send_sem=ssem, recv_sem=rsem, device_id=dev,
            device_id_type=pl.DeviceIdType.MESH,
        )

    def send_all(n, me, dev, src_at, dst_here, ssem, rsem):
        def one(k, c):
            p = lax.rem(me + k, n)
            remote(src_at(p), dst_here, ssem, rsem, dev(p)).start()
            return c
        lax.fori_loop(1, n, one, 0)

    def arrived_all(block, ssem, rsem):
        remote(block, block, ssem, rsem, sibling).wait_recv()

    def sent_all(block, ssem, rsem):
        remote(block, block, ssem, rsem, sibling).wait_send()

    phase("retention")
    need("resid", "norm_gain")
    res = resid[...].astype(F32)
    ms = jnp.mean(res * res, axis=-1, keepdims=True)
    gain_in = norm_gain[...].reshape(1, 2048).astype(F32)
    normed_in = (res * lax.rsqrt(ms + EPSILON) * gain_in).astype(BF)
    need("positions", "inv")
    pltpu.make_async_copy(wqkvg, wqkvg, load_sem.at[2]).wait()
    angles = as_column(positions[...].astype(F32).reshape(1, 32), 32) * inv[...]
    cosine, sine = jnp.cos(angles), jnp.sin(angles)
    cos2 = jnp.concatenate([cosine, cosine], axis=-1)
    sin2 = jnp.concatenate([-sine, sine], axis=-1)
    qkvg = dot(normed_in, wqkvg[...]).astype(BF).astype(F32)

    def rotate(v):
        return v * cos2 + pltpu.roll(v, 64, 1) * sin2

    query = rotate(qkvg[:, 0:128])
    key = rotate(qkvg[:, 128:256]) * (128 ** -0.5)
    value = qkvg[:, 256:384]
    gating = qkvg[:, 384:512]
    decay = 1.0 - jnp.exp2(-1.0 - 1.5 * jnp.full((1, 128), t, jnp.int32).astype(F32))
    within = jnp.sum(query * key, axis=-1, keepdims=True) * value
    query_t = jnp.transpose(query)
    phase("state")
    need("state")
    for s in range(32):
        mix[s : s + 1, :] = jnp.sum(state[s] * query_t[:, s : s + 1], axis=0, keepdims=True)
    phase("head_out")
    need("head_gain", "wo")
    mixture = within + mix[...] * decay
    centre = jnp.mean(mixture, axis=-1, keepdims=True)
    spread = jnp.mean(jnp.square(mixture - centre), axis=-1, keepdims=True)
    normed = (mixture - centre) * lax.rsqrt(spread + EPSILON)
    normed = normed * head_gain[...].reshape(1, 128).astype(F32)
    retained = (jax.nn.silu(gating) * normed).astype(BF)
    partial = dot(retained, wo[...])
    for p in range(NT):
        rs_send[p] = partial[:, 256 * p : 256 * (p + 1)].astype(BF)
    for p in range(NT):
        tile = [partial[4 * p : 4 * p + 4, 512 * q : 512 * (q + 1)] for q in range(4)]
        rr_send[p] = jnp.concatenate(tile, axis=0).astype(BF)

    phase("barrier")
    pl.semaphore_wait(barrier, NZ * NT - 1 + NZ * (NX - 1))

    phase("rs_send")
    send_all(NT, t, tdev, lambda p: rs_send.at[p], rs_recv.at[t], rs_s, rs_r)
    send_all(NT, t, tdev, lambda p: rr_send.at[p], rr_recv.at[t], rr_s, rr_r)
    rs_recv[t] = rs_send[t]
    rr_recv[t] = rr_send[t]

    need("ddown", "dgate", "dup")
    ahead, behind = lax.rem(y + 1, 4), lax.rem(y + 3, 4)
    onward = lax.rem(y + 1 + 2 * core, 4)
    origin = lax.rem(y + 3 + 2 * core, 4)
    across = lax.rem(y + 2, 4)
    parts = (pl.ds(272, 256), pl.ds(0, 272))

    def weights_to_y(h, owner, target):
        block = dw.at[2 * owner + core, parts[h]]
        return remote(block, block, wy_s, wy_r.at[h, owner], ydev(target))

    def weights_to_sibling(h, owner):
        block = dw.at[2 * owner + core, parts[h]]
        return remote(block, block, wc_s, wc_r, sibling)

    weights_to_y(0, y, ahead).start()
    weights_to_y(0, y, behind).start()
    for h in range(2):
        weights_to_sibling(h, y).start()

    key_t = jnp.transpose(key)
    for s in range(32):
        state[s] = state[s] * decay + key_t[:, s : s + 1] * value[s : s + 1, :]

    need("routes", "rweight", "ffn_gain", "w_mix")
    ids = jnp.transpose(routes[...].astype(F32))
    rw = jnp.transpose(rweight[...].astype(F32))
    lane_e = iota((32, 32), 1).astype(F32)
    hit0, hit1 = (lane_e == ids[:, 0:1]), (lane_e == ids[:, 1:2])
    both = jnp.where(hit0, 1.0, 0.0) + jnp.where(hit1, 1.0, 0.0)
    earlier = onehot(iota((32, 32), 1) < iota((32, 32), 0))
    rank = dot(earlier, both.astype(BF))
    weight_e = jnp.where(hit0, rw[:, 0:1], 0.0) + jnp.where(hit1, rw[:, 1:2], 0.0)
    lane = iota((32, 256), 1)
    widen = onehot((lane >> 3) == iota((32, 256), 0))
    slot = (lane & 3).astype(F32)
    taken = dot(both.astype(BF), widen) * jnp.where(dot(rank.astype(BF), widen) == slot, 1.0, 0.0)
    weighted = dot(weight_e.astype(BF), widen) * taken
    halves = [((lane >> 2) & 1) == h for h in range(2)]
    dispatch = [jnp.transpose(jnp.where(halves[h], taken, 0.0)).astype(BF) for h in range(2)]
    combine = [jnp.where(halves[h], weighted, 0.0).astype(BF) for h in range(2)]
    up_row, up_col = iota((128, 256), 0), iota((128, 256), 1)
    unpack = [onehot(up_col == (up_row >> 2) * 8 + 4 * h + (up_row & 3)) for h in range(2)]
    pk_row, pk_col = iota((256, 128), 0), iota((256, 128), 1)
    pack = [onehot(pk_row == (pk_col >> 2) * 8 + 4 * h + (pk_col & 3)) for h in range(2)]
    for p in range(NT):
        dw[p, 528:560, :] = jnp.zeros((32, 256), BF)
    gain_mid = ffn_gain[...].reshape(1, 2048).astype(F32)
    gain_here = gain_mid[:, 0:256]
    for p in range(1, NT):
        gain_here = jnp.where(t == p, gain_mid[:, 256 * p : 256 * (p + 1)], gain_here)
    mixer = w_mix[...].reshape(1, 2048).astype(F32)

    def as_tile(row):
        return jnp.concatenate(
            [jnp.broadcast_to(row[:, 512 * q : 512 * (q + 1)], (4, 512)) for q in range(4)], axis=0
        )

    gain_tile, mixer_tile = as_tile(gain_mid), as_tile(mixer)
    pick_row, pick_col = iota((16, 32), 0), iota((16, 32), 1)
    resid_tile = jnp.zeros((16, 512), F32)
    for q in range(4):
        pick = onehot((pick_col == 4 * t + (pick_row & 3)) & ((pick_row >> 2) == q))
        resid_tile = resid_tile + dot(pick, resid[:, 512 * q : 512 * (q + 1)])
    new_state_copy = pltpu.make_async_copy(state, new_state_h.at[:, 0], out_sem.at[0])
    new_state_copy.start()

    phase("rs_wait")
    arrived_all(rs_recv.at[0:7], rs_s, rs_r)
    phase("middle")
    columns = pl.ds(pl.multiple_of(t * 256, 256), 256)
    attention = rs_recv[0].astype(F32)
    for p in range(1, NT):
        attention = attention + rs_recv[p].astype(F32)
    middle = resid[:, columns].astype(F32) + attention
    scaled = (middle * gain_here).astype(BF)
    outgoing = dot(dispatch[0], scaled[:, 0:128]) + dot(dispatch[1], scaled[:, 128:256])
    md_send[...] = outgoing.astype(BF).reshape(NE, 8, 128)

    def spread_out(src_at, dst_here, ssem, rsem):
        def to(p):
            remote(src_at(p), dst_here, ssem, rsem, edev(p)).start()

        def one(k, c):
            for n in range(NX):
                to(lax.rem(z + k, NZ) * NX + n)
            return c
        lax.fori_loop(NZ // 2, NZ, one, 0)
        lax.fori_loop(1, NZ // 2, one, 0)
        for n in range(1, NX):
            to(z * NX + lax.rem(x + n, NX))

    spread_out(lambda p: md_send.at[p], md_recv.at[ep], md_s, md_r)
    md_recv[ep] = md_send[ep]

    phase("rr_wait")
    arrived_all(rr_recv.at[0:7], rr_s, rr_r)
    middle_tile = rr_recv[0].astype(F32)
    for p in range(1, NT):
        middle_tile = middle_tile + rr_recv[p].astype(F32)
    middle_tile = middle_tile + resid_tile

    def over_quarters(column):
        total = column[0:4] + column[4:8] + column[8:12] + column[12:16]
        return jnp.concatenate([total] * 4, axis=0)

    squares = over_quarters(jnp.sum(middle_tile * middle_tile, axis=-1, keepdims=True))
    scale_tile = lax.rsqrt(squares * (1.0 / 2048) + EPSILON)
    normed_tile = (middle_tile * scale_tile * gain_tile).astype(BF)
    mixing16 = jax.nn.sigmoid(
        over_quarters(jnp.sum(normed_tile.astype(F32) * mixer_tile, axis=-1, keepdims=True))
    )
    rows_x[x, z] = normed_tile
    send_all(NZ, z, zdev, lambda p: rows_x.at[x, z], rows_x.at[x, z], xz_s, xz_r.at[z])

    def to_x(zz):
        send_all(NX, x, xdev, lambda p: rows_x.at[x, zz], rows_x.at[x, zz], xx_s, xx_r)

    to_x(z)

    lane4, row4 = iota((4, 128), 1), iota((4, 128), 0)
    both_factors = jnp.where(lane4 == row4, scale_tile[0:4], 0.0) + jnp.where(lane4 == row4 + 4, mixing16[0:4], 0.0)
    sc_send[...] = jnp.sum(both_factors, axis=0, keepdims=True)
    send_all(NT, t, tdev, lambda p: sc_send, sc_recv.at[t], sc_s, sc_r)
    sc_recv[t] = sc_send[...]
    weights_to_y(1, y, ahead).start()
    weights_to_y(1, y, behind).start()

    def relay(h):
        weights_to_y(h, origin, onward).wait_recv()
        weights_to_y(h, origin, onward).start()
        weights_to_sibling(h, origin).start()

    phase("relay_a")
    relay(0)

    phase("xz_near")

    def pass_on(n, c):
        d = n // 2 + 1
        p = lax.rem(z + d + lax.rem(n, 2) * (NZ - 2 * d), NZ)
        remote(rows_x.at[x, p], rows_x.at[x, p], xz_s, xz_r.at[p], zdev(p)).wait_recv()
        to_x(p)
        return c
    lax.fori_loop(0, 2, pass_on, 0)

    phase("md_wait")
    arrived_all(md_recv.at[0:31], md_s, md_r)
    arrived = md_recv[...].reshape(256, 128)
    ag_recv[t] = jnp.concatenate([dot(unpack[h], arrived) for h in range(2)], axis=1).astype(BF)
    own_rows = ag_recv.at[t]

    halves_of = (pl.ds(0, 64), pl.ds(64, 64))
    for h in range(2):
        block = ag_recv.at[t, halves_of[h]]
        remote(block, block, ag_s, ah_r.at[h], ydev(onward)).start()
    remote(own_rows, own_rows, ag_s, ag_r.at[t], ydev(origin)).start()
    remote(own_rows, own_rows, ac_s, ag_r.at[t], sibling).start()

    phase("xz_wait")
    lax.fori_loop(2, NZ - 1, pass_on, 0)

    phase("relay_b")
    relay(1)

    phase("sc_wait")
    arrived_all(sc_recv.at[0:7], sc_s, sc_r)
    factors = jnp.concatenate([jnp.broadcast_to(sc_recv[p], (4, 128)) for p in range(NT)], axis=0)
    fac_lane, fac_row = iota((32, 128), 1), iota((32, 128), 0) & 3
    mixing = jnp.sum(jnp.where(fac_lane == fac_row + 4, factors, 0.0), axis=1, keepdims=True)
    factors = jnp.sum(jnp.where(fac_lane == fac_row, factors, 0.0), axis=1, keepdims=True)
    sx_send[...] = jnp.sum(taken * factors, axis=0, keepdims=True)
    spread_out(lambda p: sx_send, sx_recv.at[ep], sx_s, sx_r)
    sx_recv[ep] = sx_send[...]

    need("eg", "eu", "ed")

    def chunk(p):
        depth = pl.ds(pl.multiple_of(p * 256, 256), 256)
        rows_p = ag_recv[p]
        acc[:, 0:512] += dot(rows_p, eg[depth, :])
        acc[:, 512:1024] += dot(rows_p, eu[depth, :])

    acc[...] = jnp.zeros_like(acc)

    def group_rows(p, ssem, dev):
        block = ag_recv.at[2 * p + core]
        return remote(block, block, ssem, ag_r.at[2 * p + core], dev)

    def direct_chunk(p):
        group_rows(p, ag_s, ydev(p)).wait_recv()
        group_rows(p, ac_s, sibling).start()

    def other_chunk(p):
        block = ag_recv.at[2 * p + 1 - core]
        remote(block, block, ac_s, ag_r.at[2 * p + 1 - core], sibling).wait_recv()
        chunk(2 * p + 1 - core)

    chunk(t)
    other_chunk(y)
    phase("weights_on")
    for h in range(2):
        weights_to_y(h, onward, onward).wait_recv()
        weights_to_sibling(h, onward).start()
    phase("chunks")
    for h in range(2):
        block = ag_recv.at[2 * origin + core, halves_of[h]]
        remote(block, block, ag_s, ah_r.at[h], ydev(origin)).wait_recv()
        remote(block, block, ag_s, ag_r.at[2 * origin + core], ydev(onward)).start()
    group_rows(origin, ac_s, sibling).start()
    chunk(2 * origin + core)
    direct_chunk(onward)
    chunk(2 * onward + core)
    other_chunk(onward)
    other_chunk(origin)
    phase("weights_across")
    for h in range(2):
        weights_to_y(h, across, onward).wait_recv()
        weights_to_sibling(h, across).start()
    phase("ag_across")
    direct_chunk(across)
    phase("xx_wait")
    arrived_all(rows_x.at[0:3], xx_s, xx_r)
    phase("dense_a")
    tiles = rows_x[...].reshape(512, 512)
    spread_row = iota((128, 512), 0)
    spread_col = iota((128, 512), 1)
    for q in range(4):
        take = onehot(spread_col == (spread_row >> 2) * 16 + 4 * q + (spread_row & 3))
        block = dot(take, tiles).astype(BF)
        rows_a[2 * q] = block[:, 0:256]
        rows_a[2 * q + 1] = block[:, 256:512]

    def gate_up_by(side):
        total = jnp.zeros((128, 384), F32)
        for p in range(4):
            n = 2 * p + side
            total = total + dot_nt(rows_a[n], dw[n, 176:560])
        return total

    gate_up[...] = gate_up_by(core)
    phase("weights_wait")
    arrived_all(dw.at[0:4, 0:528], wc_s, wc_r)
    phase("dense_mm")
    both_sums = gate_up[...] + gate_up_by(1 - core)
    up = pltpu.roll(both_sums, 384 - 176, 1)
    hidden = jnp.where(iota((128, 256), 1) < 176, jax.nn.silu(both_sums[:, 0:256]) * up[:, 0:256], 0.0).astype(BF)
    x_on, x_back, x_across = lax.rem(x + 1 + 2 * core, 4), lax.rem(x + 3 + 2 * core, 4), lax.rem(x + 2, 4)

    def y_across(q):
        return remote(part_y.at[q, x_across], ry_recv.at[q], ry_s, ry_r.at[q], xdev(x_on))

    def y_back(q):
        return remote(part_y.at[q, x_back], yx_recv.at[1, q], yx_s, yx_r.at[q], xdev(x_back))

    def y_on(q):
        return remote(my_send.at[q], yx_recv.at[0, q], yx_s, yx_r.at[q], xdev(x_on))

    for q in range(4):
        for n in range(2):
            part = dot(hidden, dw[2 * q + n, 0:256]).astype(BF)
            part_y[q, :, :, 256 * n : 256 * (n + 1)] = part.reshape(NX, 32, 256)
        y_across(q).start()
        y_back(q).start()

    def merge_on():
        for q in range(4):
            y_across(q).wait_recv()
            my_send[q] = (part_y[q, x_on].astype(F32) + ry_recv[q].astype(F32)).astype(BF)
            y_on(q).start()

    phase("last_chunk")
    chunk(2 * across + core)
    other_chunk(across)
    phase("down")
    arrived_all(sx_recv.at[0:31], sx_s, sx_r)
    every = jnp.concatenate([sx_recv[p] for p in range(NE)], axis=0)
    repeat = jnp.where((iota((128, 32), 0) >> 2) == iota((128, 32), 1), 1.0, 0.0)
    every = jnp.dot(repeat, every, preferred_element_type=F32, precision=lax.Precision.HIGHEST)
    wanted = iota((128, 256), 1) == 8 * ep + (iota((128, 256), 0) & 3)
    factor = jnp.sum(jnp.where(wanted, every, 0.0), axis=1, keepdims=True)
    hidden_e = (jax.nn.silu(acc[:, 0:512] * factor) * (acc[:, 512:1024] * factor)).astype(BF)

    def down_tile(p):
        return dot(hidden_e, ed[:, pl.ds(pl.multiple_of(p * 256, 256), 256)])

    for p in (across, onward, y, origin):
        pair_send[p] = down_tile(2 * p + 1 - core).astype(BF)
        remote(pair_send.at[p], pair_recv.at[p], pair_s, pair_r.at[p], sibling).start()

    def pair_sum(p):
        own = down_tile(2 * p + core)
        remote(pair_send.at[p], pair_recv.at[p], pair_s, pair_r.at[p], sibling).wait_recv()
        return own + pair_recv[p].astype(F32)

    def group_to(p, target, slot, h, sem):
        part = pl.ds(64 * h, 64)
        return remote(er_send.at[p, part], er_recv.at[slot, part], er_s, er_r.at[sem], ydev(target))

    er_send[across] = pair_sum(across).astype(BF)
    for h in range(2):
        group_to(across, onward, 0, h, h).start()
    er_send[origin] = pair_sum(origin).astype(BF)
    for h in range(2):
        group_to(origin, origin, 1, h, 2).start()
    er_own[y] = pair_sum(y)
    er_own[onward] = pair_sum(onward)

    def group_merge():
        for h in range(2):
            group_to(across, onward, 0, h, h).wait_recv()
            part = pl.ds(64 * h, 64)
            er_send[onward, part] = (er_own[onward, part] + er_recv[0, part].astype(F32)).astype(BF)
            group_to(onward, onward, 2, h, 3).start()

    phase("merge_on")
    merge_on()
    phase("group_merge")
    group_merge()
    phase("yx_wait")
    zs_row, zs_col = iota((64, 32), 0), iota((64, 32), 1)
    to_half = [onehot(zs_row == (zs_col >> 2) * 8 + 4 * h + (zs_col & 3)) for h in range(2)]

    def to_column(p, n):
        remote(zt_send.at[p, n], zt_recv.at[z * NT + t], zt_s, zt_r, (p * NX + x, n)).start()

    for q in range(4):
        arrived_all(yx_recv.at[:, q], yx_s, yx_r.at[q])
        summed = part_y[q, x].astype(F32) + yx_recv[0, q].astype(F32) + yx_recv[1, q].astype(F32)
        summed = summed.astype(BF)
        low, high = dot(to_half[0], summed), dot(to_half[1], summed)
        for n in range(2):
            tile = low[:, 256 * n : 256 * n + 128] + high[:, 256 * n + 128 : 256 * n + 256]
            zt_send[:, 2 * q + n] = tile.astype(BF).reshape(NZ, 8, 128)

        def column_out(k, c, q=q):
            for n in range(2):
                to_column(lax.rem(z + k, NZ), 2 * q + n)
            return c
        lax.fori_loop(NZ // 2, NZ, column_out, 0)
        lax.fori_loop(1, NZ // 2, column_out, 0)

    def group_out(k, c):
        to_column(z, lax.rem(t + k, NT))
        return c
    lax.fori_loop(1, NT, group_out, 0)
    zt_recv[z * NT + t] = zt_send[z, t]

    phase("drain_early")
    sent_all(rs_recv.at[0:7], rs_s, rs_r)
    sent_all(rr_recv.at[0:7], rr_s, rr_r)
    sent_all(sc_recv.at[0:7], sc_s, sc_r)
    sent_all(sx_recv.at[0:31], sx_s, sx_r)
    sent_all(md_recv.at[0:31], md_s, md_r)
    sent_all(rows_x.at[0, 0:7], xz_s, xz_r.at[0])

    sent_all(rows_x.at[0:3], xx_s, xx_r)
    sent_all(dw.at[0:3, 0:528], wy_s, wy_r.at[0, 0])
    sent_all(dw.at[0:4, 0:528], wc_s, wc_r)
    sent_all(ry_recv, ry_s, ry_r.at[0])
    sent_all(yx_recv, yx_s, yx_r.at[0])
    sent_all(ag_recv.at[0:3], ag_s, ag_r.at[0])
    sent_all(ag_recv.at[0:4], ac_s, ag_r.at[0])
    sent_all(pair_send, pair_s, pair_r.at[0])
    new_state_copy.wait()

    phase("er_wait")
    arrived_all(er_recv.at[1], er_s, er_r.at[2])
    arrived_all(er_recv.at[2], er_s, er_r.at[3])
    result = (er_own[y] + er_recv[1].astype(F32) + er_recv[2].astype(F32)).astype(BF)
    mr_send[...] = (dot(pack[0], result[:, 0:128]) + dot(pack[1], result[:, 128:256])).astype(BF).reshape(NE, 8, 128)
    spread_out(lambda p: mr_send.at[p], mr_recv.at[ep], mr_s, mr_r)
    mr_recv[ep] = mr_send[ep]

    phase("zt_wait")
    un_row, un_col = iota((32, 512), 0), iota((32, 512), 1)
    un_token = ((un_col >> 3) & 7) * 4 + (un_col & 3)
    gather = [onehot((un_token == un_row) & (((un_col >> 2) & 1) == h)) for h in range(2)]
    sent_all(er_recv.at[0:3], er_s, er_r.at[0])
    arrived_all(zt_recv.at[0:63], zt_s, zt_r)
    columns_in = zt_recv[...].reshape(512, 128)
    dense_rows = jnp.concatenate([dot(gather[h], columns_in) for h in range(2)], axis=1) * mixing
    phase("mr_wait")
    arrived_all(mr_recv.at[0:31], mr_s, mr_r)
    returned = mr_recv[...].reshape(256, 128)
    phase("final")
    moe = jnp.concatenate([dot(combine[h], returned) for h in range(2)], axis=1)
    final_v[...] = (middle + moe + dense_rows).astype(BF)
    final_copy = pltpu.make_async_copy(final_v, final_h, out_sem.at[1])
    final_copy.start()

    phase("drain")
    sent_all(zt_recv.at[0:63], zt_s, zt_r)
    sent_all(mr_recv.at[0:31], mr_s, mr_r)
    final_copy.wait()
    phase(None)


def hand_out(final_in, state_in, final_out, state_out, final_v, state_v, in_sem, out_sem):
    pieces = [(final_in, final_v, final_out)]
    for n in range(8):
        part = pl.ds(4 * n, 4)
        pieces.append((state_in.at[part], state_v.at[part], state_out.at[part]))
    ins = [pltpu.make_async_copy(a, b, in_sem.at[n]) for n, (a, b, _) in enumerate(pieces)]
    outs = [pltpu.make_async_copy(b, c, out_sem.at[n]) for n, (_, b, c) in enumerate(pieces)]
    for copy in ins:
        copy.start()
    for copy, out in zip(ins, outs):
        copy.wait()
        out.start()
    for out in outs:
        out.wait()


def per_device(*args):
    args = list(args)
    for n in (12, 13, 15, 16):
        args[n] = args[n].T
    inv = jnp.asarray((THETA ** (-np.arange(64) / 64.0)).astype(np.float32)[None, :])
    vmem = pltpu.VMEM

    def dma(*shape):
        return pltpu.SemaphoreType.DMA(shape)

    one = pltpu.SemaphoreType.DMA

    scratch = [
        vmem((32, 2048), BF), vmem((2048,), BF), vmem((2048, 512), BF), vmem((128,), BF),
        vmem((128, 2048), BF), vmem((32, 128, 128), F32), vmem((32,), jnp.int32), vmem((2048,), BF),
        vmem((2048,), BF), vmem((2, 32), jnp.int32), vmem((2, 32), BF),
        vmem((2048, 512), BF), vmem((2048, 512), BF), vmem((512, 2048), BF), vmem((1, 64), F32),
        vmem((32, 128), F32), vmem((8, 32, 256), BF), vmem((8, 32, 256), BF),
        vmem((8, 16, 512), BF), vmem((8, 16, 512), BF), vmem((1, 128), F32), vmem((8, 1, 128), F32),
        vmem((1, 256), F32), vmem((32, 1, 256), F32), vmem((4, 8, 16, 512), BF), vmem((8, 560, 256), BF),
        vmem((4, 4, 32, 512), BF), vmem((4, 32, 512), BF), vmem((4, 32, 512), BF), vmem((2, 4, 32, 512), BF),
        vmem((32, 8, 128), BF), vmem((32, 8, 128), BF), vmem((8, 128, 256), BF),
        vmem((4, 128, 256), BF), vmem((4, 128, 256), BF), vmem((4, 128, 256), F32),
        vmem((4, 128, 256), BF), vmem((4, 128, 256), BF), vmem((32, 8, 128), BF), vmem((32, 8, 128), BF),
        vmem((8, 8, 8, 128), BF), vmem((64, 8, 128), BF), vmem((128, 1024), F32), vmem((32, 256), BF),
        vmem((8, 128, 256), BF), vmem((128, 384), F32),
        dma(21), dma(2),
        one, one, one, one, one, one, one, one, one, dma(8), one, one,
        one, dma(2, 4), one, one, one, dma(4), one, dma(4),
        one, one, one, dma(8), dma(2), one, one, dma(4), one, dma(4), one, one, one, one,
    ]
    hbm = pl.BlockSpec(memory_space=pltpu.HBM)
    final, new_state = pl.pallas_call(
        step_kernel,
        out_shape=(
            jax.ShapeDtypeStruct((32, 256), BF),
            jax.ShapeDtypeStruct((32, 1, 128, 128), F32),
        ),
        in_specs=[hbm] * 21,
        out_specs=(hbm, hbm),
        scratch_shapes=scratch,
        compiler_params=pltpu.CompilerParams(
            collective_id=0, has_side_effects=True, vmem_limit_bytes=63200 * 1024
        ),
    )(*args, inv)
    return pl.pallas_call(
        hand_out,
        out_shape=(
            jax.ShapeDtypeStruct((32, 256), BF),
            jax.ShapeDtypeStruct((32, 1, 128, 128), F32),
        ),
        in_specs=[hbm, hbm],
        out_specs=(hbm, hbm),
        scratch_shapes=[vmem((32, 256), BF), vmem((32, 1, 128, 128), F32), dma(9), dma(9)],
        compiler_params=pltpu.CompilerParams(vmem_limit_bytes=63200 * 1024),
    )(final, new_state)


def solution(mesh):
    in_specs = (
        P("ep", None), P(), P(None, "tp"), P(None, "tp"), P(None, "tp"), P(None, "tp"), P("tp"),
        P("tp", None), P("ep", "tp", None, None), P("ep"), P(), P(), P("tp", "ep"), P("tp", "ep"),
        P("ep", "tp"), P("ep", None), P("ep", None), P("ep", None, "tp"), P("ep", None, "tp"),
        P("ep", "tp", None),
    )
    out_specs = (P("ep", "tp"), P("ep", "tp", None, None))
    return jax.shard_map(per_device, mesh=mesh, in_specs=in_specs, out_specs=out_specs, check_vma=False)
```

```python
import numpy as np
import jax
import jax.numpy as jnp
from jax import lax
from jax.experimental import pallas as pl
from jax.experimental.pallas import tpu as pltpu
from jax.sharding import PartitionSpec as P

EPSILON = 1e-06
THETA = 10000.0
BF = jnp.bfloat16
F32 = jnp.float32
NZ, NX, NT, NE = 8, 4, 8, 32


def iota(shape, dim):
    return lax.broadcasted_iota(jnp.int32, shape, dim)


def onehot(condition):
    return jnp.where(condition, 1.0, 0.0).astype(BF)


def dot(a, b):
    return jnp.dot(a, b, preferred_element_type=F32)


def dot_nt(a, b):
    return lax.dot_general(a, b, (((1,), (1,)), ((), ())), preferred_element_type=F32)


def as_column(row, n):
    return jnp.sum(jnp.where(iota((n, n), 0) == iota((n, n), 1), row, 0.0), axis=1, keepdims=True)


def as_row(column, n):
    return jnp.sum(jnp.where(iota((n, n), 0) == iota((n, n), 1), column, 0.0), axis=0, keepdims=True)


def step_kernel(
    resid_h, norm_gain_h, wq_h, wk_h, wv_h, wg_h, head_gain_h, wo_h, state_h, positions_h,
    ffn_gain_h, w_mix_h, dgate_h, dup_h, ddown_h, routes_h, rweight_h, eg_h, eu_h, ed_h, inv_h,
    final_v, new_state,
    resid, norm_gain, wqkvg, head_gain, wo, state, positions, ffn_gain, w_mix,
    routes, rweight, eg, eu, ed, inv,
    mix, rs_send, rs_recv, rr_send, rr_recv, sc_send, sc_recv, sx_send, sx_recv, rows_x, dw,
    part_y, ry_recv, my_send, yx_recv, md_send, md_recv, ag_recv, pair_send, pair_recv, er_own, er_send, er_recv, mr_send, mr_recv,
    zt_send, zt_recv, acc, rows_a, gate_up,
    load_sem,
    rs_s, rs_r, rr_s, rr_r, sc_s, sc_r, sx_s, sx_r, xz_s, xz_r, xx_s, xx_r, wy_s, wy_r, wc_s, wc_r,
    ry_s, ry_r, yx_s, yx_r,
    md_s, md_r, ag_s, ag_r, ah_r, ac_s, pair_s, pair_r, er_s, er_r, mr_s, mr_r, zt_s, zt_r,
):
    ep = lax.axis_index("ep")
    t = lax.axis_index("tp")
    z = ep // NX
    x = lax.rem(ep, NX)
    y = t // 2
    core = lax.rem(t, 2)

    def zdev(p):
        return (p * NX + x, t)

    def xdev(p):
        return (z * NX + p, t)

    def tdev(p):
        return (ep, p)

    def ydev(p):
        return (ep, 2 * p + core)

    def edev(p):
        return (p, t)

    sibling = (ep, t + 1 - 2 * core)

    scope = []

    def phase(name):
        if scope:
            scope.pop().__exit__(None, None, None)
        if name:
            scope.append(jax.named_scope(name))
            scope[0].__enter__()

    loads = {}
    pairs = [
        ("resid", resid_h, resid), ("norm_gain", norm_gain_h, norm_gain),
        ("wq", wq_h, wqkvg.at[:, 0:128]), ("wk", wk_h, wqkvg.at[:, 128:256]),
        ("wv", wv_h, wqkvg.at[:, 256:384]), ("wg", wg_h, wqkvg.at[:, 384:512]),
        ("positions", positions_h, positions), ("inv", inv_h, inv), ("head_gain", head_gain_h, head_gain),
        ("state", state_h.at[:, 0], state), ("wo", wo_h, wo),
        ("ffn_gain", ffn_gain_h, ffn_gain), ("w_mix", w_mix_h, w_mix),
        ("routes", routes_h, routes), ("rweight", rweight_h, rweight),
        ("ddown", ddown_h, dw.at[t, 0:176]), ("dgate", dgate_h, dw.at[t, 176:352]),
        ("dup", dup_h, dw.at[t, 352:528]),
        ("eg", eg_h.at[0], eg), ("eu", eu_h.at[0], eu), ("ed", ed_h.at[0], ed),
    ]
    for n, (name, src, dst) in enumerate(pairs):
        slot = 2 if name in ("wq", "wk", "wv", "wg") else n
        loads[name] = pltpu.make_async_copy(src, dst, load_sem.at[slot])
        loads[name].start()

    phase("greet")
    barrier = pltpu.get_barrier_semaphore()

    def greet(dev):
        pl.semaphore_signal(barrier, inc=1, device_id=dev, device_id_type=pl.DeviceIdType.MESH)

    def greet_column(k, c):
        for p in range(NT):
            greet((lax.rem(z + k, NZ) * NX + x, p))
        return c

    def greet_planes(k, c):
        for n in range(1, NX):
            greet((lax.rem(z + k, NZ) * NX + lax.rem(x + n, NX), t))
        return c

    def greet_group(k, c):
        greet(tdev(lax.rem(t + k, NT)))
        return c

    lax.fori_loop(NZ // 2, NZ, greet_column, 0)
    lax.fori_loop(NZ // 2, NZ, greet_planes, 0)
    lax.fori_loop(1, NZ // 2, greet_column, 0)
    lax.fori_loop(0, NZ // 2, greet_planes, 0)
    lax.fori_loop(1, NT, greet_group, 0)

    def need(*names):
        for name in names:
            loads[name].wait()

    def remote(src, dst, ssem, rsem, dev):
        return pltpu.make_async_remote_copy(
            src_ref=src, dst_ref=dst, send_sem=ssem, recv_sem=rsem, device_id=dev,
            device_id_type=pl.DeviceIdType.MESH,
        )

    def send_all(n, me, dev, src_at, dst_here, ssem, rsem):
        def one(k, c):
            p = lax.rem(me + k, n)
            remote(src_at(p), dst_here, ssem, rsem, dev(p)).start()
            return c
        lax.fori_loop(1, n, one, 0)

    def arrived_all(block, ssem, rsem):
        remote(block, block, ssem, rsem, sibling).wait_recv()

    def sent_all(block, ssem, rsem):
        remote(block, block, ssem, rsem, sibling).wait_send()

    phase("retention")
    need("resid", "norm_gain")
    res = resid[...].astype(F32)
    ms = jnp.mean(res * res, axis=-1, keepdims=True)
    gain_in = norm_gain[...].reshape(1, 2048).astype(F32)
    normed_in = (res * lax.rsqrt(ms + EPSILON) * gain_in).astype(BF)
    need("positions", "inv")
    pltpu.make_async_copy(wqkvg, wqkvg, load_sem.at[2]).wait()
    angles = as_column(positions[...].astype(F32).reshape(1, 32), 32) * inv[...]
    cosine, sine = jnp.cos(angles), jnp.sin(angles)
    cos2 = jnp.concatenate([cosine, cosine], axis=-1)
    sin2 = jnp.concatenate([-sine, sine], axis=-1)
    qkvg = dot(normed_in, wqkvg[...]).astype(BF).astype(F32)

    def rotate(v):
        return v * cos2 + pltpu.roll(v, 64, 1) * sin2

    query = rotate(qkvg[:, 0:128])
    key = rotate(qkvg[:, 128:256]) * (128 ** -0.5)
    value = qkvg[:, 256:384]
    gating = qkvg[:, 384:512]
    decay = 1.0 - jnp.exp2(-1.0 - 1.5 * jnp.full((1, 128), t, jnp.int32).astype(F32))
    within = jnp.sum(query * key, axis=-1, keepdims=True) * value
    query_t = jnp.transpose(query)
    phase("state")
    need("state")
    for s in range(32):
        mix[s : s + 1, :] = jnp.sum(state[s] * query_t[:, s : s + 1], axis=0, keepdims=True)
    phase("head_out")
    need("head_gain", "wo")
    mixture = within + mix[...] * decay
    centre = jnp.mean(mixture, axis=-1, keepdims=True)
    spread = jnp.mean(jnp.square(mixture - centre), axis=-1, keepdims=True)
    normed = (mixture - centre) * lax.rsqrt(spread + EPSILON)
    normed = normed * head_gain[...].reshape(1, 128).astype(F32)
    retained = (jax.nn.silu(gating) * normed).astype(BF)
    partial = dot(retained, wo[...])
    for p in range(NT):
        rs_send[p] = partial[:, 256 * p : 256 * (p + 1)].astype(BF)
    for p in range(NT):
        tile = [partial[4 * p : 4 * p + 4, 512 * q : 512 * (q + 1)] for q in range(4)]
        rr_send[p] = jnp.concatenate(tile, axis=0).astype(BF)

    phase("barrier")
    pl.semaphore_wait(barrier, NZ * NT - 1 + NZ * (NX - 1))

    phase("rs_send")
    send_all(NT, t, tdev, lambda p: rs_send.at[p], rs_recv.at[t], rs_s, rs_r)
    send_all(NT, t, tdev, lambda p: rr_send.at[p], rr_recv.at[t], rr_s, rr_r)
    rs_recv[t] = rs_send[t]
    rr_recv[t] = rr_send[t]

    need("ddown", "dgate", "dup")
    ahead, behind = lax.rem(y + 1, 4), lax.rem(y + 3, 4)
    onward = lax.rem(y + 1 + 2 * core, 4)
    origin = lax.rem(y + 3 + 2 * core, 4)
    across = lax.rem(y + 2, 4)
    parts = (pl.ds(272, 256), pl.ds(0, 272))

    def weights_to_y(h, owner, target):
        block = dw.at[2 * owner + core, parts[h]]
        return remote(block, block, wy_s, wy_r.at[h, owner], ydev(target))

    def weights_to_sibling(h, owner):
        block = dw.at[2 * owner + core, parts[h]]
        return remote(block, block, wc_s, wc_r, sibling)

    weights_to_y(0, y, ahead).start()
    weights_to_y(0, y, behind).start()
    for h in range(2):
        weights_to_sibling(h, y).start()

    key_t = jnp.transpose(key)
    for s in range(32):
        new_state[s, 0] = state[s] * decay + key_t[:, s : s + 1] * value[s : s + 1, :]

    need("routes", "rweight", "ffn_gain", "w_mix")
    ids = jnp.transpose(routes[...].astype(F32))
    rw = jnp.transpose(rweight[...].astype(F32))
    lane_e = iota((32, 32), 1).astype(F32)
    hit0, hit1 = (lane_e == ids[:, 0:1]), (lane_e == ids[:, 1:2])
    both = jnp.where(hit0, 1.0, 0.0) + jnp.where(hit1, 1.0, 0.0)
    earlier = onehot(iota((32, 32), 1) < iota((32, 32), 0))
    rank = dot(earlier, both.astype(BF))
    weight_e = jnp.where(hit0, rw[:, 0:1], 0.0) + jnp.where(hit1, rw[:, 1:2], 0.0)
    lane = iota((32, 256), 1)
    widen = onehot((lane >> 3) == iota((32, 256), 0))
    slot = (lane & 3).astype(F32)
    taken = dot(both.astype(BF), widen) * jnp.where(dot(rank.astype(BF), widen) == slot, 1.0, 0.0)
    weighted = dot(weight_e.astype(BF), widen) * taken
    halves = [((lane >> 2) & 1) == h for h in range(2)]
    dispatch = [jnp.transpose(jnp.where(halves[h], taken, 0.0)).astype(BF) for h in range(2)]
    combine = [jnp.where(halves[h], weighted, 0.0).astype(BF) for h in range(2)]
    up_row, up_col = iota((128, 256), 0), iota((128, 256), 1)
    unpack = [onehot(up_col == (up_row >> 2) * 8 + 4 * h + (up_row & 3)) for h in range(2)]
    pk_row, pk_col = iota((256, 128), 0), iota((256, 128), 1)
    pack = [onehot(pk_row == (pk_col >> 2) * 8 + 4 * h + (pk_col & 3)) for h in range(2)]
    for p in range(NT):
        dw[p, 528:560, :] = jnp.zeros((32, 256), BF)
    gain_mid = ffn_gain[...].reshape(1, 2048).astype(F32)
    gain_here = gain_mid[:, 0:256]
    for p in range(1, NT):
        gain_here = jnp.where(t == p, gain_mid[:, 256 * p : 256 * (p + 1)], gain_here)
    mixer = w_mix[...].reshape(1, 2048).astype(F32)

    def as_tile(row):
        return jnp.concatenate(
            [jnp.broadcast_to(row[:, 512 * q : 512 * (q + 1)], (4, 512)) for q in range(4)], axis=0
        )

    gain_tile, mixer_tile = as_tile(gain_mid), as_tile(mixer)
    pick_row, pick_col = iota((16, 32), 0), iota((16, 32), 1)
    resid_tile = jnp.zeros((16, 512), F32)
    for q in range(4):
        pick = onehot((pick_col == 4 * t + (pick_row & 3)) & ((pick_row >> 2) == q))
        resid_tile = resid_tile + dot(pick, resid[:, 512 * q : 512 * (q + 1)])

    phase("rs_wait")
    arrived_all(rs_recv.at[0:7], rs_s, rs_r)
    phase("middle")
    columns = pl.ds(pl.multiple_of(t * 256, 256), 256)
    attention = rs_recv[0].astype(F32)
    for p in range(1, NT):
        attention = attention + rs_recv[p].astype(F32)
    middle = resid[:, columns].astype(F32) + attention
    scaled = (middle * gain_here).astype(BF)
    outgoing = dot(dispatch[0], scaled[:, 0:128]) + dot(dispatch[1], scaled[:, 128:256])
    md_send[...] = outgoing.astype(BF).reshape(NE, 8, 128)

    def spread_out(src_at, dst_here, ssem, rsem):
        def to(p):
            remote(src_at(p), dst_here, ssem, rsem, edev(p)).start()

        def one(k, c):
            for n in range(NX):
                to(lax.rem(z + k, NZ) * NX + n)
            return c
        lax.fori_loop(NZ // 2, NZ, one, 0)
        lax.fori_loop(1, NZ // 2, one, 0)
        for n in range(1, NX):
            to(z * NX + lax.rem(x + n, NX))

    spread_out(lambda p: md_send.at[p], md_recv.at[ep], md_s, md_r)
    md_recv[ep] = md_send[ep]

    phase("rr_wait")
    arrived_all(rr_recv.at[0:7], rr_s, rr_r)
    middle_tile = rr_recv[0].astype(F32)
    for p in range(1, NT):
        middle_tile = middle_tile + rr_recv[p].astype(F32)
    middle_tile = middle_tile + resid_tile

    def over_quarters(column):
        total = column[0:4] + column[4:8] + column[8:12] + column[12:16]
        return jnp.concatenate([total] * 4, axis=0)

    squares = over_quarters(jnp.sum(middle_tile * middle_tile, axis=-1, keepdims=True))
    scale_tile = lax.rsqrt(squares * (1.0 / 2048) + EPSILON)
    normed_tile = (middle_tile * scale_tile * gain_tile).astype(BF)
    mixing16 = jax.nn.sigmoid(
        over_quarters(jnp.sum(normed_tile.astype(F32) * mixer_tile, axis=-1, keepdims=True))
    )
    rows_x[x, z] = normed_tile
    send_all(NZ, z, zdev, lambda p: rows_x.at[x, z], rows_x.at[x, z], xz_s, xz_r.at[z])

    def to_x(zz):
        send_all(NX, x, xdev, lambda p: rows_x.at[x, zz], rows_x.at[x, zz], xx_s, xx_r)

    to_x(z)

    lane4, row4 = iota((4, 128), 1), iota((4, 128), 0)
    both_factors = jnp.where(lane4 == row4, scale_tile[0:4], 0.0) + jnp.where(lane4 == row4 + 4, mixing16[0:4], 0.0)
    sc_send[...] = jnp.sum(both_factors, axis=0, keepdims=True)
    send_all(NT, t, tdev, lambda p: sc_send, sc_recv.at[t], sc_s, sc_r)
    sc_recv[t] = sc_send[...]
    weights_to_y(1, y, ahead).start()
    weights_to_y(1, y, behind).start()

    def relay(h):
        weights_to_y(h, origin, onward).wait_recv()
        weights_to_y(h, origin, onward).start()
        weights_to_sibling(h, origin).start()

    phase("relay_a")
    relay(0)

    phase("xz_near")

    def pass_on(n, c):
        d = n // 2 + 1
        p = lax.rem(z + d + lax.rem(n, 2) * (NZ - 2 * d), NZ)
        remote(rows_x.at[x, p], rows_x.at[x, p], xz_s, xz_r.at[p], zdev(p)).wait_recv()
        to_x(p)
        return c
    lax.fori_loop(0, 2, pass_on, 0)

    phase("md_wait")
    arrived_all(md_recv.at[0:31], md_s, md_r)
    arrived = md_recv[...].reshape(256, 128)
    ag_recv[t] = jnp.concatenate([dot(unpack[h], arrived) for h in range(2)], axis=1).astype(BF)
    own_rows = ag_recv.at[t]

    halves_of = (pl.ds(0, 64), pl.ds(64, 64))
    for h in range(2):
        block = ag_recv.at[t, halves_of[h]]
        remote(block, block, ag_s, ah_r.at[h], ydev(onward)).start()
    remote(own_rows, own_rows, ag_s, ag_r.at[t], ydev(origin)).start()
    remote(own_rows, own_rows, ac_s, ag_r.at[t], sibling).start()

    phase("xz_wait")
    lax.fori_loop(2, NZ - 1, pass_on, 0)

    phase("relay_b")
    relay(1)

    phase("sc_wait")
    arrived_all(sc_recv.at[0:7], sc_s, sc_r)
    factors = jnp.concatenate([jnp.broadcast_to(sc_recv[p], (4, 128)) for p in range(NT)], axis=0)
    fac_lane, fac_row = iota((32, 128), 1), iota((32, 128), 0) & 3
    mixing = jnp.sum(jnp.where(fac_lane == fac_row + 4, factors, 0.0), axis=1, keepdims=True)
    factors = jnp.sum(jnp.where(fac_lane == fac_row, factors, 0.0), axis=1, keepdims=True)
    sx_send[...] = jnp.sum(taken * factors, axis=0, keepdims=True)
    spread_out(lambda p: sx_send, sx_recv.at[ep], sx_s, sx_r)
    sx_recv[ep] = sx_send[...]

    need("eg", "eu", "ed")

    def chunk(p):
        depth = pl.ds(pl.multiple_of(p * 256, 256), 256)
        rows_p = ag_recv[p]
        acc[:, 0:512] += dot(rows_p, eg[depth, :])
        acc[:, 512:1024] += dot(rows_p, eu[depth, :])

    acc[...] = jnp.zeros_like(acc)

    def group_rows(p, ssem, dev):
        block = ag_recv.at[2 * p + core]
        return remote(block, block, ssem, ag_r.at[2 * p + core], dev)

    def direct_chunk(p):
        group_rows(p, ag_s, ydev(p)).wait_recv()
        group_rows(p, ac_s, sibling).start()

    def other_chunk(p):
        block = ag_recv.at[2 * p + 1 - core]
        remote(block, block, ac_s, ag_r.at[2 * p + 1 - core], sibling).wait_recv()
        chunk(2 * p + 1 - core)

    chunk(t)
    other_chunk(y)
    phase("weights_on")
    for h in range(2):
        weights_to_y(h, onward, onward).wait_recv()
        weights_to_sibling(h, onward).start()
    phase("chunks")
    for h in range(2):
        block = ag_recv.at[2 * origin + core, halves_of[h]]
        remote(block, block, ag_s, ah_r.at[h], ydev(origin)).wait_recv()
        remote(block, block, ag_s, ag_r.at[2 * origin + core], ydev(onward)).start()
    group_rows(origin, ac_s, sibling).start()
    chunk(2 * origin + core)
    direct_chunk(onward)
    chunk(2 * onward + core)
    other_chunk(onward)
    other_chunk(origin)
    phase("weights_across")
    for h in range(2):
        weights_to_y(h, across, onward).wait_recv()
        weights_to_sibling(h, across).start()
    phase("ag_across")
    direct_chunk(across)
    phase("xx_wait")
    arrived_all(rows_x.at[0:3], xx_s, xx_r)
    phase("dense_a")
    tiles = rows_x[...].reshape(512, 512)
    spread_row = iota((128, 512), 0)
    spread_col = iota((128, 512), 1)
    for q in range(4):
        take = onehot(spread_col == (spread_row >> 2) * 16 + 4 * q + (spread_row & 3))
        block = dot(take, tiles).astype(BF)
        rows_a[2 * q] = block[:, 0:256]
        rows_a[2 * q + 1] = block[:, 256:512]

    def gate_up_by(side):
        total = jnp.zeros((128, 384), F32)
        for p in range(4):
            n = 2 * p + side
            total = total + dot_nt(rows_a[n], dw[n, 176:560])
        return total

    gate_up[...] = gate_up_by(core)
    phase("weights_wait")
    arrived_all(dw.at[0:4, 0:528], wc_s, wc_r)
    phase("dense_mm")
    both_sums = gate_up[...] + gate_up_by(1 - core)
    up = pltpu.roll(both_sums, 384 - 176, 1)
    hidden = jnp.where(iota((128, 256), 1) < 176, jax.nn.silu(both_sums[:, 0:256]) * up[:, 0:256], 0.0).astype(BF)
    x_on, x_back, x_across = lax.rem(x + 1 + 2 * core, 4), lax.rem(x + 3 + 2 * core, 4), lax.rem(x + 2, 4)

    def y_across(q):
        return remote(part_y.at[q, x_across], ry_recv.at[q], ry_s, ry_r.at[q], xdev(x_on))

    def y_back(q):
        return remote(part_y.at[q, x_back], yx_recv.at[1, q], yx_s, yx_r.at[q], xdev(x_back))

    def y_on(q):
        return remote(my_send.at[q], yx_recv.at[0, q], yx_s, yx_r.at[q], xdev(x_on))

    for q in range(4):
        for n in range(2):
            part = dot(hidden, dw[2 * q + n, 0:256]).astype(BF)
            part_y[q, :, :, 256 * n : 256 * (n + 1)] = part.reshape(NX, 32, 256)
        y_across(q).start()
        y_back(q).start()

    def merge_on():
        for q in range(4):
            y_across(q).wait_recv()
            my_send[q] = (part_y[q, x_on].astype(F32) + ry_recv[q].astype(F32)).astype(BF)
            y_on(q).start()

    phase("last_chunk")
    chunk(2 * across + core)
    other_chunk(across)
    phase("down")
    arrived_all(sx_recv.at[0:31], sx_s, sx_r)
    every = jnp.concatenate([sx_recv[p] for p in range(NE)], axis=0)
    repeat = jnp.where((iota((128, 32), 0) >> 2) == iota((128, 32), 1), 1.0, 0.0)
    every = jnp.dot(repeat, every, preferred_element_type=F32, precision=lax.Precision.HIGHEST)
    wanted = iota((128, 256), 1) == 8 * ep + (iota((128, 256), 0) & 3)
    factor = jnp.sum(jnp.where(wanted, every, 0.0), axis=1, keepdims=True)
    hidden_e = (jax.nn.silu(acc[:, 0:512] * factor) * (acc[:, 512:1024] * factor)).astype(BF)

    def down_tile(p):
        return dot(hidden_e, ed[:, pl.ds(pl.multiple_of(p * 256, 256), 256)])

    for p in (across, onward, y, origin):
        pair_send[p] = down_tile(2 * p + 1 - core).astype(BF)
        remote(pair_send.at[p], pair_recv.at[p], pair_s, pair_r.at[p], sibling).start()

    def pair_sum(p):
        own = down_tile(2 * p + core)
        remote(pair_send.at[p], pair_recv.at[p], pair_s, pair_r.at[p], sibling).wait_recv()
        return own + pair_recv[p].astype(F32)

    def group_to(p, target, slot, h, sem):
        part = pl.ds(64 * h, 64)
        return remote(er_send.at[p, part], er_recv.at[slot, part], er_s, er_r.at[sem], ydev(target))

    er_send[across] = pair_sum(across).astype(BF)
    for h in range(2):
        group_to(across, onward, 0, h, h).start()
    er_send[origin] = pair_sum(origin).astype(BF)
    for h in range(2):
        group_to(origin, origin, 1, h, 2).start()
    er_own[y] = pair_sum(y)
    er_own[onward] = pair_sum(onward)

    def group_merge():
        for h in range(2):
            group_to(across, onward, 0, h, h).wait_recv()
            part = pl.ds(64 * h, 64)
            er_send[onward, part] = (er_own[onward, part] + er_recv[0, part].astype(F32)).astype(BF)
            group_to(onward, onward, 2, h, 3).start()

    phase("merge_on")
    merge_on()
    phase("group_merge")
    group_merge()
    phase("yx_wait")
    zs_row, zs_col = iota((64, 32), 0), iota((64, 32), 1)
    to_half = [onehot(zs_row == (zs_col >> 2) * 8 + 4 * h + (zs_col & 3)) for h in range(2)]

    def to_column(p, n):
        remote(zt_send.at[p, n], zt_recv.at[z * NT + t], zt_s, zt_r, (p * NX + x, n)).start()

    for q in range(4):
        arrived_all(yx_recv.at[:, q], yx_s, yx_r.at[q])
        summed = part_y[q, x].astype(F32) + yx_recv[0, q].astype(F32) + yx_recv[1, q].astype(F32)
        summed = summed.astype(BF)
        low, high = dot(to_half[0], summed), dot(to_half[1], summed)
        for n in range(2):
            tile = low[:, 256 * n : 256 * n + 128] + high[:, 256 * n + 128 : 256 * n + 256]
            zt_send[:, 2 * q + n] = tile.astype(BF).reshape(NZ, 8, 128)

        def column_out(k, c, q=q):
            for n in range(2):
                to_column(lax.rem(z + k, NZ), 2 * q + n)
            return c
        lax.fori_loop(NZ // 2, NZ, column_out, 0)
        lax.fori_loop(1, NZ // 2, column_out, 0)

    def group_out(k, c):
        to_column(z, lax.rem(t + k, NT))
        return c
    lax.fori_loop(1, NT, group_out, 0)
    zt_recv[z * NT + t] = zt_send[z, t]

    phase("drain_early")
    sent_all(rs_recv.at[0:7], rs_s, rs_r)
    sent_all(rr_recv.at[0:7], rr_s, rr_r)
    sent_all(sc_recv.at[0:7], sc_s, sc_r)
    sent_all(sx_recv.at[0:31], sx_s, sx_r)
    sent_all(md_recv.at[0:31], md_s, md_r)
    sent_all(rows_x.at[0, 0:7], xz_s, xz_r.at[0])

    sent_all(rows_x.at[0:3], xx_s, xx_r)
    sent_all(dw.at[0:3, 0:528], wy_s, wy_r.at[0, 0])
    sent_all(dw.at[0:4, 0:528], wc_s, wc_r)
    sent_all(ry_recv, ry_s, ry_r.at[0])
    sent_all(yx_recv, yx_s, yx_r.at[0])
    sent_all(ag_recv.at[0:3], ag_s, ag_r.at[0])
    sent_all(ag_recv.at[0:4], ac_s, ag_r.at[0])
    sent_all(pair_send, pair_s, pair_r.at[0])

    phase("er_wait")
    arrived_all(er_recv.at[1], er_s, er_r.at[2])
    arrived_all(er_recv.at[2], er_s, er_r.at[3])
    result = (er_own[y] + er_recv[1].astype(F32) + er_recv[2].astype(F32)).astype(BF)
    mr_send[...] = (dot(pack[0], result[:, 0:128]) + dot(pack[1], result[:, 128:256])).astype(BF).reshape(NE, 8, 128)
    spread_out(lambda p: mr_send.at[p], mr_recv.at[ep], mr_s, mr_r)
    mr_recv[ep] = mr_send[ep]

    phase("zt_wait")
    un_row, un_col = iota((32, 512), 0), iota((32, 512), 1)
    un_token = ((un_col >> 3) & 7) * 4 + (un_col & 3)
    gather = [onehot((un_token == un_row) & (((un_col >> 2) & 1) == h)) for h in range(2)]
    sent_all(er_recv.at[0:3], er_s, er_r.at[0])
    arrived_all(zt_recv.at[0:63], zt_s, zt_r)
    columns_in = zt_recv[...].reshape(512, 128)
    dense_rows = jnp.concatenate([dot(gather[h], columns_in) for h in range(2)], axis=1) * mixing
    phase("mr_wait")
    arrived_all(mr_recv.at[0:31], mr_s, mr_r)
    returned = mr_recv[...].reshape(256, 128)
    phase("final")
    moe = jnp.concatenate([dot(combine[h], returned) for h in range(2)], axis=1)
    final_v[...] = (middle + moe + dense_rows).astype(BF)

    phase("drain")
    sent_all(zt_recv.at[0:63], zt_s, zt_r)
    sent_all(mr_recv.at[0:31], mr_s, mr_r)
    phase(None)


def hand_out(final_v, state_v, final_out, state_out, sem):
    copies = [pltpu.make_async_copy(final_v, final_out, sem.at[8])]
    for n in range(8):
        part = pl.ds(4 * n, 4)
        copies.append(pltpu.make_async_copy(state_v.at[part], state_out.at[part], sem.at[n]))
    for copy in copies:
        copy.start()
    for copy in copies:
        copy.wait()


def per_device(*args):
    args = list(args)
    for n in (12, 13, 15, 16):
        args[n] = args[n].T
    inv = jnp.asarray((THETA ** (-np.arange(64) / 64.0)).astype(np.float32)[None, :])
    vmem = pltpu.VMEM

    def dma(*shape):
        return pltpu.SemaphoreType.DMA(shape)

    one = pltpu.SemaphoreType.DMA

    scratch = [
        vmem((32, 2048), BF), vmem((2048,), BF), vmem((2048, 512), BF), vmem((128,), BF),
        vmem((128, 2048), BF), vmem((32, 128, 128), F32), vmem((32,), jnp.int32), vmem((2048,), BF),
        vmem((2048,), BF), vmem((2, 32), jnp.int32), vmem((2, 32), BF),
        vmem((2048, 512), BF), vmem((2048, 512), BF), vmem((512, 2048), BF), vmem((1, 64), F32),
        vmem((32, 128), F32), vmem((8, 32, 256), BF), vmem((8, 32, 256), BF),
        vmem((8, 16, 512), BF), vmem((8, 16, 512), BF), vmem((1, 128), F32), vmem((8, 1, 128), F32),
        vmem((1, 256), F32), vmem((32, 1, 256), F32), vmem((4, 8, 16, 512), BF), vmem((8, 560, 256), BF),
        vmem((4, 4, 32, 512), BF), vmem((4, 32, 512), BF), vmem((4, 32, 512), BF), vmem((2, 4, 32, 512), BF),
        vmem((32, 8, 128), BF), vmem((32, 8, 128), BF), vmem((8, 128, 256), BF),
        vmem((4, 128, 256), BF), vmem((4, 128, 256), BF), vmem((4, 128, 256), F32),
        vmem((4, 128, 256), BF), vmem((4, 128, 256), BF), vmem((32, 8, 128), BF), vmem((32, 8, 128), BF),
        vmem((8, 8, 8, 128), BF), vmem((64, 8, 128), BF), vmem((128, 1024), F32),
        vmem((8, 128, 256), BF), vmem((128, 384), F32),
        dma(21),
        one, one, one, one, one, one, one, one, one, dma(8), one, one,
        one, dma(2, 4), one, one, one, dma(4), one, dma(4),
        one, one, one, dma(8), dma(2), one, one, dma(4), one, dma(4), one, one, one, one,
    ]
    hbm = pl.BlockSpec(memory_space=pltpu.HBM)
    here = pl.BlockSpec(memory_space=pltpu.VMEM)
    args = [pltpu.with_memory_space_constraint(a, pltpu.HBM) for a in args]
    inv = pltpu.with_memory_space_constraint(inv, pltpu.HBM)
    final, new_state = pl.pallas_call(
        step_kernel,
        out_shape=(
            jax.ShapeDtypeStruct((32, 256), BF),
            jax.ShapeDtypeStruct((32, 1, 128, 128), F32),
        ),
        in_specs=[hbm] * 21,
        out_specs=(here, here),
        scratch_shapes=scratch,
        compiler_params=pltpu.CompilerParams(
            collective_id=0, has_side_effects=True, vmem_limit_bytes=50000 * 1024
        ),
    )(*args, inv)
    return pl.pallas_call(
        hand_out,
        out_shape=(
            jax.ShapeDtypeStruct((32, 256), BF),
            jax.ShapeDtypeStruct((32, 1, 128, 128), F32),
        ),
        in_specs=[here, here],
        out_specs=(hbm, hbm),
        scratch_shapes=[dma(9)],
        compiler_params=pltpu.CompilerParams(vmem_limit_bytes=16384 * 1024),
    )(final, new_state)


def solution(mesh):
    in_specs = (
        P("ep", None), P(), P(None, "tp"), P(None, "tp"), P(None, "tp"), P(None, "tp"), P("tp"),
        P("tp", None), P("ep", "tp", None, None), P("ep"), P(), P(), P("tp", "ep"), P("tp", "ep"),
        P("ep", "tp"), P("ep", None), P("ep", None), P("ep", None, "tp"), P("ep", None, "tp"),
        P("ep", "tp", None),
    )
    out_specs = (P("ep", "tp"), P("ep", "tp", None, None))
    return jax.shard_map(per_device, mesh=mesh, in_specs=in_specs, out_specs=out_specs, check_vma=False)
```

```python
import numpy as np
import jax
import jax.numpy as jnp
from jax import lax
from jax.experimental import pallas as pl
from jax.experimental.pallas import tpu as pltpu
from jax.sharding import PartitionSpec as P

EPSILON = 1e-06
THETA = 10000.0
BF = jnp.bfloat16
F32 = jnp.float32
NZ, NX, NT, NE = 8, 4, 8, 32


def iota(shape, dim):
    return lax.broadcasted_iota(jnp.int32, shape, dim)


def onehot(condition):
    return jnp.where(condition, 1.0, 0.0).astype(BF)


def dot(a, b):
    return jnp.dot(a, b, preferred_element_type=F32)


def dot_nt(a, b):
    return lax.dot_general(a, b, (((1,), (1,)), ((), ())), preferred_element_type=F32)


def as_column(row, n):
    return jnp.sum(jnp.where(iota((n, n), 0) == iota((n, n), 1), row, 0.0), axis=1, keepdims=True)


def as_row(column, n):
    return jnp.sum(jnp.where(iota((n, n), 0) == iota((n, n), 1), column, 0.0), axis=0, keepdims=True)


def step_kernel(
    resid_h, norm_gain_h, wq_h, wk_h, wv_h, wg_h, head_gain_h, wo_h, state_h, positions_h,
    ffn_gain_h, w_mix_h, dgate_h, dup_h, ddown_h, routes_h, rweight_h, eg_h, eu_h, ed_h, inv_h,
    final_v, new_state,
    resid, norm_gain, wqkvg, head_gain, wo, state, positions, ffn_gain, w_mix,
    routes, rweight, eg, eu, ed, inv,
    mix, rs_send, rs_recv, rr_send, rr_recv, sc_send, sc_recv, sx_send, sx_recv, rows_x, dw,
    part_y, ry_recv, my_send, yx_recv, md_send, md_recv, ag_recv, pair_send, pair_recv, er_own, er_send, er_recv, mr_send, mr_recv,
    zt_send, zt_recv, acc, rows_a, gate_up,
    load_sem,
    rs_s, rs_r, rr_s, rr_r, sc_s, sc_r, sx_s, sx_r, xz_s, xz_r, xx_s, xx_r, wy_s, wy_r, wc_s, wc_r,
    ry_s, ry_r, yx_s, yx_r,
    md_s, md_r, ag_s, ag_r, ah_r, ac_s, pair_s, pair_r, er_s, er_r, mr_s, mr_r, zt_s, zt_r,
):
    ep = lax.axis_index("ep")
    t = lax.axis_index("tp")
    z = ep // NX
    x = lax.rem(ep, NX)
    y = t // 2
    core = lax.rem(t, 2)

    def zdev(p):
        return (p * NX + x, t)

    def xdev(p):
        return (z * NX + p, t)

    def tdev(p):
        return (ep, p)

    def ydev(p):
        return (ep, 2 * p + core)

    def edev(p):
        return (p, t)

    sibling = (ep, t + 1 - 2 * core)

    scope = []

    def phase(name):
        if scope:
            scope.pop().__exit__(None, None, None)
        if name:
            scope.append(jax.named_scope(name))
            scope[0].__enter__()

    loads = {}
    pairs = [
        ("resid", resid_h, resid), ("norm_gain", norm_gain_h, norm_gain),
        ("wq", wq_h, wqkvg.at[:, 0:128]), ("wk", wk_h, wqkvg.at[:, 128:256]),
        ("wv", wv_h, wqkvg.at[:, 256:384]), ("wg", wg_h, wqkvg.at[:, 384:512]),
        ("positions", positions_h, positions), ("inv", inv_h, inv), ("head_gain", head_gain_h, head_gain),
        ("state", state_h.at[:, 0], state), ("wo", wo_h, wo),
        ("ffn_gain", ffn_gain_h, ffn_gain), ("w_mix", w_mix_h, w_mix),
        ("routes", routes_h, routes), ("rweight", rweight_h, rweight),
        ("ddown", ddown_h, dw.at[t, 0:176]), ("dgate", dgate_h, dw.at[t, 176:352]),
        ("dup", dup_h, dw.at[t, 352:528]),
        ("eg", eg_h.at[0], eg), ("eu", eu_h.at[0], eu), ("ed", ed_h.at[0], ed),
    ]
    for n, (name, src, dst) in enumerate(pairs):
        slot = n if n < 2 else max(2, n - 3)
        loads[name] = pltpu.make_async_copy(src, dst, load_sem.at[slot])
        loads[name].start()

    phase("greet")
    barrier = pltpu.get_barrier_semaphore()

    def greet(dev):
        pl.semaphore_signal(barrier, inc=1, device_id=dev, device_id_type=pl.DeviceIdType.MESH)

    def greet_column(k, c):
        for p in range(NT):
            greet((lax.rem(z + k, NZ) * NX + x, p))
        return c

    def greet_planes(k, c):
        for n in range(1, NX):
            greet((lax.rem(z + k, NZ) * NX + lax.rem(x + n, NX), t))
        return c

    def greet_group(k, c):
        greet(tdev(lax.rem(t + k, NT)))
        return c

    lax.fori_loop(NZ // 2, NZ, greet_column, 0)
    lax.fori_loop(NZ // 2, NZ, greet_planes, 0)
    lax.fori_loop(1, NZ // 2, greet_column, 0)
    lax.fori_loop(0, NZ // 2, greet_planes, 0)
    lax.fori_loop(1, NT, greet_group, 0)

    def need(*names):
        for name in names:
            loads[name].wait()

    def remote(src, dst, ssem, rsem, dev):
        return pltpu.make_async_remote_copy(
            src_ref=src, dst_ref=dst, send_sem=ssem, recv_sem=rsem, device_id=dev,
            device_id_type=pl.DeviceIdType.MESH,
        )

    def send_all(n, me, dev, src_at, dst_here, ssem, rsem):
        def one(k, c):
            p = lax.rem(me + k, n)
            remote(src_at(p), dst_here, ssem, rsem, dev(p)).start()
            return c
        lax.fori_loop(1, n, one, 0)

    def arrived_all(block, ssem, rsem):
        remote(block, block, ssem, rsem, sibling).wait_recv()

    def sent_all(block, ssem, rsem):
        remote(block, block, ssem, rsem, sibling).wait_send()

    phase("retention")
    need("resid", "norm_gain")
    res = resid[...].astype(F32)
    ms = jnp.mean(res * res, axis=-1, keepdims=True)
    gain_in = norm_gain[...].reshape(1, 2048).astype(F32)
    normed_in = (res * lax.rsqrt(ms + EPSILON) * gain_in).astype(BF)
    need("positions", "inv")
    pltpu.make_async_copy(wqkvg, wqkvg, load_sem.at[2]).wait()
    angles = as_column(positions[...].astype(F32).reshape(1, 32), 32) * inv[...]
    cosine, sine = jnp.cos(angles), jnp.sin(angles)
    cos2 = jnp.concatenate([cosine, cosine], axis=-1)
    sin2 = jnp.concatenate([-sine, sine], axis=-1)
    qkvg = dot(normed_in, wqkvg[...]).astype(BF).astype(F32)

    def rotate(v):
        return v * cos2 + pltpu.roll(v, 64, 1) * sin2

    query = rotate(qkvg[:, 0:128])
    key = rotate(qkvg[:, 128:256]) * (128 ** -0.5)
    value = qkvg[:, 256:384]
    gating = qkvg[:, 384:512]
    decay = 1.0 - jnp.exp2(-1.0 - 1.5 * jnp.full((1, 128), t, jnp.int32).astype(F32))
    within = jnp.sum(query * key, axis=-1, keepdims=True) * value
    query_t = jnp.transpose(query)
    phase("state")
    need("state")
    for s in range(32):
        mix[s : s + 1, :] = jnp.sum(state[s] * query_t[:, s : s + 1], axis=0, keepdims=True)
    phase("head_out")
    need("head_gain", "wo")
    mixture = within + mix[...] * decay
    centre = jnp.mean(mixture, axis=-1, keepdims=True)
    spread = jnp.mean(jnp.square(mixture - centre), axis=-1, keepdims=True)
    normed = (mixture - centre) * lax.rsqrt(spread + EPSILON)
    normed = normed * head_gain[...].reshape(1, 128).astype(F32)
    retained = (jax.nn.silu(gating) * normed).astype(BF)
    partial = dot(retained, wo[...])
    for p in range(NT):
        rs_send[p] = partial[:, 256 * p : 256 * (p + 1)].astype(BF)
    phase("barrier")
    pl.semaphore_wait(barrier, NZ * NT - 1 + NZ * (NX - 1))

    phase("rs_send")
    send_all(NT, t, tdev, lambda p: rs_send.at[p], rs_recv.at[t], rs_s, rs_r)
    for p in range(NT):
        tile = [partial[4 * p : 4 * p + 4, 512 * q : 512 * (q + 1)] for q in range(4)]
        rr_send[p] = jnp.concatenate(tile, axis=0).astype(BF)
    send_all(NT, t, tdev, lambda p: rr_send.at[p], rr_recv.at[t], rr_s, rr_r)
    rs_recv[t] = rs_send[t]
    rr_recv[t] = rr_send[t]

    need("ddown", "dgate", "dup")
    ahead, behind = lax.rem(y + 1, 4), lax.rem(y + 3, 4)
    onward = lax.rem(y + 1 + 2 * core, 4)
    origin = lax.rem(y + 3 + 2 * core, 4)
    across = lax.rem(y + 2, 4)
    parts = (pl.ds(272, 256), pl.ds(0, 272))

    def weights_to_y(h, owner, target):
        block = dw.at[2 * owner + core, parts[h]]
        return remote(block, block, wy_s, wy_r.at[h, owner], ydev(target))

    def weights_to_sibling(h, owner):
        block = dw.at[2 * owner + core, parts[h]]
        return remote(block, block, wc_s, wc_r, sibling)

    weights_to_y(0, y, ahead).start()
    weights_to_y(0, y, behind).start()
    for h in range(2):
        weights_to_sibling(h, y).start()

    key_t = jnp.transpose(key)
    for s in range(32):
        new_state[s, 0] = state[s] * decay + key_t[:, s : s + 1] * value[s : s + 1, :]

    need("routes", "rweight", "ffn_gain", "w_mix")
    ids = jnp.transpose(routes[...].astype(F32))
    rw = jnp.transpose(rweight[...].astype(F32))
    lane_e = iota((32, 32), 1).astype(F32)
    hit0, hit1 = (lane_e == ids[:, 0:1]), (lane_e == ids[:, 1:2])
    both = jnp.where(hit0, 1.0, 0.0) + jnp.where(hit1, 1.0, 0.0)
    earlier = onehot(iota((32, 32), 1) < iota((32, 32), 0))
    rank = dot(earlier, both.astype(BF))
    weight_e = jnp.where(hit0, rw[:, 0:1], 0.0) + jnp.where(hit1, rw[:, 1:2], 0.0)
    lane = iota((32, 256), 1)
    widen = onehot((lane >> 3) == iota((32, 256), 0))
    slot = (lane & 3).astype(F32)
    taken = dot(both.astype(BF), widen) * jnp.where(dot(rank.astype(BF), widen) == slot, 1.0, 0.0)
    weighted = dot(weight_e.astype(BF), widen) * taken
    halves = [((lane >> 2) & 1) == h for h in range(2)]
    dispatch = [jnp.transpose(jnp.where(halves[h], taken, 0.0)).astype(BF) for h in range(2)]
    combine = [jnp.where(halves[h], weighted, 0.0).astype(BF) for h in range(2)]
    up_row, up_col = iota((128, 256), 0), iota((128, 256), 1)
    unpack = [onehot(up_col == (up_row >> 2) * 8 + 4 * h + (up_row & 3)) for h in range(2)]
    pk_row, pk_col = iota((256, 128), 0), iota((256, 128), 1)
    pack = [onehot(pk_row == (pk_col >> 2) * 8 + 4 * h + (pk_col & 3)) for h in range(2)]
    for p in range(NT):
        dw[p, 528:560, :] = jnp.zeros((32, 256), BF)
    gain_mid = ffn_gain[...].reshape(1, 2048).astype(F32)
    gain_here = gain_mid[:, 0:256]
    for p in range(1, NT):
        gain_here = jnp.where(t == p, gain_mid[:, 256 * p : 256 * (p + 1)], gain_here)
    mixer = w_mix[...].reshape(1, 2048).astype(F32)

    def as_tile(row):
        return jnp.concatenate(
            [jnp.broadcast_to(row[:, 512 * q : 512 * (q + 1)], (4, 512)) for q in range(4)], axis=0
        )

    gain_tile, mixer_tile = as_tile(gain_mid), as_tile(mixer)
    pick_row, pick_col = iota((16, 32), 0), iota((16, 32), 1)
    resid_tile = jnp.zeros((16, 512), F32)
    for q in range(4):
        pick = onehot((pick_col == 4 * t + (pick_row & 3)) & ((pick_row >> 2) == q))
        resid_tile = resid_tile + dot(pick, resid[:, 512 * q : 512 * (q + 1)])

    phase("rs_wait")
    arrived_all(rs_recv.at[0:7], rs_s, rs_r)
    phase("middle")
    columns = pl.ds(pl.multiple_of(t * 256, 256), 256)
    attention = rs_recv[0].astype(F32)
    for p in range(1, NT):
        attention = attention + rs_recv[p].astype(F32)
    middle = resid[:, columns].astype(F32) + attention
    scaled = (middle * gain_here).astype(BF)
    outgoing = dot(dispatch[0], scaled[:, 0:128]) + dot(dispatch[1], scaled[:, 128:256])
    md_send[...] = outgoing.astype(BF).reshape(NE, 8, 128)

    def spread_out(src_at, dst_here, ssem, rsem):
        def to(p):
            remote(src_at(p), dst_here, ssem, rsem, edev(p)).start()

        def one(k, c):
            for n in range(NX):
                to(lax.rem(z + k, NZ) * NX + n)
            return c
        lax.fori_loop(NZ // 2, NZ, one, 0)
        lax.fori_loop(1, NZ // 2, one, 0)
        for n in range(1, NX):
            to(z * NX + lax.rem(x + n, NX))

    spread_out(lambda p: md_send.at[p], md_recv.at[ep], md_s, md_r)
    md_recv[ep] = md_send[ep]

    phase("rr_wait")
    arrived_all(rr_recv.at[0:7], rr_s, rr_r)
    middle_tile = rr_recv[0].astype(F32)
    for p in range(1, NT):
        middle_tile = middle_tile + rr_recv[p].astype(F32)
    middle_tile = middle_tile + resid_tile

    def over_quarters(column):
        total = column[0:4] + column[4:8] + column[8:12] + column[12:16]
        return jnp.concatenate([total] * 4, axis=0)

    squares = over_quarters(jnp.sum(middle_tile * middle_tile, axis=-1, keepdims=True))
    scale_tile = lax.rsqrt(squares * (1.0 / 2048) + EPSILON)
    normed_tile = (middle_tile * scale_tile * gain_tile).astype(BF)
    mixing16 = jax.nn.sigmoid(
        over_quarters(jnp.sum(normed_tile.astype(F32) * mixer_tile, axis=-1, keepdims=True))
    )
    rows_x[x, z] = normed_tile
    send_all(NZ, z, zdev, lambda p: rows_x.at[x, z], rows_x.at[x, z], xz_s, xz_r.at[z])

    def to_x(zz):
        send_all(NX, x, xdev, lambda p: rows_x.at[x, zz], rows_x.at[x, zz], xx_s, xx_r)

    to_x(z)

    lane4, row4 = iota((4, 128), 1), iota((4, 128), 0)
    both_factors = jnp.where(lane4 == row4, scale_tile[0:4], 0.0) + jnp.where(lane4 == row4 + 4, mixing16[0:4], 0.0)
    sc_send[...] = jnp.sum(both_factors, axis=0, keepdims=True)
    send_all(NT, t, tdev, lambda p: sc_send, sc_recv.at[t], sc_s, sc_r)
    sc_recv[t] = sc_send[...]
    weights_to_y(1, y, ahead).start()
    weights_to_y(1, y, behind).start()

    def relay(h):
        weights_to_y(h, origin, onward).wait_recv()
        weights_to_y(h, origin, onward).start()
        weights_to_sibling(h, origin).start()

    phase("relay_a")
    relay(0)

    phase("xz_near")

    def pass_on(n, c):
        d = n // 2 + 1
        p = lax.rem(z + d + lax.rem(n, 2) * (NZ - 2 * d), NZ)
        remote(rows_x.at[x, p], rows_x.at[x, p], xz_s, xz_r.at[p], zdev(p)).wait_recv()
        to_x(p)
        return c
    lax.fori_loop(0, 2, pass_on, 0)

    phase("md_wait")
    arrived_all(md_recv.at[0:31], md_s, md_r)
    arrived = md_recv[...].reshape(256, 128)
    ag_recv[t] = jnp.concatenate([dot(unpack[h], arrived) for h in range(2)], axis=1).astype(BF)
    own_rows = ag_recv.at[t]

    halves_of = (pl.ds(0, 64), pl.ds(64, 64))
    for h in range(2):
        block = ag_recv.at[t, halves_of[h]]
        remote(block, block, ag_s, ah_r.at[h], ydev(onward)).start()
    remote(own_rows, own_rows, ag_s, ag_r.at[t], ydev(origin)).start()
    remote(own_rows, own_rows, ac_s, ag_r.at[t], sibling).start()

    phase("xz_wait")
    lax.fori_loop(2, NZ - 1, pass_on, 0)

    phase("relay_b")
    relay(1)

    phase("sc_wait")
    arrived_all(sc_recv.at[0:7], sc_s, sc_r)
    factors = jnp.concatenate([jnp.broadcast_to(sc_recv[p], (4, 128)) for p in range(NT)], axis=0)
    fac_lane, fac_row = iota((32, 128), 1), iota((32, 128), 0) & 3
    mixing = jnp.sum(jnp.where(fac_lane == fac_row + 4, factors, 0.0), axis=1, keepdims=True)
    factors = jnp.sum(jnp.where(fac_lane == fac_row, factors, 0.0), axis=1, keepdims=True)
    sx_send[...] = jnp.sum(taken * factors, axis=0, keepdims=True)
    spread_out(lambda p: sx_send, sx_recv.at[ep], sx_s, sx_r)
    sx_recv[ep] = sx_send[...]

    need("eg", "eu", "ed")

    def chunk(p):
        depth = pl.ds(pl.multiple_of(p * 256, 256), 256)
        rows_p = ag_recv[p]
        acc[:, 0:512] += dot(rows_p, eg[depth, :])
        acc[:, 512:1024] += dot(rows_p, eu[depth, :])

    acc[...] = jnp.zeros_like(acc)

    def group_rows(p, ssem, dev):
        block = ag_recv.at[2 * p + core]
        return remote(block, block, ssem, ag_r.at[2 * p + core], dev)

    def direct_chunk(p):
        group_rows(p, ag_s, ydev(p)).wait_recv()
        group_rows(p, ac_s, sibling).start()

    def other_chunk(p):
        block = ag_recv.at[2 * p + 1 - core]
        remote(block, block, ac_s, ag_r.at[2 * p + 1 - core], sibling).wait_recv()
        chunk(2 * p + 1 - core)

    chunk(t)
    other_chunk(y)
    phase("weights_on")
    for h in range(2):
        weights_to_y(h, onward, onward).wait_recv()
        weights_to_sibling(h, onward).start()
    phase("chunks")
    for h in range(2):
        block = ag_recv.at[2 * origin + core, halves_of[h]]
        remote(block, block, ag_s, ah_r.at[h], ydev(origin)).wait_recv()
        remote(block, block, ag_s, ag_r.at[2 * origin + core], ydev(onward)).start()
    group_rows(origin, ac_s, sibling).start()
    chunk(2 * origin + core)
    direct_chunk(onward)
    chunk(2 * onward + core)
    other_chunk(onward)
    other_chunk(origin)
    phase("weights_across")
    for h in range(2):
        weights_to_y(h, across, onward).wait_recv()
        weights_to_sibling(h, across).start()
    phase("ag_across")
    direct_chunk(across)
    phase("xx_wait")
    arrived_all(rows_x.at[0:3], xx_s, xx_r)
    phase("dense_a")
    tiles = rows_x[...].reshape(512, 512)
    spread_row = iota((128, 512), 0)
    spread_col = iota((128, 512), 1)
    for q in range(4):
        take = onehot(spread_col == (spread_row >> 2) * 16 + 4 * q + (spread_row & 3))
        block = dot(take, tiles).astype(BF)
        rows_a[2 * q] = block[:, 0:256]
        rows_a[2 * q + 1] = block[:, 256:512]

    def gate_up_by(side):
        total = jnp.zeros((128, 384), F32)
        for p in range(4):
            n = 2 * p + side
            total = total + dot_nt(rows_a[n], dw[n, 176:560])
        return total

    gate_up[...] = gate_up_by(core)
    phase("weights_wait")
    arrived_all(dw.at[0:4, 0:528], wc_s, wc_r)
    phase("dense_mm")
    both_sums = gate_up[...] + gate_up_by(1 - core)
    up = pltpu.roll(both_sums, 384 - 176, 1)
    hidden = jnp.where(iota((128, 256), 1) < 176, jax.nn.silu(both_sums[:, 0:256]) * up[:, 0:256], 0.0).astype(BF)
    x_on, x_back, x_across = lax.rem(x + 1 + 2 * core, 4), lax.rem(x + 3 + 2 * core, 4), lax.rem(x + 2, 4)

    def y_across(q):
        return remote(part_y.at[q, x_across], ry_recv.at[q], ry_s, ry_r.at[q], xdev(x_on))

    def y_back(q):
        return remote(part_y.at[q, x_back], yx_recv.at[1, q], yx_s, yx_r.at[q], xdev(x_back))

    def y_on(q):
        return remote(my_send.at[q], yx_recv.at[0, q], yx_s, yx_r.at[q], xdev(x_on))

    for q in range(4):
        for n in range(2):
            part = dot(hidden, dw[2 * q + n, 0:256]).astype(BF)
            part_y[q, :, :, 256 * n : 256 * (n + 1)] = part.reshape(NX, 32, 256)
        y_across(q).start()
        y_back(q).start()

    def merge_on():
        for q in range(4):
            y_across(q).wait_recv()
            my_send[q] = (part_y[q, x_on].astype(F32) + ry_recv[q].astype(F32)).astype(BF)
            y_on(q).start()

    phase("last_chunk")
    chunk(2 * across + core)
    other_chunk(across)
    phase("down")
    arrived_all(sx_recv.at[0:31], sx_s, sx_r)
    every = jnp.concatenate([sx_recv[p] for p in range(NE)], axis=0)
    repeat = jnp.where((iota((128, 32), 0) >> 2) == iota((128, 32), 1), 1.0, 0.0)
    every = jnp.dot(repeat, every, preferred_element_type=F32, precision=lax.Precision.HIGHEST)
    wanted = iota((128, 256), 1) == 8 * ep + (iota((128, 256), 0) & 3)
    factor = jnp.sum(jnp.where(wanted, every, 0.0), axis=1, keepdims=True)
    hidden_e = (jax.nn.silu(acc[:, 0:512] * factor) * (acc[:, 512:1024] * factor)).astype(BF)

    def down_tile(p):
        return dot(hidden_e, ed[:, pl.ds(pl.multiple_of(p * 256, 256), 256)])

    for p in (across, onward, y, origin):
        pair_send[p] = down_tile(2 * p + 1 - core).astype(BF)
        remote(pair_send.at[p], pair_recv.at[p], pair_s, pair_r.at[p], sibling).start()

    def pair_sum(p):
        own = down_tile(2 * p + core)
        remote(pair_send.at[p], pair_recv.at[p], pair_s, pair_r.at[p], sibling).wait_recv()
        return own + pair_recv[p].astype(F32)

    def group_to(p, target, slot, h, sem):
        part = pl.ds(64 * h, 64)
        return remote(er_send.at[p, part], er_recv.at[slot, part], er_s, er_r.at[sem], ydev(target))

    er_send[across] = pair_sum(across).astype(BF)
    for h in range(2):
        group_to(across, onward, 0, h, h).start()
    er_send[origin] = pair_sum(origin).astype(BF)
    for h in range(2):
        group_to(origin, origin, 1, h, 2).start()
    er_own[y] = pair_sum(y)
    er_own[onward] = pair_sum(onward)

    def group_merge():
        for h in range(2):
            group_to(across, onward, 0, h, h).wait_recv()
            part = pl.ds(64 * h, 64)
            er_send[onward, part] = (er_own[onward, part] + er_recv[0, part].astype(F32)).astype(BF)
            group_to(onward, onward, 2, h, 3).start()

    phase("merge_on")
    merge_on()
    phase("group_merge")
    group_merge()
    phase("yx_wait")
    zs_row, zs_col = iota((64, 32), 0), iota((64, 32), 1)
    to_half = [onehot(zs_row == (zs_col >> 2) * 8 + 4 * h + (zs_col & 3)) for h in range(2)]

    def to_column(p, n):
        remote(zt_send.at[p, n], zt_recv.at[z * NT + t], zt_s, zt_r, (p * NX + x, n)).start()

    for q in range(4):
        arrived_all(yx_recv.at[:, q], yx_s, yx_r.at[q])
        summed = part_y[q, x].astype(F32) + yx_recv[0, q].astype(F32) + yx_recv[1, q].astype(F32)
        summed = summed.astype(BF)
        low, high = dot(to_half[0], summed), dot(to_half[1], summed)
        for n in range(2):
            tile = low[:, 256 * n : 256 * n + 128] + high[:, 256 * n + 128 : 256 * n + 256]
            zt_send[:, 2 * q + n] = tile.astype(BF).reshape(NZ, 8, 128)

        def column_out(k, c, q=q):
            for n in range(2):
                to_column(lax.rem(z + k, NZ), 2 * q + n)
            return c
        lax.fori_loop(NZ // 2, NZ, column_out, 0)
        lax.fori_loop(1, NZ // 2, column_out, 0)

    def group_out(k, c):
        to_column(z, lax.rem(t + k, NT))
        return c
    lax.fori_loop(1, NT, group_out, 0)
    zt_recv[z * NT + t] = zt_send[z, t]

    phase("drain_early")
    sent_all(rs_recv.at[0:7], rs_s, rs_r)
    sent_all(rr_recv.at[0:7], rr_s, rr_r)
    sent_all(sc_recv.at[0:7], sc_s, sc_r)
    sent_all(sx_recv.at[0:31], sx_s, sx_r)
    sent_all(md_recv.at[0:31], md_s, md_r)
    sent_all(rows_x.at[0, 0:7], xz_s, xz_r.at[0])

    sent_all(rows_x.at[0:3], xx_s, xx_r)
    sent_all(dw.at[0:3, 0:528], wy_s, wy_r.at[0, 0])
    sent_all(dw.at[0:4, 0:528], wc_s, wc_r)
    sent_all(ry_recv, ry_s, ry_r.at[0])
    sent_all(yx_recv, yx_s, yx_r.at[0])
    sent_all(ag_recv.at[0:3], ag_s, ag_r.at[0])
    sent_all(ag_recv.at[0:4], ac_s, ag_r.at[0])
    sent_all(pair_send, pair_s, pair_r.at[0])

    phase("er_wait")
    arrived_all(er_recv.at[1], er_s, er_r.at[2])
    arrived_all(er_recv.at[2], er_s, er_r.at[3])
    result = (er_own[y] + er_recv[1].astype(F32) + er_recv[2].astype(F32)).astype(BF)
    mr_send[...] = (dot(pack[0], result[:, 0:128]) + dot(pack[1], result[:, 128:256])).astype(BF).reshape(NE, 8, 128)
    spread_out(lambda p: mr_send.at[p], mr_recv.at[ep], mr_s, mr_r)
    mr_recv[ep] = mr_send[ep]

    phase("zt_wait")
    un_row, un_col = iota((32, 512), 0), iota((32, 512), 1)
    un_token = ((un_col >> 3) & 7) * 4 + (un_col & 3)
    gather = [onehot((un_token == un_row) & (((un_col >> 2) & 1) == h)) for h in range(2)]
    sent_all(er_recv.at[0:3], er_s, er_r.at[0])
    arrived_all(zt_recv.at[0:63], zt_s, zt_r)
    columns_in = zt_recv[...].reshape(512, 128)
    dense_rows = jnp.concatenate([dot(gather[h], columns_in) for h in range(2)], axis=1) * mixing
    phase("mr_wait")
    arrived_all(mr_recv.at[0:31], mr_s, mr_r)
    returned = mr_recv[...].reshape(256, 128)
    phase("final")
    moe = jnp.concatenate([dot(combine[h], returned) for h in range(2)], axis=1)
    final_v[...] = (middle + moe + dense_rows).astype(BF)

    phase("drain")
    sent_all(zt_recv.at[0:63], zt_s, zt_r)
    sent_all(mr_recv.at[0:31], mr_s, mr_r)
    phase(None)


def hand_out(final_v, state_v, final_out, state_out, sem):
    copies = [pltpu.make_async_copy(final_v, final_out, sem.at[8])]
    for n in range(8):
        part = pl.ds(4 * n, 4)
        copies.append(pltpu.make_async_copy(state_v.at[part], state_out.at[part], sem.at[n]))
    for copy in copies:
        copy.start()
    for copy in copies:
        copy.wait()


def per_device(*args):
    args = list(args)
    for n in (12, 13, 15, 16):
        args[n] = args[n].T
    inv = jnp.asarray((THETA ** (-np.arange(64) / 64.0)).astype(np.float32)[None, :])
    vmem = pltpu.VMEM

    def dma(*shape):
        return pltpu.SemaphoreType.DMA(shape)

    one = pltpu.SemaphoreType.DMA

    scratch = [
        vmem((32, 2048), BF), vmem((2048,), BF), vmem((2048, 512), BF), vmem((128,), BF),
        vmem((128, 2048), BF), vmem((32, 128, 128), F32), vmem((32,), jnp.int32), vmem((2048,), BF),
        vmem((2048,), BF), vmem((2, 32), jnp.int32), vmem((2, 32), BF),
        vmem((2048, 512), BF), vmem((2048, 512), BF), vmem((512, 2048), BF), vmem((1, 64), F32),
        vmem((32, 128), F32), vmem((8, 32, 256), BF), vmem((8, 32, 256), BF),
        vmem((8, 16, 512), BF), vmem((8, 16, 512), BF), vmem((1, 128), F32), vmem((8, 1, 128), F32),
        vmem((1, 256), F32), vmem((32, 1, 256), F32), vmem((4, 8, 16, 512), BF), vmem((8, 560, 256), BF),
        vmem((4, 4, 32, 512), BF), vmem((4, 32, 512), BF), vmem((4, 32, 512), BF), vmem((2, 4, 32, 512), BF),
        vmem((32, 8, 128), BF), vmem((32, 8, 128), BF), vmem((8, 128, 256), BF),
        vmem((4, 128, 256), BF), vmem((4, 128, 256), BF), vmem((4, 128, 256), F32),
        vmem((4, 128, 256), BF), vmem((4, 128, 256), BF), vmem((32, 8, 128), BF), vmem((32, 8, 128), BF),
        vmem((8, 8, 8, 128), BF), vmem((64, 8, 128), BF), vmem((128, 1024), F32),
        vmem((8, 128, 256), BF), vmem((128, 384), F32),
        dma(18),
        one, one, one, one, one, one, one, one, one, dma(8), one, one,
        one, dma(2, 4), one, one, one, dma(4), one, dma(4),
        one, one, one, dma(8), dma(2), one, one, dma(4), one, dma(4), one, one, one, one,
    ]
    hbm = pl.BlockSpec(memory_space=pltpu.HBM)
    here = pl.BlockSpec(memory_space=pltpu.VMEM)
    args = [pltpu.with_memory_space_constraint(a, pltpu.HBM) for a in args]
    inv = pltpu.with_memory_space_constraint(inv, pltpu.HBM)
    final, new_state = pl.pallas_call(
        step_kernel,
        out_shape=(
            jax.ShapeDtypeStruct((32, 256), BF),
            jax.ShapeDtypeStruct((32, 1, 128, 128), F32),
        ),
        in_specs=[hbm] * 21,
        out_specs=(here, here),
        scratch_shapes=scratch,
        compiler_params=pltpu.CompilerParams(
            collective_id=0, has_side_effects=True, vmem_limit_bytes=50000 * 1024
        ),
    )(*args, inv)
    return pl.pallas_call(
        hand_out,
        out_shape=(
            jax.ShapeDtypeStruct((32, 256), BF),
            jax.ShapeDtypeStruct((32, 1, 128, 128), F32),
        ),
        in_specs=[here, here],
        out_specs=(hbm, hbm),
        scratch_shapes=[dma(9)],
        compiler_params=pltpu.CompilerParams(vmem_limit_bytes=16384 * 1024),
    )(final, new_state)


def solution(mesh):
    in_specs = (
        P("ep", None), P(), P(None, "tp"), P(None, "tp"), P(None, "tp"), P(None, "tp"), P("tp"),
        P("tp", None), P("ep", "tp", None, None), P("ep"), P(), P(), P("tp", "ep"), P("tp", "ep"),
        P("ep", "tp"), P("ep", None), P("ep", None), P("ep", None, "tp"), P("ep", None, "tp"),
        P("ep", "tp", None),
    )
    out_specs = (P("ep", "tp"), P("ep", "tp", None, None))
    return jax.shard_map(per_device, mesh=mesh, in_specs=in_specs, out_specs=out_specs, check_vma=False)
```
